256 devices in a mesh: ep: 128 (over z, y, x), tp: 2 (over core).
Axes of the slice: x: 4, y: 4, z: 8, core: 2. Of those that a mesh axis runs over, the one named last changes fastest.
Arguments:
- hidden: bfloat16 [2048, 2048], P('ep'), may hold values from -6 to 6
- attn_gain: bfloat16 [2048], replicated, may hold values from 0.099609375 to 1.8984375
- query_weight: bfloat16 [2048, 2048], P(None, 'tp'), may hold values from -0.125 to 0.125
- key_weight: bfloat16 [2048, 128], P(None, 'tp'), may hold values from -0.125 to 0.125
- value_weight: bfloat16 [2048, 128], P(None, 'tp'), may hold values from -0.125 to 0.125
- forget_weight: bfloat16 [2048, 32], P(None, 'tp'), may hold values from -0.125 to 0.125
- forget_bias: float32 [32], P('tp'), may hold values from -1 to 4
- cache_keys: bfloat16 [2048, 2, 64, 1024], P('ep', 'tp'), may hold values from -64 to 64
- cache_values: bfloat16 [2048, 2, 64, 1024], P('ep', 'tp'), may hold values from -6 to 6
- cache_logsum: float32 [2048, 32, 1024], P('ep', 'tp'), may hold values from -144 to 0, as said below
- lengths: int32 [2048], P('ep'), may hold values from 2 to 1023, as said below
- out_weight: bfloat16 [2048, 2048], P('ep'), may hold values from -0.125 to 0.125
- ffn_gain: bfloat16 [2048], replicated, may hold values from 0.099609375 to 1.8984375
- expert_ids: int32 [2048, 6], P('ep'), may hold values from 0 to 127, all different within a row; in each aligned block of 16 rows (0 to 15, 16 to 31, ...) at most 2 rows name the same one
- expert_scores: float32 [2048, 6], P('ep'), may hold values from 0.1 to 1
- gate_weights: bfloat16 [128, 2048, 512], P('ep', None, 'tp'), may hold values from -0.125 to 0.125
- up_weights: bfloat16 [128, 2048, 512], P('ep', None, 'tp'), may hold values from -0.125 to 0.125
- down_weights: bfloat16 [128, 512, 2048], P('ep', 'tp'), may hold values from -0.25 to 0.25
Outputs:
- updated: bfloat16 [2048, 2048], P('ep')
- new_key: bfloat16 [2048, 2, 64], P('ep', 'tp')
- new_value: bfloat16 [2048, 2, 64], P('ep', 'tp')
- new_logsum: float32 [2048, 32], P('ep', 'tp')
The draws below stay inside these ranges and needn't reach their ends.
Inputs may be any that keep to these rules, and one draw needn't show every extreme that they name: `cache_logsum`: non-increasing along the positions. The new token stands at position lengths; some sequence has 1023 cached positions. `expert_ids`: each row names 6 different experts; the rows of one index of ep name one expert at most 2 times.
All inputs are finite; a program needn't handle non-finite values.
Results may differ from the reference program's by a relative error of at most 0.006.
Values may be sent and summed in bfloat16 or wider, within the bound.
A program may use at most 64 MiB of HBM per device.

```python
import math
import jax
import jax.numpy as jnp
import numpy as np
from jax import lax

D = 2048
HEADS = 32
HD = 64
KV_HEADS = 2
DEXP = 512
TOP_K = 6
CACHE_POSITIONS = 1024
SEQ_DEV = 16
BATCH_SEQUENCES = 2048
EXPERTS = 128
CAP = 2
N_EP = 128
N_TP = 2


def draw_cache_keys(key, part):
    random_subkeys = jax.random.split(key, 1)
    values_drawn = jnp.clip(jax.random.normal(random_subkeys[0], (BATCH_SEQUENCES, KV_HEADS, HD, CACHE_POSITIONS), jnp.float32), -6.0, 6.0)
    return values_drawn.astype(jnp.bfloat16)


def draw_cache_logsum(key, part):
    random_subkeys = jax.random.split(key, 7)
    head_order = jax.random.permutation(random_subkeys[0], HEADS)
    is_sluggish = head_order < HEADS // 2
    is_sluggish = is_sluggish.astype(jnp.float32)[None, :, None]
    slow_rate = jax.random.uniform(random_subkeys[1], (1, HEADS, 1), jnp.float32, 0.2, 0.8) / CACHE_POSITIONS
    fast_rate = 1.0 / jax.random.uniform(random_subkeys[2], (1, HEADS, 1), jnp.float32, 30.0, 100.0)
    decay_rate = is_sluggish * slow_rate + (1.0 - is_sluggish) * fast_rate
    sequence_factor = jnp.exp(jax.random.uniform(random_subkeys[3], (BATCH_SEQUENCES, 1, 1), jnp.float32, math.log(0.5), math.log(2.0)))
    random_wobble = jax.random.uniform(random_subkeys[4], (BATCH_SEQUENCES, HEADS, CACHE_POSITIONS), jnp.float32, 0.4, 1.6)
    spike_mask = (jax.random.uniform(random_subkeys[5], (BATCH_SEQUENCES, 1, CACHE_POSITIONS)) < 3.0 / CACHE_POSITIONS).astype(jnp.float32)
    shift_amount = jax.random.uniform(random_subkeys[6], (BATCH_SEQUENCES, HEADS, CACHE_POSITIONS), jnp.float32, 0.22, 0.69)
    step_logarithm = -(decay_rate * sequence_factor * random_wobble) - spike_mask * shift_amount * is_sluggish
    return jnp.cumsum(step_logarithm, axis=-1).astype(jnp.float32)


def draw_lengths(key, part):
    random_subkeys = jax.random.split(key, 2)
    groups = BATCH_SEQUENCES // SEQ_DEV
    device_top = jax.random.randint(random_subkeys[0], (groups, 1), CACHE_POSITIONS // 8, CACHE_POSITIONS - 1)
    raw_bits = jax.random.randint(random_subkeys[1], (groups, SEQ_DEV), 0, 1 << 20)
    lengths_drawn = 2 + raw_bits % (device_top - 1)
    lengths_drawn = lengths_drawn.reshape(BATCH_SEQUENCES).at[0].set(CACHE_POSITIONS - 1)
    return lengths_drawn.astype(jnp.int32)


def levels(own_key, dims, pieces, smallest, high):
    level, own = 1.0, jax.random.fold_in(own_key, 6)
    for position, blocks in pieces:
        steps = jnp.exp(jax.random.uniform(jax.random.fold_in(own, position), (blocks,), jnp.float32, smallest / len(pieces), high / len(pieces)))
        level = level * jnp.repeat(steps, dims[position] // blocks).reshape([-1 if axis == position else 1 for axis in range(len(dims))])
    return level


def deal_out(key, own, number, rows, number_of, top, most, lean):
    sequence = jax.random.permutation(key, number_of)
    packed, ordinary = load_shares(number_of, rows * top, most, lean, True), load_shares(number_of, rows * top, most, lean, False)
    places = jnp.arange(number_of)

    def named(tallies, turn):
        used = int((tallies > 0).sum())
        fixed = max(1, used // 4)
        moved = fixed + (places - fixed + turn * (used - fixed)) % max(1, number_of - fixed)
        return jnp.zeros((number_of,), jnp.int32).at[sequence[jnp.where(places < fixed, places, moved)]].set(jnp.asarray(tallies, jnp.int32))

    tallies = jnp.where(number % 4 == 0, named(packed, number // 4), named(ordinary, number - number // 4 - 1))
    mixed = jax.random.permutation(jax.random.fold_in(own, 3), number_of)
    donor, receiver = mixed[0:number_of // 2 * 2:2], mixed[1:number_of // 2 * 2:2]
    room = jnp.minimum(tallies[donor] - 1, most - tallies[receiver]) // 2
    room = jnp.where((donor == sequence[0]) | (receiver == sequence[0]) | (tallies[receiver] == 0), 0, jnp.maximum(room, 0))
    moved = jax.random.randint(jax.random.fold_in(own, 4), (number_of // 2,), 0, 1 << 20) % (room + 1)
    tallies = tallies.at[donor].add(-moved).at[receiver].add(moved)
    items = jnp.searchsorted(jnp.cumsum(tallies), jnp.arange(rows * top), side="right").astype(jnp.int32)
    listing = items.reshape(top, rows).T
    listing = listing[jax.random.permutation(jax.random.fold_in(own, 1), rows)]
    turn = jax.random.randint(jax.random.fold_in(own, 2), (rows, 1), 0, top)
    return jnp.take_along_axis(listing, (jnp.arange(top)[None, :] + turn) % top, axis=1)


def load_shares(amount, total, reach, skew, full):
    portions = [(1 << 20) // math.isqrt(standing ** skew) + 1 for standing in range(1, amount + 1)]
    largest = reach if full else min(reach, max(-(-total // amount), total * portions[0] // sum(portions)))
    least = 1 if total - largest >= amount - 1 else 0
    given, rest = [largest] + [least] * (amount - 1), total - largest - least * (amount - 1)
    while rest > 0:
        movable = [i for i in range(1, amount) if given[i] < largest] or [i for i in range(1, amount) if given[i] < reach]
        whole, remaining = sum([portions[i] for i in movable]), rest
        for i in movable:
            more = min(reach - given[i], max(1, remaining * portions[i] // whole), rest)
            given[i] = given[i] + more
            rest = rest - more
    return np.array(given)


def bell_draw(stream_key, dims, spread, reach, cuts=(), kind=jnp.bfloat16):
    values = jax.random.normal(stream_key, dims, jnp.float32) * spread
    if len(cuts) > 0:
        values = levels(stream_key, dims, cuts, -0.22, 0.18) * values
    return jnp.clip(values, min=-reach, max=reach).astype(kind)


def setup_inputs(seed: int = 0) -> dict:
    arg_keys = jax.random.split(jax.random.key(seed), 19)
    hidden = bell_draw(arg_keys[0], (BATCH_SEQUENCES, D), 1.0, 6.0, ((0, 128),))
    attn_gain = jnp.clip(1.0 + 0.18 * jax.random.normal(arg_keys[1], (D,), jnp.float32), 0.099609375, 1.8984375).astype(jnp.bfloat16)
    query_weight = bell_draw(arg_keys[2], (D, HEADS * HD), D ** -0.5, 0.125, ((1, 2),))
    key_weight = bell_draw(arg_keys[3], (D, KV_HEADS * HD), D ** -0.5, 0.125, ((1, 2),))
    value_weight = bell_draw(arg_keys[4], (D, KV_HEADS * HD), D ** -0.5, 0.125, ((1, 2),))
    forget_weight = bell_draw(arg_keys[5], (D, HEADS), D ** -0.5, 0.125, ((1, 2),))
    forget_bias = jnp.clip(-1.0 + 5.0 * jax.random.uniform(arg_keys[6], (HEADS,), jnp.float32) ** levels(arg_keys[6], (HEADS,), ((0, 2),), -0.2, 0.2), -1.0, 4.0)
    cache_keys = draw_cache_keys(jax.random.fold_in(arg_keys[18], 71), 0)
    cache_values = bell_draw(arg_keys[8], (BATCH_SEQUENCES, KV_HEADS, HD, CACHE_POSITIONS), 1.0, 6.0, ((0, 128), (1, 2)))
    cache_logsum = draw_cache_logsum(jax.random.fold_in(arg_keys[18], 71), 0)
    lengths = draw_lengths(jax.random.fold_in(arg_keys[18], 71), 0)
    out_weight = bell_draw(arg_keys[11], (D, HEADS * HD), (HEADS * HD) ** -0.5, 0.125, ((0, 128),))
    ffn_gain = jnp.clip(1.0 + 0.18 * jax.random.normal(arg_keys[12], (D,), jnp.float32), 0.099609375, 1.8984375).astype(jnp.bfloat16)
    expert_ids_keys = jax.random.split(jax.random.fold_in(arg_keys[13], 1), BATCH_SEQUENCES // SEQ_DEV)
    expert_ids_turns = jax.random.permutation(jax.random.fold_in(arg_keys[13], 3), BATCH_SEQUENCES // SEQ_DEV)
    expert_ids = jax.vmap(lambda own, number: deal_out(jax.random.fold_in(arg_keys[13], 2), own, number, SEQ_DEV, EXPERTS, TOP_K, CAP, 2))(expert_ids_keys, expert_ids_turns).reshape((BATCH_SEQUENCES, TOP_K))
    expert_scores = jnp.clip(jnp.exp(math.log(1.0) - 2.3025851 * jax.random.uniform(arg_keys[14], (BATCH_SEQUENCES, TOP_K), jnp.float32) ** levels(arg_keys[14], (BATCH_SEQUENCES, TOP_K), ((0, 128),), -0.2, 0.2)), 0.1, 1.0)
    gate_weights = bell_draw(arg_keys[15], (EXPERTS, D, DEXP), D ** -0.5, 0.125, ((0, 128), (2, 2)))
    up_weights = bell_draw(arg_keys[16], (EXPERTS, D, DEXP), D ** -0.5, 0.125, ((0, 128), (2, 2)))
    down_weights = bell_draw(arg_keys[17], (EXPERTS, DEXP, D), DEXP ** -0.5, 0.25, ((0, 128), (1, 2)))
    return {"hidden": hidden, "attn_gain": attn_gain, "query_weight": query_weight, "key_weight": key_weight, "value_weight": value_weight, "forget_weight": forget_weight, "forget_bias": forget_bias, "cache_keys": cache_keys, "cache_values": cache_values, "cache_logsum": cache_logsum, "lengths": lengths, "out_weight": out_weight, "ffn_gain": ffn_gain, "expert_ids": expert_ids, "expert_scores": expert_scores, "gate_weights": gate_weights, "up_weights": up_weights, "down_weights": down_weights}


epsilon = 1e-06

def root_norm(values_in, gain):
    floats = values_in.astype(jnp.float32)
    inv_root = lax.rsqrt(lax.optimization_barrier(jnp.mean(floats * floats, axis=-1, keepdims=True)) + epsilon)
    return floats * inv_root * gain.astype(jnp.float32)

def attend(block):
    queries, keys_block, values_block, logsum_block, lengths_block, key_new, value_new, newsum = block
    rows_here = queries.shape[0]
    query_heads = queries.shape[1] // HD
    key_heads = keys_block.shape[1]
    group_size = query_heads // key_heads
    score_scale = HD ** (-0.5)
    grouped = queries.astype(jnp.float32).reshape(rows_here, key_heads, group_size, HD)
    scores = jnp.einsum('sgjd,sgdp->sgjp', grouped, keys_block.astype(jnp.float32))
    scores = scores.reshape(rows_here, query_heads, CACHE_POSITIONS) * score_scale
    scores = scores + newsum[:, :, None] - logsum_block
    positions = jnp.arange(CACHE_POSITIONS, dtype=jnp.int32)
    is_live = positions[None, :] < lengths_block[:, None]
    scores = jnp.where(is_live[:, None, :], scores, -jnp.inf)
    own_score = jnp.einsum('sgjd,sgd->sgj', grouped, key_new.astype(jnp.float32)).reshape(rows_here, query_heads) * score_scale
    top_score = jnp.maximum(lax.optimization_barrier(jnp.max(scores, axis=-1)), own_score)
    past_exp = jnp.exp(scores - top_score[:, :, None])
    own_exp = jnp.exp(own_score - top_score)
    denominator = lax.optimization_barrier(jnp.sum(past_exp, axis=-1)) + own_exp
    past_weight = (past_exp / denominator[:, :, None]).astype(jnp.bfloat16)
    own_weight = (own_exp / denominator).astype(jnp.bfloat16)
    attended = jnp.einsum('sgjp,sgdp->sgjd', past_weight.astype(jnp.float32).reshape(rows_here, key_heads, group_size, CACHE_POSITIONS), values_block.astype(jnp.float32))
    attended = attended + own_weight.astype(jnp.float32).reshape(rows_here, key_heads, group_size)[:, :, :, None] * value_new.astype(jnp.float32)[:, :, None, :]
    return attended.reshape(rows_here, query_heads * HD).astype(jnp.bfloat16)

def blocked(array):
    return array.reshape((BATCH_SEQUENCES // SEQ_DEV, SEQ_DEV) + array.shape[1:])

def reference(hidden, attn_gain, query_weight, key_weight, value_weight, forget_weight, forget_bias, cache_keys, cache_values, cache_logsum, lengths, out_weight, ffn_gain, expert_ids, expert_scores, gate_weights, up_weights, down_weights):
    normed = root_norm(hidden, attn_gain).astype(jnp.bfloat16)
    queries = jnp.dot(normed, query_weight, preferred_element_type=jnp.float32).astype(jnp.bfloat16)
    new_key = jnp.dot(normed, key_weight, preferred_element_type=jnp.float32).astype(jnp.bfloat16).reshape(BATCH_SEQUENCES, KV_HEADS, HD)
    new_value = jnp.dot(normed, value_weight, preferred_element_type=jnp.float32).astype(jnp.bfloat16).reshape(BATCH_SEQUENCES, KV_HEADS, HD)
    log_forget = jax.nn.log_sigmoid(jnp.dot(normed, forget_weight, preferred_element_type=jnp.float32) + forget_bias)
    positions = jnp.arange(CACHE_POSITIONS, dtype=jnp.int32)
    is_last = positions[None, :] == (lengths - 1)[:, None]
    new_logsum = lax.optimization_barrier(jnp.sum(jnp.where(is_last[:, None, :], cache_logsum, 0.0), axis=-1)) + log_forget
    blocks = tuple((blocked(array) for array in (queries, cache_keys, cache_values, cache_logsum, lengths, new_key, new_value, new_logsum)))
    attended = lax.map(attend, blocks).reshape(BATCH_SEQUENCES, HEADS * HD)
    mixed = jnp.dot(attended, out_weight.T, preferred_element_type=jnp.float32).astype(jnp.bfloat16)
    residual = hidden.astype(jnp.float32) + mixed.astype(jnp.float32)
    ffn_in = root_norm(residual, ffn_gain).astype(jnp.bfloat16)
    route_count = BATCH_SEQUENCES * TOP_K
    flat_ids = expert_ids.reshape(route_count)
    onehot = (flat_ids[:, None] == jnp.arange(EXPERTS, dtype=jnp.int32)[None, :]).astype(jnp.int32)
    running = jnp.cumsum(onehot.reshape(N_EP, SEQ_DEV * TOP_K, EXPERTS), axis=1).reshape(route_count, EXPERTS)
    slot_index = lax.optimization_barrier(jnp.sum(running * onehot, axis=1)) - 1
    source = jnp.arange(route_count, dtype=jnp.int32) // (SEQ_DEV * TOP_K)
    placement = flat_ids * (N_EP * CAP) + source * CAP + slot_index
    token_of_route = jnp.arange(route_count, dtype=jnp.int32) // TOP_K
    slot_table = jnp.full((EXPERTS * N_EP * CAP,), BATCH_SEQUENCES, dtype=jnp.int32).at[placement].set(token_of_route)
    padded = jnp.concatenate([ffn_in, jnp.zeros((1, D), jnp.bfloat16)], axis=0)
    expert_rows = padded[slot_table].reshape(EXPERTS, N_EP * CAP, D)
    share_width = DEXP // N_TP

    def run_expert(block):
        rows_in, gate_one, up_one, down_one = block
        gate_act = jnp.dot(rows_in, gate_one, preferred_element_type=jnp.float32)
        up_act = jnp.dot(rows_in, up_one, preferred_element_type=jnp.float32)
        hidden_act = (jax.nn.silu(gate_act) * up_act).astype(jnp.bfloat16)
        summed = jnp.zeros((rows_in.shape[0], D), jnp.float32)
        for block_index in range(N_TP):
            lower = block_index * share_width
            partial_value = jnp.dot(hidden_act[:, lower:lower + share_width], down_one[lower:lower + share_width], preferred_element_type=jnp.float32)
            summed = summed + partial_value.astype(jnp.bfloat16).astype(jnp.float32)
        return summed.astype(jnp.bfloat16)
    expert_outputs = lax.map(run_expert, (expert_rows, gate_weights, up_weights, down_weights))
    route_out = expert_outputs.reshape(EXPERTS * N_EP * CAP, D)[placement].astype(jnp.float32).reshape(BATCH_SEQUENCES, TOP_K, D)
    route_weight = expert_scores / lax.optimization_barrier(jnp.sum(expert_scores, axis=-1, keepdims=True))
    updated = (residual + lax.optimization_barrier(jnp.sum(route_out * route_weight[:, :, None], axis=1))).astype(jnp.bfloat16)
    return (updated, new_key, new_value, new_logsum)
```

```python
import jax
import jax.numpy as jnp
from jax import lax
from jax.sharding import Mesh
from jax.experimental import pallas as pl
from jax.experimental.pallas import tpu as pltpu
from jax.sharding import PartitionSpec as P

HD = 64
TOP_K = 6
EP = ("ep_0", "ep_1", "ep_2")


epsilon = 1e-06


def root_norm(values_in, gain):
    floats = values_in.astype(jnp.float32)
    inv_root = lax.rsqrt(jnp.mean(floats * floats, axis=-1, keepdims=True) + epsilon)
    return floats * inv_root * gain.astype(jnp.float32)


NZ = 8
NX = 4
PLANE = 16
ROWS = 16
HALF = 1024
MESH = pl.DeviceIdType.MESH


def layer_kernel(
    att_ref,
    hid_ref,
    wo_ref,
    gain_ref,
    info_ref,
    gate_ref,
    up_ref,
    down_ref,
    out_ref,
    hsub,
    hall,
    infoall,
    wall,
    aall,
    part,
    part_in,
    mixed,
    res,
    sq,
    sq_in,
    disp,
    xrow,
    gate_v,
    up_v,
    down_v,
    o_out,
    o_in,
    ret,
    back,
    psum,
    tsum,
    upd,
    upd_in,
    z_send,
    z_recv,
    p_send,
    p_recv,
    f_send,
    f_recv,
    t_send,
    t_recv,
    w_sem,
):
    z = lax.axis_index("ep_0")
    y = lax.axis_index("ep_1")
    x = lax.axis_index("ep_2")
    t = lax.axis_index("tp")
    me = y * NX + x
    o = 1 - t

    def z_copy(phase, src, dst, i, zz, slot):
        return pltpu.make_async_remote_copy(
            src_ref=src,
            dst_ref=dst,
            send_sem=z_send.at[phase, i],
            recv_sem=z_recv.at[phase, slot],
            device_id={"ep_0": zz},
            device_id_type=MESH,
        )

    def p_copy(phase, src, dst, i, pp, slot):
        return pltpu.make_async_remote_copy(
            src_ref=src,
            dst_ref=dst,
            send_sem=p_send.at[phase, i],
            recv_sem=p_recv.at[phase, slot],
            device_id={"ep_1": pp // NX, "ep_2": lax.rem(pp, NX)},
            device_id_type=MESH,
        )

    def t_copy(phase, src, dst):
        return pltpu.make_async_remote_copy(
            src_ref=src,
            dst_ref=dst,
            send_sem=t_send.at[phase],
            recv_sem=t_recv.at[phase],
            device_id={"tp": o},
            device_id_type=MESH,
        )

    def over_z(fn):
        def step(d, carry):
            fn(d, lax.rem(z + d, NZ))
            return carry

        lax.fori_loop(1, NZ, step, 0)

    def over_plane(fn):
        def step(d, carry):
            fn(d, lax.rem(me + d, PLANE))
            return carry

        lax.fori_loop(1, PLANE, step, 0)

    barrier = pltpu.get_barrier_semaphore()
    over_z(lambda d, zz: pl.semaphore_signal(barrier, inc=1, device_id={"ep_0": zz}, device_id_type=MESH))
    over_plane(
        lambda d, pp: pl.semaphore_signal(
            barrier,
            inc=1,
            device_id={"ep_1": pp // NX, "ep_2": lax.rem(pp, NX)},
            device_id_type=MESH,
        )
    )
    pl.semaphore_signal(barrier, inc=1, device_id={"tp": o}, device_id_type=MESH)

    loads = []
    for zz in range(NZ):
        for h in range(2):
            rows = pl.ds(zz * 256 + h * 128, 128)
            put = pl.ds(zz * 128, 128)
            n = zz * 2 + h
            loads.append(pltpu.make_async_copy(gate_ref.at[0, rows, :], gate_v.at[h, put, :], w_sem.at[0, n]))
            loads.append(pltpu.make_async_copy(up_ref.at[0, rows, :], up_v.at[h, put, :], w_sem.at[1, n]))
            loads.append(pltpu.make_async_copy(down_ref.at[0, :, rows], down_v.at[h, :, put], w_sem.at[2, n]))
    for load in loads:
        load.start()

    for zz in range(NZ):
        hsub[:, zz * 128 : (zz + 1) * 128] = hid_ref[:, pl.ds(pl.multiple_of(zz * 256 + t * 128, 128), 128)]
    hall[z] = hsub[...]
    infoall[z] = info_ref[...]
    aall[z] = att_ref[...]
    my_columns = pl.ds(pl.multiple_of(t * HALF, HALF), HALF)
    wall[me] = wo_ref[:, my_columns]

    pl.semaphore_wait(barrier, (NZ - 1) + (PLANE - 1) + 1)

    over_z(lambda d, zz: z_copy(0, att_ref, aall.at[z], d, zz, z).start())
    over_plane(lambda d, pp: p_copy(0, wo_ref.at[:, my_columns], wall.at[me], d, pp, me).start())
    over_z(lambda d, zz: z_copy(1, info_ref, infoall.at[z], d, zz, z).start())
    over_z(lambda d, zz: z_copy(2, hsub, hall.at[z], d, zz, z).start())

    over_plane(lambda d, pp: p_copy(0, wo_ref.at[:, my_columns], wall.at[pp], d, pp, pp).wait_recv())
    over_z(lambda d, zz: z_copy(0, att_ref, aall.at[zz], d, zz, zz).wait_recv())

    att = aall[...].reshape(NZ * ROWS, HALF)
    for h in range(2):
        weights = wall[h * 8 : (h + 1) * 8].reshape(128, HALF)
        part[h] = lax.dot_general(att, weights, (((1,), (1,)), ((), ())), preferred_element_type=jnp.float32)
    give = t_copy(0, part.at[o], part_in)
    give.start()

    over_z(lambda d, zz: z_copy(1, info_ref, infoall.at[zz], d, zz, zz).wait_recv())
    info = jnp.sum(infoall[...], axis=0)
    row = lax.broadcasted_iota(jnp.int32, (PLANE * ROWS, NZ * ROWS), 0)
    token = lax.broadcasted_iota(jnp.int32, (PLANE * ROWS, NZ * ROWS), 1)
    expert = (row // ROWS + z * PLANE).astype(jnp.float32)
    named = jnp.zeros((PLANE * ROWS, NZ * ROWS), jnp.float32)
    scale = jnp.zeros((PLANE * ROWS, NZ * ROWS), jnp.float32)
    for j in range(TOP_K):
        hit = info[j : j + 1, :] == expert
        named = named + jnp.where(hit, 1.0, 0.0)
        scale = scale + jnp.where(hit, info[8 + j : 9 + j, :], 0.0)
    first = lax.broadcasted_iota(jnp.int32, (NZ * ROWS, NZ * ROWS), 0)
    second = lax.broadcasted_iota(jnp.int32, (NZ * ROWS, NZ * ROWS), 1)
    ahead = jnp.where((first // ROWS == second // ROWS) & (first < second), 1.0, 0.0).astype(jnp.bfloat16)
    rank = jnp.dot(named.astype(jnp.bfloat16), ahead, preferred_element_type=jnp.float32)
    slot = lax.rem(row, 2).astype(jnp.float32)
    here = lax.rem(row, ROWS) // 2 == token // ROWS
    pick = jnp.where(here & (rank == slot), named, 0.0)
    pick_half = pick.astype(jnp.bfloat16)
    combine = jnp.transpose(pick * scale)
    combine_high = combine.astype(jnp.bfloat16)
    combine_low = (combine - combine_high.astype(jnp.float32)).astype(jnp.bfloat16)

    give.wait_recv()
    mixed[z] = (part[t] + part_in[...]).astype(jnp.bfloat16)
    over_z(lambda d, zz: z_copy(3, mixed.at[z], mixed.at[z], d, zz, z).start())
    over_z(lambda d, zz: z_copy(2, hsub, hall.at[zz], d, zz, zz).wait_recv())
    over_z(lambda d, zz: z_copy(3, mixed.at[zz], mixed.at[zz], d, zz, zz).wait_recv())

    squares = jnp.zeros((NZ * ROWS, 128), jnp.float32)
    for zz in range(NZ):
        block = hall[:, :, zz * 128 : (zz + 1) * 128].reshape(NZ * ROWS, 128).astype(jnp.float32)
        block = block + mixed[zz].astype(jnp.float32)
        res[zz] = block
        squares = squares + block * block
    sq[...] = jnp.broadcast_to(jnp.sum(squares, axis=-1, keepdims=True), (NZ * ROWS, 128))
    give_sq = t_copy(1, sq, sq_in)
    give_sq.start()
    give_sq.wait_recv()
    inverse = lax.rsqrt((sq[...] + sq_in[...]) * (1.0 / 2048.0) + epsilon)
    for zz in range(NZ):
        gain = gain_ref[pl.ds(2 * zz + t, 1), :]
        block = (res[zz] * inverse * gain).astype(jnp.bfloat16)
        rows = jnp.dot(pick_half, block, preferred_element_type=jnp.float32)
        disp[:, :, zz * 128 : (zz + 1) * 128] = rows.astype(jnp.bfloat16).reshape(PLANE, ROWS, 128)

    over_plane(lambda d, pp: p_copy(1, disp.at[pp], xrow.at[t, me], d, pp, me).start())
    xrow[t, me] = disp[me]

    def forward(pp):
        return pltpu.make_async_remote_copy(
            src_ref=xrow.at[t, pp],
            dst_ref=xrow.at[t, pp],
            send_sem=f_send.at[pp],
            recv_sem=f_recv.at[pp],
            device_id={"tp": o},
            device_id_type=MESH,
        )

    def arrival(pp):
        return pltpu.make_async_remote_copy(
            src_ref=xrow.at[o, pp],
            dst_ref=xrow.at[o, pp],
            send_sem=f_send.at[pp],
            recv_sem=f_recv.at[pp],
            device_id={"tp": o},
            device_id_type=MESH,
        )

    forward(me).start()

    def pass_on(d, pp):
        p_copy(1, disp.at[pp], xrow.at[t, pp], d, pp, pp).wait_recv()
        forward(pp).start()

    over_plane(pass_on)
    for load in loads:
        load.wait()
    mine = xrow[t].reshape(PLANE * ROWS, HALF)
    gate_act = jnp.dot(mine, gate_v[t], preferred_element_type=jnp.float32)
    up_act = jnp.dot(mine, up_v[t], preferred_element_type=jnp.float32)
    over = lax.fori_loop(0, PLANE, lambda i, c: (arrival(i).wait_recv(), c)[1], 0)
    other = xrow[o].reshape(PLANE * ROWS, HALF)
    gate_act = gate_act + jnp.dot(other, gate_v[o], preferred_element_type=jnp.float32)
    up_act = up_act + jnp.dot(other, up_v[o], preferred_element_type=jnp.float32)
    act = (gate_act * (1.0 / (1.0 + jnp.exp(-gate_act))) * up_act).astype(jnp.bfloat16)
    o_out[...] = jnp.dot(act, down_v[o], preferred_element_type=jnp.float32).astype(jnp.bfloat16)
    give_o = t_copy(2, o_out, o_in)
    give_o.start()
    own = jnp.dot(act, down_v[t], preferred_element_type=jnp.float32).astype(jnp.bfloat16)
    give_o.wait_recv()
    both = own.astype(jnp.float32) + o_in[...].astype(jnp.float32)
    ret[...] = both.astype(jnp.bfloat16).reshape(PLANE, ROWS, HALF)
    over_plane(lambda d, pp: p_copy(2, ret.at[pp], back.at[me], d, pp, me).start())
    back[me] = ret[me]
    over_plane(lambda d, pp: p_copy(2, ret.at[pp], back.at[pp], d, pp, pp).wait_recv())

    outs = back[...].reshape(PLANE * ROWS, HALF)
    total = jnp.dot(combine_high, outs, preferred_element_type=jnp.float32)
    total = total + jnp.dot(combine_low, outs, preferred_element_type=jnp.float32)
    psum[...] = total.astype(jnp.bfloat16).reshape(NZ, ROWS, HALF)
    over_z(lambda d, zz: z_copy(4, psum.at[zz], tsum.at[z], d, zz, z).start())
    tsum[z] = psum[z]
    over_z(lambda d, zz: z_copy(4, psum.at[zz], tsum.at[zz], d, zz, zz).wait_recv())
    mix = jnp.sum(tsum[...].astype(jnp.float32), axis=0)
    my_rows = pl.ds(pl.multiple_of(z * ROWS, ROWS), ROWS)
    for zz in range(NZ):
        upd[:, zz * 128 : (zz + 1) * 128] = (
            res[zz, my_rows, :] + mix[:, zz * 128 : (zz + 1) * 128]
        ).astype(jnp.bfloat16)
    give_u = t_copy(3, upd, upd_in)
    give_u.start()
    for zz in range(NZ):
        out_ref[:, pl.ds(pl.multiple_of(zz * 256 + t * 128, 128), 128)] = upd[:, zz * 128 : (zz + 1) * 128]
    give_u.wait_recv()
    for zz in range(NZ):
        out_ref[:, pl.ds(pl.multiple_of(zz * 256 + o * 128, 128), 128)] = upd_in[:, zz * 128 : (zz + 1) * 128]

    over_z(lambda d, zz: z_copy(0, att_ref, aall.at[z], d, zz, z).wait_send())
    over_z(lambda d, zz: z_copy(1, info_ref, infoall.at[z], d, zz, z).wait_send())
    over_z(lambda d, zz: z_copy(2, hsub, hall.at[z], d, zz, z).wait_send())
    over_z(lambda d, zz: z_copy(3, mixed.at[z], mixed.at[z], d, zz, z).wait_send())
    over_z(lambda d, zz: z_copy(4, psum.at[zz], tsum.at[z], d, zz, z).wait_send())
    over_plane(lambda d, pp: p_copy(0, wo_ref.at[:, my_columns], wall.at[me], d, pp, me).wait_send())
    over_plane(lambda d, pp: p_copy(1, disp.at[pp], xrow.at[t, me], d, pp, me).wait_send())
    over_plane(lambda d, pp: p_copy(2, ret.at[pp], back.at[me], d, pp, me).wait_send())
    lax.fori_loop(0, PLANE, lambda i, c: (forward(i).wait_send(), c)[1], 0)
    for give_one in (give, give_sq, give_o, give_u):
        give_one.wait_send()


def after_attention(attended, hidden, out_weight, ffn_gain, info, gate_weights, up_weights, down_weights):
    bf16, f32 = jnp.bfloat16, jnp.float32
    tokens = NZ * ROWS
    vmem = pl.BlockSpec(memory_space=pltpu.VMEM)
    hbm = pl.BlockSpec(memory_space=pl.ANY)
    return pl.pallas_call(
        layer_kernel,
        out_shape=jax.ShapeDtypeStruct(hidden.shape, bf16),
        in_specs=[vmem] * 5 + [hbm] * 3,
        out_specs=vmem,
        scratch_shapes=[
            pltpu.VMEM((ROWS, HALF), bf16),
            pltpu.VMEM((NZ, ROWS, HALF), bf16),
            pltpu.VMEM((NZ, 16, 128), f32),
            pltpu.VMEM((PLANE, ROWS, HALF), bf16),
            pltpu.VMEM((NZ, ROWS, HALF), bf16),
            pltpu.VMEM((2, tokens, 128), f32),
            pltpu.VMEM((tokens, 128), f32),
            pltpu.VMEM((NZ, tokens, 128), bf16),
            pltpu.VMEM((NZ, tokens, 128), f32),
            pltpu.VMEM((tokens, 128), f32),
            pltpu.VMEM((tokens, 128), f32),
            pltpu.VMEM((PLANE, ROWS, HALF), bf16),
            pltpu.VMEM((2, PLANE, ROWS, HALF), bf16),
            pltpu.VMEM((2, HALF, 256), bf16),
            pltpu.VMEM((2, HALF, 256), bf16),
            pltpu.VMEM((2, 256, HALF), bf16),
            pltpu.VMEM((PLANE * ROWS, HALF), bf16),
            pltpu.VMEM((PLANE * ROWS, HALF), bf16),
            pltpu.VMEM((PLANE, ROWS, HALF), bf16),
            pltpu.VMEM((PLANE, ROWS, HALF), bf16),
            pltpu.VMEM((NZ, ROWS, HALF), bf16),
            pltpu.VMEM((NZ, ROWS, HALF), bf16),
            pltpu.VMEM((ROWS, HALF), bf16),
            pltpu.VMEM((ROWS, HALF), bf16),
            pltpu.SemaphoreType.DMA((5, NZ)),
            pltpu.SemaphoreType.DMA((5, NZ)),
            pltpu.SemaphoreType.DMA((3, PLANE)),
            pltpu.SemaphoreType.DMA((3, PLANE)),
            pltpu.SemaphoreType.DMA((PLANE,)),
            pltpu.SemaphoreType.DMA((PLANE,)),
            pltpu.SemaphoreType.DMA((4,)),
            pltpu.SemaphoreType.DMA((4,)),
            pltpu.SemaphoreType.DMA((3, 16)),
        ],
        compiler_params=pltpu.CompilerParams(
            collective_id=0, has_side_effects=True, vmem_limit_bytes=56 * 1024 * 1024
        ),
    )(attended, hidden, out_weight, ffn_gain, info, gate_weights, up_weights, down_weights)


def per_device(
    hidden,
    attn_gain,
    query_weight,
    key_weight,
    value_weight,
    forget_weight,
    forget_bias,
    cache_keys,
    cache_values,
    cache_logsum,
    lengths,
    out_weight,
    ffn_gain,
    expert_ids,
    expert_scores,
    gate_weights,
    up_weights,
    down_weights,
):
    rows_here = hidden.shape[0]
    query_heads = query_weight.shape[1] // HD
    key_heads = key_weight.shape[1] // HD
    group_size = query_heads // key_heads
    cache_len = cache_keys.shape[-1]
    score_scale = HD ** (-0.5)
    normed = root_norm(hidden, attn_gain).astype(jnp.bfloat16)
    queries = jnp.dot(normed, query_weight, preferred_element_type=jnp.float32).astype(jnp.bfloat16)
    key_new = (
        jnp.dot(normed, key_weight, preferred_element_type=jnp.float32)
        .astype(jnp.bfloat16)
        .reshape(rows_here, key_heads, HD)
    )
    value_new = (
        jnp.dot(normed, value_weight, preferred_element_type=jnp.float32)
        .astype(jnp.bfloat16)
        .reshape(rows_here, key_heads, HD)
    )
    log_forget = jax.nn.log_sigmoid(
        jnp.dot(normed, forget_weight, preferred_element_type=jnp.float32) + forget_bias
    )
    positions = jnp.arange(cache_len, dtype=jnp.int32)
    is_last = positions[None, :] == (lengths - 1)[:, None]
    new_logsum = jnp.sum(jnp.where(is_last[:, None, :], cache_logsum, 0.0), axis=-1) + log_forget
    grouped = queries.reshape(rows_here, key_heads, group_size, HD)
    scores = jnp.einsum("sgjd,sgdp->sgjp", grouped, cache_keys, preferred_element_type=jnp.float32)
    scores = scores.reshape(rows_here, query_heads, cache_len) * score_scale
    scores = scores + new_logsum[:, :, None] - cache_logsum
    is_live = positions[None, :] < lengths[:, None]
    scores = jnp.where(is_live[:, None, :], scores, -jnp.inf)
    own_score = (
        jnp.einsum("sgjd,sgd->sgj", grouped, key_new, preferred_element_type=jnp.float32).reshape(
            rows_here, query_heads
        )
        * score_scale
    )
    top_score = jnp.maximum(jnp.max(scores, axis=-1), own_score)
    past_exp = jnp.exp(scores - top_score[:, :, None])
    own_exp = jnp.exp(own_score - top_score)
    denominator = jnp.sum(past_exp, axis=-1) + own_exp
    past_weight = (past_exp / denominator[:, :, None]).astype(jnp.bfloat16)
    own_weight = (own_exp / denominator).astype(jnp.bfloat16)
    attended = jnp.einsum(
        "sgjp,sgdp->sgjd",
        past_weight.reshape(rows_here, key_heads, group_size, cache_len),
        cache_values,
        preferred_element_type=jnp.float32,
    )
    attended = (
        attended
        + own_weight.astype(jnp.float32).reshape(rows_here, key_heads, group_size)[:, :, :, None]
        * value_new.astype(jnp.float32)[:, :, None, :]
    )
    attended = attended.reshape(rows_here, query_heads * HD).astype(jnp.bfloat16)
    route_weight = expert_scores / jnp.sum(expert_scores, axis=-1, keepdims=True)
    facts = jnp.zeros((16, rows_here), jnp.float32)
    facts = facts.at[:TOP_K].set(expert_ids.astype(jnp.float32).T).at[8 : 8 + TOP_K].set(route_weight.T)
    lanes = jnp.arange(NZ * ROWS, dtype=jnp.int32) // ROWS
    info = jnp.where(lanes[None, :] == lax.axis_index("ep_0"), jnp.tile(facts, (1, NZ)), 0.0)
    gain = ffn_gain.astype(jnp.float32).reshape(16, 128)
    updated = after_attention(
        attended, hidden, out_weight, gain, info, gate_weights, up_weights, down_weights
    )
    return (updated, key_new, value_new, new_logsum)


def solution(mesh):
    split = Mesh(mesh.devices.reshape(8, 4, 4, mesh.shape["tp"]), ("ep_0", "ep_1", "ep_2", "tp"))
    in_specs = (
        P(EP, None),
        P(),
        P(None, "tp"),
        P(None, "tp"),
        P(None, "tp"),
        P(None, "tp"),
        P("tp"),
        P(EP, "tp", None, None),
        P(EP, "tp", None, None),
        P(EP, "tp", None),
        P(EP),
        P(EP, None),
        P(),
        P(EP, None),
        P(EP, None),
        P(EP, None, "tp"),
        P(EP, None, "tp"),
        P(EP, "tp", None),
    )
    out_specs = (P(EP, None), P(EP, "tp", None), P(EP, "tp", None), P(EP, "tp"))
    return jax.shard_map(
        per_device, mesh=split, in_specs=in_specs, out_specs=out_specs, check_vma=False
    )
```

```python
import jax
import jax.numpy as jnp
from jax import lax
from jax.experimental import pallas as pl
from jax.experimental.pallas import tpu as pltpu
from jax.sharding import Mesh
from jax.sharding import PartitionSpec as P

HD = 64
TOP_K = 6
EP = ("ep_0", "ep_1", "ep_2")
NZ = 8
NX = 4
PLANE = 16
ROWS = 16
HALF = 1024
WIDE = 2048
MESH = pl.DeviceIdType.MESH

epsilon = 1e-06


def layer_kernel(
    len_ref,
    attn_gain_ref,
    ffn_gain_ref,
    bias_ref,
    ids_ref,
    scores_ref,
    hid_hbm,
    wq_hbm,
    wk_hbm,
    wv_hbm,
    wf_hbm,
    keys_hbm,
    values_hbm,
    logsum_hbm,
    wo_ref,
    gate_ref,
    up_ref,
    down_ref,
    out_ref,
    key_out,
    value_out,
    logsum_out,
    hid_ref,
    wq,
    wkvf,
    keys,
    values,
    logsum,
    normed,
    queries,
    spread,
    heads_q,
    gate_col,
    own_col,
    new_val,
    att_rows,
    att_flat,
    att_ref,
    gains,
    info_ref,
    infoall,
    wall,
    aall,
    hcol,
    part,
    part_in,
    mixed,
    rounded,
    mown,
    rall,
    sq,
    sq_in,
    disp,
    xrow,
    gate_v,
    up_v,
    down_v,
    o_out,
    o_in,
    ret,
    back,
    psum,
    tsum,
    upd,
    upd_in,
    z_send,
    z_recv,
    p_send,
    p_recv,
    f_send,
    f_recv,
    t_send,
    t_recv,
    w_sem,
    a_sem,
):
    z = lax.axis_index("ep_0")
    y = lax.axis_index("ep_1")
    x = lax.axis_index("ep_2")
    t = lax.axis_index("tp")
    me = y * NX + x
    o = 1 - t
    parity = lax.rem(z, 2)
    pair = z // 2

    def z_copy(phase, src, dst, zz, i, slot):
        return pltpu.make_async_remote_copy(
            src_ref=src,
            dst_ref=dst,
            send_sem=z_send.at[phase, i],
            recv_sem=z_recv.at[phase, slot],
            device_id={"ep_0": zz},
            device_id_type=MESH,
        )

    def p_copy(phase, src, dst, pp, i, slot):
        return pltpu.make_async_remote_copy(
            src_ref=src,
            dst_ref=dst,
            send_sem=p_send.at[phase, i],
            recv_sem=p_recv.at[phase, slot],
            device_id={"ep_1": pp // NX, "ep_2": lax.rem(pp, NX)},
            device_id_type=MESH,
        )

    def t_copy(phase, src, dst):
        return pltpu.make_async_remote_copy(
            src_ref=src,
            dst_ref=dst,
            send_sem=t_send.at[phase],
            recv_sem=t_recv.at[phase],
            device_id={"tp": o},
            device_id_type=MESH,
        )

    def over_z(fn):
        def step(d, carry):
            fn(d, lax.rem(z + d, NZ))
            return carry

        lax.fori_loop(1, NZ, step, 0)

    def over_plane(fn):
        def step(d, carry):
            fn(d, lax.rem(me + d, PLANE))
            return carry

        lax.fori_loop(1, PLANE, step, 0)

    get_hid = pltpu.make_async_copy(hid_hbm, hid_ref, a_sem.at[0])
    get_hid.start()
    get_q = []
    for i in range(4):
        rows = pl.ds(i * 512, 512)
        get_q.append(pltpu.make_async_copy(wq_hbm.at[rows, :], wq.at[rows, :], a_sem.at[1 + i]))
    get_small = [
        pltpu.make_async_copy(wk_hbm, wkvf.at[pl.ds(0, 64)], a_sem.at[5]),
        pltpu.make_async_copy(wv_hbm, wkvf.at[pl.ds(64, 64)], a_sem.at[6]),
        pltpu.make_async_copy(wf_hbm, wkvf.at[pl.ds(128, 16)], a_sem.at[7]),
    ]
    get_cache = []
    for i in range(4):
        rows = pl.ds(i * 4, 4)
        get_cache.append(
            (
                pltpu.make_async_copy(keys_hbm.at[rows, 0], keys.at[rows], a_sem.at[8 + i]),
                pltpu.make_async_copy(logsum_hbm.at[rows], logsum.at[rows], a_sem.at[12 + i]),
                pltpu.make_async_copy(values_hbm.at[rows, 0], values.at[rows], a_sem.at[16 + i]),
            )
        )
    for copy in get_q + get_small:
        copy.start()
    for group in get_cache:
        for copy in group:
            copy.start()

    barrier = pltpu.get_barrier_semaphore()
    over_z(lambda d, zz: pl.semaphore_signal(barrier, inc=1, device_id={"ep_0": zz}, device_id_type=MESH))
    over_plane(
        lambda d, pp: pl.semaphore_signal(
            barrier,
            inc=1,
            device_id={"ep_1": pp // NX, "ep_2": lax.rem(pp, NX)},
            device_id_type=MESH,
        )
    )
    pl.semaphore_signal(barrier, inc=1, device_id={"tp": o}, device_id_type=MESH)

    info_ref[...] = jnp.zeros((2, 16, 128), jnp.float32)
    shares = scores_ref[...] / jnp.sum(scores_ref[...], axis=0, keepdims=True)
    info_ref[0, 0:TOP_K, 0:ROWS] = ids_ref[...].astype(jnp.float32)
    info_ref[0, 8 : 8 + TOP_K, 0:ROWS] = shares
    facts = info_ref[0]
    info_ref[0] = pltpu.roll(facts, pair * ROWS + parity * 64, 1)
    info_ref[1] = pltpu.roll(facts, pair * ROWS + (1 - parity) * 64, 1)
    infoall[z] = info_ref[parity]
    gains[0] = attn_gain_ref[...].astype(jnp.float32).reshape(16, 128)
    gains[1] = ffn_gain_ref[...].astype(jnp.float32).reshape(16, 128)

    get_hid.wait()
    total_sq = jnp.zeros((ROWS, 128), jnp.float32)
    for i in range(16):
        block = hid_ref[:, i * 128 : (i + 1) * 128].astype(jnp.float32)
        total_sq = total_sq + block * block
    inverse = lax.rsqrt(jnp.sum(total_sq, axis=-1, keepdims=True) * (1.0 / WIDE) + epsilon)
    for i in range(16):
        block = hid_ref[:, i * 128 : (i + 1) * 128].astype(jnp.float32)
        normed[:, i * 128 : (i + 1) * 128] = (block * inverse * gains[0, i : i + 1, :]).astype(jnp.bfloat16)
    my_columns = pl.ds(pl.multiple_of(t * HALF, HALF), HALF)

    def hid_block(zz):
        return hid_ref.at[:, pl.ds(pl.multiple_of(zz * 256 + t * 128, 128), 128)]

    hcol[0, pair] = hid_block(z)[...]

    query = jnp.zeros((ROWS, HALF), jnp.float32)
    for i in range(4):
        get_q[i].wait()
        query = query + jnp.dot(
            normed[:, i * 512 : (i + 1) * 512],
            wq[i * 512 : (i + 1) * 512, :],
            preferred_element_type=jnp.float32,
        )
    queries[...] = query.astype(jnp.bfloat16).astype(jnp.float32)

    with jax.named_scope("a_barrier"):
        pl.semaphore_wait(barrier, (NZ - 1) + (PLANE - 1) + 1)
    get_wo = pltpu.make_async_copy(wo_ref.at[:, my_columns], wall.at[me], a_sem.at[20])
    get_wo.start()

    def send_wo(d, pp):
        return p_copy(0, wo_ref.at[:, my_columns], wall.at[me], pp, d, me)

    def send_hid(d, zz):
        return z_copy(2, hid_block(zz), hcol.at[lax.rem(d, 2), pair], zz, d, z)

    def send_info(d, zz):
        return z_copy(3, info_ref.at[lax.rem(zz, 2)], infoall.at[z], zz, d, z)

    over_plane(lambda d, pp: send_wo(d, pp).start())
    over_z(lambda d, zz: send_hid(d, zz).start())
    over_z(lambda d, zz: send_info(d, zz).start())
    loads = []
    for zz in range(NZ):
        for h in range(2):
            rows = pl.ds(zz * 256 + h * 128, 128)
            put = pl.ds(zz * 128, 128)
            n = zz * 2 + h
            loads.append(pltpu.make_async_copy(gate_ref.at[0, rows, :], gate_v.at[h, put, :], w_sem.at[0, n]))
            loads.append(pltpu.make_async_copy(up_ref.at[0, rows, :], up_v.at[h, put, :], w_sem.at[1, n]))
            loads.append(pltpu.make_async_copy(down_ref.at[0, :, rows], down_v.at[h, :, put], w_sem.at[2, n]))
    for load in loads:
        load.start()

    for copy in get_small:
        copy.wait()
    three = lax.dot_general(
        normed[...], wkvf[...], (((1,), (1,)), ((), ())), preferred_element_type=jnp.float32
    )
    new_key = three[:, 0:64].astype(jnp.bfloat16)
    new_value = three[:, 64:128].astype(jnp.bfloat16)
    key_out[...] = new_key
    value_out[...] = new_value
    own_col[...] = new_key.astype(jnp.float32)
    new_val[...] = new_value.astype(jnp.float32)
    pre = three[:, 128:144] + bias_ref[...].reshape(1, 16)
    gate_col[...] = -(jnp.maximum(-pre, 0.0) + jnp.log1p(jnp.exp(-jnp.abs(pre))))

    head_of_row = lax.broadcasted_iota(jnp.int32, (ROWS, HALF), 0)
    head_of_lane = lax.broadcasted_iota(jnp.int32, (ROWS, HALF), 1) // HD
    own_lanes = head_of_row == head_of_lane
    for s in range(ROWS):
        spread[s * 16 : (s + 1) * 16, :] = jnp.where(
            own_lanes, jnp.broadcast_to(queries[s : s + 1, :], (16, HALF)), 0.0
        ).astype(jnp.bfloat16)
    fold = jnp.where(
        lax.rem(lax.broadcasted_iota(jnp.int32, (HALF, HD), 0), HD)
        == lax.broadcasted_iota(jnp.int32, (HALF, HD), 1),
        1.0,
        0.0,
    ).astype(jnp.bfloat16)
    heads_q[...] = jnp.dot(spread[...], fold, preferred_element_type=jnp.float32).astype(jnp.bfloat16)

    position = lax.broadcasted_iota(jnp.int32, (16, 1024), 1)
    diagonal = lax.broadcasted_iota(jnp.int32, (16, 16), 0) == lax.broadcasted_iota(jnp.int32, (16, 16), 1)
    score_scale = HD ** (-0.5)

    def send_att(piece, d, zz):
        rows = pl.ds(piece * 8, 8)
        return z_copy(piece, att_ref.at[rows], aall.at[lax.rem(d, 2), pair, rows], zz, d, z)

    for s in range(ROWS):
        if s % 4 == 0:
            for copy in get_cache[s // 4]:
                copy.wait()
        rows = slice(s * 16, (s + 1) * 16)
        q_s = heads_q[rows, :]
        scores = jnp.dot(q_s, keys[s], preferred_element_type=jnp.float32) * score_scale
        length = len_ref[s]
        sums = logsum[s]
        last = jnp.sum(jnp.where(position == length - 1, sums, 0.0), axis=-1, keepdims=True)
        forget = jnp.sum(
            jnp.where(diagonal, jnp.broadcast_to(gate_col[s : s + 1, :], (16, 16)), 0.0), axis=-1, keepdims=True
        )
        new_sum = last + forget
        logsum_out[s : s + 1, :] = jnp.sum(
            jnp.where(diagonal, jnp.broadcast_to(new_sum, (16, 16)), 0.0), axis=0, keepdims=True
        )
        scores = jnp.where(position < length, scores + new_sum - sums, -jnp.inf)
        own_score = (
            jnp.sum(q_s.astype(jnp.float32) * own_col[s : s + 1, :], axis=-1, keepdims=True) * score_scale
        )
        top = jnp.maximum(jnp.max(scores, axis=-1, keepdims=True), own_score)
        past = jnp.exp(scores - top)
        own_exp = jnp.exp(own_score - top)
        share = 1.0 / (jnp.sum(past, axis=-1, keepdims=True) + own_exp)
        past_weight = (past * share).astype(jnp.bfloat16)
        own_weight = (own_exp * share).astype(jnp.bfloat16).astype(jnp.float32)
        attended = lax.dot_general(
            past_weight, values[s], (((1,), (1,)), ((), ())), preferred_element_type=jnp.float32
        )
        att_rows[rows, :] = (attended + own_weight * new_val[s : s + 1, :]).astype(jnp.bfloat16)
        if s % 8 == 7:
            piece = s // 8
            wide = lax.dot_general(
                att_rows[piece * 128 : (piece + 1) * 128, :],
                fold,
                (((1,), (1,)), ((), ())),
                preferred_element_type=jnp.float32,
            )
            for i in range(8):
                att_flat[i : i + 1, :] = jnp.sum(
                    jnp.where(own_lanes, wide[i * 16 : (i + 1) * 16, :], 0.0), axis=0, keepdims=True
                )
            att_ref[piece * 8 : (piece + 1) * 8, :] = att_flat[...].astype(jnp.bfloat16)
            over_z(lambda d, zz, piece=piece: send_att(piece, d, zz).start())
    aall[0, pair] = att_ref[...]

    with jax.named_scope("d_info"):
        over_z(lambda d, zz: z_copy(3, info_ref.at[0], infoall.at[zz], zz, d, zz).wait_recv())
    info = jnp.sum(infoall[...], axis=0)
    row = lax.broadcasted_iota(jnp.int32, (256, 128), 0)
    token = lax.broadcasted_iota(jnp.int32, (256, 128), 1)
    expert = (lax.rem(row, 128) // 8 + z * PLANE).astype(jnp.float32)
    named = jnp.zeros((256, 128), jnp.float32)
    scale = jnp.zeros((256, 128), jnp.float32)
    for j in range(TOP_K):
        hit = info[j : j + 1, :] == expert
        named = named + jnp.where(hit, 1.0, 0.0)
        scale = scale + jnp.where(hit, info[8 + j : 9 + j, :], 0.0)
    first = lax.broadcasted_iota(jnp.int32, (128, 128), 0)
    second = lax.broadcasted_iota(jnp.int32, (128, 128), 1)
    ahead = jnp.where((first // ROWS == second // ROWS) & (first < second), 1.0, 0.0).astype(jnp.bfloat16)
    rank = jnp.dot(named.astype(jnp.bfloat16), ahead, preferred_element_type=jnp.float32)
    slot = lax.rem(row, 2).astype(jnp.float32)
    here = (row // 128) * 4 + lax.rem(row, 8) // 2 == token // ROWS
    pick = jnp.where(here & (rank == slot), named, 0.0)
    combine = jnp.transpose(pick * scale)
    picks = [pick[0:128, 0:64].astype(jnp.bfloat16), pick[128:256, 64:128].astype(jnp.bfloat16)]
    combine_high, combine_low = [], []
    for j in range(2):
        part_of = combine[j * 64 : (j + 1) * 64, j * 128 : (j + 1) * 128]
        combine_high.append(part_of.astype(jnp.bfloat16))
        combine_low.append((part_of - combine_high[j].astype(jnp.float32)).astype(jnp.bfloat16))

    get_wo.wait()
    with jax.named_scope("b_w"):
        over_plane(lambda d, pp: p_copy(0, wo_ref.at[:, my_columns], wall.at[pp], pp, d, pp).wait_recv())
    with jax.named_scope("c_att"):
        for piece in range(2):
            rows = pl.ds(piece * 8, 8)
            over_z(
                lambda d, zz, piece=piece, rows=rows: z_copy(
                    piece, att_ref.at[rows], aall.at[lax.rem(d, 2), zz // 2, rows], zz, d, zz
                ).wait_recv()
            )

    att = aall[...].reshape(NZ * ROWS, HALF)
    for h in range(2):
        weights = wall[h * 8 : (h + 1) * 8].reshape(128, HALF)
        part[h] = lax.dot_general(att, weights, (((1,), (1,)), ((), ())), preferred_element_type=jnp.float32)
    give = t_copy(0, part.at[o], part_in)
    give.start()
    with jax.named_scope("e_hid"):
        over_z(lambda d, zz: z_copy(2, hid_block(zz), hcol.at[lax.rem(d, 2), zz // 2], zz, d, zz).wait_recv())
    with jax.named_scope("e_give"):
        give.wait_recv()
    mixed_now = (part[t] + part_in[...]).astype(jnp.bfloat16)
    mixed[...] = mixed_now.reshape(2, 4, ROWS, 128)
    residual = hcol[...].reshape(NZ * ROWS, 128).astype(jnp.float32) + mixed_now.astype(jnp.float32)
    rounded[...] = residual.astype(jnp.bfloat16).reshape(2, 4, ROWS, 128)

    def send_rounded(j, d, zz):
        return z_copy(4 + j, rounded.at[lax.rem(d + j, 2)], rall.at[j, z], zz, d, z)

    def send_mixed(d, zz):
        return z_copy(6, mixed.at[lax.rem(d, 2), zz // 2], mown.at[z], zz, d, z)

    for j in range(2):
        over_z(lambda d, zz, j=j: send_rounded(j, d, zz).start())
        rall[j, z] = rounded[j]
    over_z(lambda d, zz: send_mixed(d, zz).start())
    mown[z] = mixed[0, pair]

    def send_rows(j, d, pp):
        return p_copy(1 + j, disp.at[j, pp], xrow.at[t, j, me], pp, d, me)

    def forward(j, pp):
        return pltpu.make_async_remote_copy(
            src_ref=xrow.at[t, j, pp],
            dst_ref=xrow.at[t, j, pp],
            send_sem=f_send.at[j, pp],
            recv_sem=f_recv.at[j, pp],
            device_id={"tp": o},
            device_id_type=MESH,
        )

    def arrival(j, pp):
        return pltpu.make_async_remote_copy(
            src_ref=xrow.at[o, j, pp],
            dst_ref=xrow.at[o, j, pp],
            send_sem=f_send.at[j, pp],
            recv_sem=f_recv.at[j, pp],
            device_id={"tp": o},
            device_id_type=MESH,
        )

    give_sq = [t_copy(1 + j, sq.at[j], sq_in.at[j]) for j in range(2)]
    for j in range(2):
        with jax.named_scope(f"g_mixed#j={j}"):
            over_z(lambda d, zz, j=j: z_copy(4 + j, rounded.at[0], rall.at[j, zz], zz, d, zz).wait_recv())
        squares = jnp.zeros((64, 128), jnp.float32)
        for zz in range(NZ):
            block = rall[j, zz].reshape(64, 128).astype(jnp.float32)
            squares = squares + block * block
        sq[j] = jnp.broadcast_to(jnp.sum(squares, axis=-1, keepdims=True), (64, 128))
        give_sq[j].start()
        with jax.named_scope(f"h_sq#j={j}"):
            give_sq[j].wait_recv()
        inverse = lax.rsqrt((sq[j] + sq_in[j]) * (1.0 / WIDE) + epsilon)
        for zz in range(NZ):
            gain = gains[1, pl.ds(2 * zz + t, 1), :]
            block = rall[j, zz].reshape(64, 128).astype(jnp.float32)
            block = (block * inverse * gain).astype(jnp.bfloat16)
            rows = jnp.dot(picks[j], block, preferred_element_type=jnp.float32)
            disp[j, :, :, zz * 128 : (zz + 1) * 128] = rows.astype(jnp.bfloat16).reshape(PLANE, 8, 128)
        over_plane(lambda d, pp, j=j: send_rows(j, d, pp).start())
        xrow[t, j, me] = disp[j, me]
        forward(j, me).start()

    def send_ret(j, d, pp):
        return p_copy(3 + j, ret.at[j, pp], back.at[j, me], pp, d, me)

    give_o = [t_copy(3 + j, o_out.at[j], o_in.at[j]) for j in range(2)]
    for j in range(2):

        def pass_on(d, pp, j=j):
            p_copy(1 + j, disp.at[j, pp], xrow.at[t, j, pp], pp, d, pp).wait_recv()
            forward(j, pp).start()

        with jax.named_scope(f"i_disp#j={j}"):
            over_plane(pass_on)
        if j == 0:
            for load in loads:
                load.wait()
        mine = xrow[t, j].reshape(128, HALF)
        gate_act = jnp.dot(mine, gate_v[t], preferred_element_type=jnp.float32)
        up_act = jnp.dot(mine, up_v[t], preferred_element_type=jnp.float32)
        with jax.named_scope(f"k_fwd#j={j}"):
            lax.fori_loop(0, PLANE, lambda i, c, j=j: (arrival(j, i).wait_recv(), c)[1], 0)
        other = xrow[o, j].reshape(128, HALF)
        gate_act = gate_act + jnp.dot(other, gate_v[o], preferred_element_type=jnp.float32)
        up_act = up_act + jnp.dot(other, up_v[o], preferred_element_type=jnp.float32)
        act = (gate_act * (1.0 / (1.0 + jnp.exp(-gate_act))) * up_act).astype(jnp.bfloat16)
        o_out[j] = jnp.dot(act, down_v[o], preferred_element_type=jnp.float32).astype(jnp.bfloat16)
        give_o[j].start()
        own = jnp.dot(act, down_v[t], preferred_element_type=jnp.float32).astype(jnp.bfloat16)
        with jax.named_scope(f"l_o#j={j}"):
            give_o[j].wait_recv()
        both = own.astype(jnp.float32) + o_in[j].astype(jnp.float32)
        ret[j] = both.astype(jnp.bfloat16).reshape(PLANE, 8, HALF)
        over_plane(lambda d, pp, j=j: send_ret(j, d, pp).start())
        back[j, me] = ret[j, me]

    def send_sum(j, d, zz):
        return z_copy(7, psum.at[j, zz // 2], tsum.at[z], zz, d, z)

    for j in range(2):
        with jax.named_scope(f"m_ret#j={j}"):
            over_plane(lambda d, pp, j=j: p_copy(3 + j, ret.at[j, pp], back.at[j, pp], pp, d, pp).wait_recv())
        outs = back[j].reshape(128, HALF)
        total = jnp.dot(combine_high[j], outs, preferred_element_type=jnp.float32)
        total = total + jnp.dot(combine_low[j], outs, preferred_element_type=jnp.float32)
        psum[j] = total.astype(jnp.bfloat16).reshape(4, ROWS, HALF)
        for d in range(1, NZ):
            if d % 2 == j:
                send_sum(j, d, lax.rem(z + d, NZ)).start()
        if j == 0:
            tsum[z] = psum[0, pair]
    over_z(lambda d, zz: z_copy(6, mixed.at[0, 0], mown.at[zz], zz, d, zz).wait_recv())
    with jax.named_scope("n_z"):
        over_z(lambda d, zz: z_copy(7, psum.at[0, 0], tsum.at[zz], zz, d, zz).wait_recv())
    mix = jnp.sum(tsum[...].astype(jnp.float32), axis=0)
    for zz in range(NZ):
        block = hid_block(zz)[...].astype(jnp.float32) + mown[zz].astype(jnp.float32)
        upd[:, zz * 128 : (zz + 1) * 128] = (block + mix[:, zz * 128 : (zz + 1) * 128]).astype(jnp.bfloat16)
    give_u = t_copy(5, upd, upd_in)
    give_u.start()
    for zz in range(NZ):
        out_ref[:, pl.ds(pl.multiple_of(zz * 256 + t * 128, 128), 128)] = upd[:, zz * 128 : (zz + 1) * 128]
    with jax.named_scope("o_u"):
        give_u.wait_recv()
    for zz in range(NZ):
        out_ref[:, pl.ds(pl.multiple_of(zz * 256 + o * 128, 128), 128)] = upd_in[:, zz * 128 : (zz + 1) * 128]

    with jax.named_scope("p_sends"):
        over_plane(lambda d, pp: send_wo(d, pp).wait_send())
        over_z(lambda d, zz: send_hid(d, zz).wait_send())
        over_z(lambda d, zz: send_info(d, zz).wait_send())
        over_z(lambda d, zz: send_mixed(d, zz).wait_send())
        for j in range(2):
            over_z(lambda d, zz, j=j: send_att(j, d, zz).wait_send())
            over_z(lambda d, zz, j=j: send_rounded(j, d, zz).wait_send())
            over_plane(lambda d, pp, j=j: send_rows(j, d, pp).wait_send())
            over_plane(lambda d, pp, j=j: send_ret(j, d, pp).wait_send())
            lax.fori_loop(0, PLANE, lambda i, c, j=j: (forward(j, i).wait_send(), c)[1], 0)
        over_z(lambda d, zz: send_sum(0, d, zz).wait_send())
        for give_one in [give, give_u] + give_sq + give_o:
            give_one.wait_send()


def layer(lengths, *arrays):
    bf16, f32 = jnp.bfloat16, jnp.float32
    vmem = pl.BlockSpec(memory_space=pltpu.VMEM)
    hbm = pl.BlockSpec(memory_space=pl.ANY)
    dma = pltpu.SemaphoreType.DMA
    return pl.pallas_call(
        layer_kernel,
        out_shape=(
            jax.ShapeDtypeStruct((ROWS, WIDE), bf16),
            jax.ShapeDtypeStruct((ROWS, HD), bf16),
            jax.ShapeDtypeStruct((ROWS, HD), bf16),
            jax.ShapeDtypeStruct((ROWS, 16), f32),
        ),
        in_specs=[pl.BlockSpec(memory_space=pltpu.SMEM)] + [vmem] * 5 + [hbm] * 12,
        out_specs=(vmem,) * 4,
        scratch_shapes=[
            pltpu.VMEM((ROWS, WIDE), bf16),
            pltpu.VMEM((WIDE, HALF), bf16),
            pltpu.VMEM((144, WIDE), bf16),
            pltpu.VMEM((ROWS, HD, 1024), bf16),
            pltpu.VMEM((ROWS, HD, 1024), bf16),
            pltpu.VMEM((ROWS, 16, 1024), f32),
            pltpu.VMEM((ROWS, WIDE), bf16),
            pltpu.VMEM((ROWS, HALF), f32),
            pltpu.VMEM((256, HALF), bf16),
            pltpu.VMEM((256, HD), bf16),
            pltpu.VMEM((ROWS, 16), f32),
            pltpu.VMEM((ROWS, HD), f32),
            pltpu.VMEM((ROWS, HD), f32),
            pltpu.VMEM((256, HD), bf16),
            pltpu.VMEM((8, HALF), f32),
            pltpu.VMEM((ROWS, HALF), bf16),
            pltpu.VMEM((2, 16, 128), f32),
            pltpu.VMEM((2, 16, 128), f32),
            pltpu.VMEM((NZ, 16, 128), f32),
            pltpu.VMEM((PLANE, ROWS, HALF), bf16),
            pltpu.VMEM((2, 4, ROWS, HALF), bf16),
            pltpu.VMEM((2, 4, ROWS, 128), bf16),
            pltpu.VMEM((2, NZ * ROWS, 128), f32),
            pltpu.VMEM((NZ * ROWS, 128), f32),
            pltpu.VMEM((2, 4, ROWS, 128), bf16),
            pltpu.VMEM((2, 4, ROWS, 128), bf16),
            pltpu.VMEM((NZ, ROWS, 128), bf16),
            pltpu.VMEM((2, NZ, 4, ROWS, 128), bf16),
            pltpu.VMEM((2, 64, 128), f32),
            pltpu.VMEM((2, 64, 128), f32),
            pltpu.VMEM((2, PLANE, 8, HALF), bf16),
            pltpu.VMEM((2, 2, PLANE, 8, HALF), bf16),
            pltpu.VMEM((2, HALF, 256), bf16),
            pltpu.VMEM((2, HALF, 256), bf16),
            pltpu.VMEM((2, 256, HALF), bf16),
            pltpu.VMEM((2, 128, HALF), bf16),
            pltpu.VMEM((2, 128, HALF), bf16),
            pltpu.VMEM((2, PLANE, 8, HALF), bf16),
            pltpu.VMEM((2, PLANE, 8, HALF), bf16),
            pltpu.VMEM((2, 4, ROWS, HALF), bf16),
            pltpu.VMEM((NZ, ROWS, HALF), bf16),
            pltpu.VMEM((ROWS, HALF), bf16),
            pltpu.VMEM((ROWS, HALF), bf16),
            dma((8, NZ)),
            dma((8, NZ)),
            dma((5, PLANE)),
            dma((5, PLANE)),
            dma((2, PLANE)),
            dma((2, PLANE)),
            dma((6,)),
            dma((6,)),
            dma((3, 16)),
            dma((21,)),
        ],
        compiler_params=pltpu.CompilerParams(
            collective_id=0, has_side_effects=True, vmem_limit_bytes=56 * 1024 * 1024
        ),
    )(lengths, *arrays)


def hand_over(*refs):
    for source, target in zip(refs[:4], refs[4:]):
        target[...] = source[...]


def write_out(*results):
    vmem = pl.BlockSpec(memory_space=pltpu.VMEM)
    return pl.pallas_call(
        hand_over,
        out_shape=tuple(jax.ShapeDtypeStruct(r.shape, r.dtype) for r in results),
        in_specs=[vmem] * 4,
        out_specs=(vmem,) * 4,
    )(*results)


def per_device(
    hidden,
    attn_gain,
    query_weight,
    key_weight,
    value_weight,
    forget_weight,
    forget_bias,
    cache_keys,
    cache_values,
    cache_logsum,
    lengths,
    out_weight,
    ffn_gain,
    expert_ids,
    expert_scores,
    gate_weights,
    up_weights,
    down_weights,
):
    results = layer(
        lengths,
        attn_gain,
        ffn_gain,
        forget_bias,
        expert_ids.T,
        expert_scores.T,
        hidden,
        query_weight,
        key_weight.T,
        value_weight.T,
        forget_weight.T,
        cache_keys,
        cache_values,
        cache_logsum,
        out_weight,
        gate_weights,
        up_weights,
        down_weights,
    )
    updated, key_new, value_new, new_logsum = write_out(*results)
    return (updated, key_new[:, None, :], value_new[:, None, :], new_logsum)


def solution(mesh):
    split = Mesh(mesh.devices.reshape(8, 4, 4, mesh.shape["tp"]), ("ep_0", "ep_1", "ep_2", "tp"))
    in_specs = (
        P(EP, None),
        P(),
        P(None, "tp"),
        P(None, "tp"),
        P(None, "tp"),
        P(None, "tp"),
        P("tp"),
        P(EP, "tp", None, None),
        P(EP, "tp", None, None),
        P(EP, "tp", None),
        P(EP),
        P(EP, None),
        P(),
        P(EP, None),
        P(EP, None),
        P(EP, None, "tp"),
        P(EP, None, "tp"),
        P(EP, "tp", None),
    )
    out_specs = (P(EP, None), P(EP, "tp", None), P(EP, "tp", None), P(EP, "tp"))
    return jax.shard_map(
        per_device, mesh=split, in_specs=in_specs, out_specs=out_specs, check_vma=False
    )
```

```python
import jax
import jax.numpy as jnp
from jax import lax
from jax.experimental import pallas as pl
from jax.experimental.pallas import tpu as pltpu
from jax.sharding import Mesh
from jax.sharding import PartitionSpec as P

HD = 64
TOP_K = 6
EP = ("ep_0", "ep_1", "ep_2")
NZ = 8
NX = 4
PLANE = 16
ROWS = 16
HALF = 1024
WIDE = 2048
MESH = pl.DeviceIdType.MESH

epsilon = 1e-06


def layer_kernel(
    len_ref,
    attn_gain_ref,
    ffn_gain_ref,
    bias_ref,
    ids_ref,
    scores_ref,
    hid_hbm,
    wq_hbm,
    wk_hbm,
    wv_hbm,
    wf_hbm,
    keys_hbm,
    values_hbm,
    logsum_hbm,
    wo_ref,
    gate_ref,
    up_ref,
    down_ref,
    out_ref,
    key_out,
    value_out,
    logsum_out,
    hid_ref,
    wq,
    wkvf,
    keys,
    values,
    logsum,
    normed,
    queries,
    spread,
    heads_q,
    gate_col,
    own_col,
    new_val,
    att_rows,
    att_flat,
    att_ref,
    gains,
    info_ref,
    infoall,
    wall,
    aall,
    hcol,
    part,
    part_in,
    mixed,
    rounded,
    mown,
    rall,
    ss,
    ssall,
    disp,
    xrow,
    gate_v,
    up_v,
    down_v,
    o_out,
    o_in,
    ret,
    back,
    psum,
    tsum,
    upd,
    upd_in,
    z_send,
    z_recv,
    p_send,
    p_recv,
    f_send,
    f_recv,
    t_send,
    t_recv,
    w_sem,
    a_sem,
):
    z = lax.axis_index("ep_0")
    y = lax.axis_index("ep_1")
    x = lax.axis_index("ep_2")
    t = lax.axis_index("tp")
    me = y * NX + x
    o = 1 - t
    parity = lax.rem(z, 2)
    pair = z // 2

    def z_copy(phase, src, dst, zz):
        return pltpu.make_async_remote_copy(
            src_ref=src,
            dst_ref=dst,
            send_sem=z_send.at[phase],
            recv_sem=z_recv.at[phase],
            device_id={"ep_0": zz},
            device_id_type=MESH,
        )

    def p_copy(phase, src, dst, pp, arrive):
        return pltpu.make_async_remote_copy(
            src_ref=src,
            dst_ref=dst,
            send_sem=p_send.at[phase],
            recv_sem=p_recv.at[arrive],
            device_id={"ep_1": pp // NX, "ep_2": lax.rem(pp, NX)},
            device_id_type=MESH,
        )

    def t_copy(phase, src, dst):
        return pltpu.make_async_remote_copy(
            src_ref=src,
            dst_ref=dst,
            send_sem=t_send.at[phase],
            recv_sem=t_recv.at[phase],
            device_id={"tp": o},
            device_id_type=MESH,
        )

    z_steps = (4, 3, 5, 2, 6, 1, 7)
    p_steps = sorted(
        ((dy, dx) for dy in range(4) for dx in range(4) if dy or dx),
        key=lambda d: -(min(d[0], 4 - d[0]) + min(d[1], 4 - d[1])),
    )

    def over_z(fn):
        for d in z_steps:
            fn(d, lax.rem(z + d, NZ))

    def over_plane(fn):
        for i, (dy, dx) in enumerate(p_steps):
            fn(i, lax.rem(y + dy, 4) * NX + lax.rem(x + dx, 4))

    def source(i):
        dy, dx = p_steps[i]
        return lax.rem(y + 4 - dy, 4) * NX + lax.rem(x + 4 - dx, 4)

    def z_wait(phase, ref):
        z_copy(phase, ref, ref, lax.rem(z + 1, NZ)).wait_recv()

    def p_wait(arrive, ref):
        p_copy(0, ref, ref, lax.rem(me + 1, PLANE), arrive).wait_recv()

    get_hid = pltpu.make_async_copy(hid_hbm, hid_ref, a_sem.at[0])
    get_hid.start()
    get_q = []
    for i in range(4):
        rows = pl.ds(i * 512, 512)
        get_q.append(pltpu.make_async_copy(wq_hbm.at[rows, :], wq.at[rows, :], a_sem.at[1 + i]))
    get_small = [
        pltpu.make_async_copy(wk_hbm, wkvf.at[pl.ds(0, 64)], a_sem.at[5]),
        pltpu.make_async_copy(wv_hbm, wkvf.at[pl.ds(64, 64)], a_sem.at[6]),
        pltpu.make_async_copy(wf_hbm, wkvf.at[pl.ds(128, 16)], a_sem.at[7]),
    ]
    get_cache = []
    for i in range(4):
        rows = pl.ds(i * 4, 4)
        get_cache.append(
            (
                pltpu.make_async_copy(keys_hbm.at[rows, 0], keys.at[rows], a_sem.at[8 + i]),
                pltpu.make_async_copy(logsum_hbm.at[rows], logsum.at[rows], a_sem.at[12 + i]),
                pltpu.make_async_copy(values_hbm.at[rows, 0], values.at[rows], a_sem.at[16 + i]),
            )
        )
    for copy in get_q + get_small:
        copy.start()
    for group in get_cache:
        for copy in group:
            copy.start()

    barrier = pltpu.get_barrier_semaphore()
    over_z(lambda d, zz: pl.semaphore_signal(barrier, inc=1, device_id={"ep_0": zz}, device_id_type=MESH))
    over_plane(
        lambda d, pp: pl.semaphore_signal(
            barrier,
            inc=1,
            device_id={"ep_1": pp // NX, "ep_2": lax.rem(pp, NX)},
            device_id_type=MESH,
        )
    )
    pl.semaphore_signal(barrier, inc=1, device_id={"tp": o}, device_id_type=MESH)

    info_ref[...] = jnp.zeros((2, 16, 128), jnp.float32)
    shares = scores_ref[...] / jnp.sum(scores_ref[...], axis=0, keepdims=True)
    info_ref[0, 0:TOP_K, 0:ROWS] = ids_ref[...].astype(jnp.float32)
    info_ref[0, 8 : 8 + TOP_K, 0:ROWS] = shares
    facts = info_ref[0]
    info_ref[0] = pltpu.roll(facts, pair * ROWS + parity * 64, 1)
    info_ref[1] = pltpu.roll(facts, pair * ROWS + (1 - parity) * 64, 1)
    infoall[z] = info_ref[parity]
    gains[0] = attn_gain_ref[...].astype(jnp.float32).reshape(16, 128)
    gains[1] = ffn_gain_ref[...].astype(jnp.float32).reshape(16, 128)

    get_hid.wait()
    total_sq = jnp.zeros((ROWS, 128), jnp.float32)
    for i in range(16):
        block = hid_ref[:, i * 128 : (i + 1) * 128].astype(jnp.float32)
        total_sq = total_sq + block * block
    inverse = lax.rsqrt(jnp.sum(total_sq, axis=-1, keepdims=True) * (1.0 / WIDE) + epsilon)
    for i in range(16):
        block = hid_ref[:, i * 128 : (i + 1) * 128].astype(jnp.float32)
        normed[:, i * 128 : (i + 1) * 128] = (block * inverse * gains[0, i : i + 1, :]).astype(jnp.bfloat16)
    my_columns = pl.ds(pl.multiple_of(t * HALF, HALF), HALF)

    def hid_block(zz):
        return hid_ref.at[:, pl.ds(pl.multiple_of(zz * 256 + t * 128, 128), 128)]

    def hid_cols(zz):
        return hid_ref.at[:, pl.ds(pl.multiple_of(zz * 256, 256), 256)]

    hcol[pair] = hid_cols(z)[...]

    query = jnp.zeros((ROWS, HALF), jnp.float32)
    for i in range(4):
        get_q[i].wait()
        query = query + jnp.dot(
            normed[:, i * 512 : (i + 1) * 512],
            wq[i * 512 : (i + 1) * 512, :],
            preferred_element_type=jnp.float32,
        )
    queries[...] = query.astype(jnp.bfloat16).astype(jnp.float32)

    get_wo = pltpu.make_async_copy(wo_ref.at[:, my_columns], wall.at[me], a_sem.at[20])
    get_wo.start()
    loads = []
    for zz in range(NZ):
        for h in range(2):
            rows = pl.ds(zz * 256 + h * 128, 128)
            put = pl.ds(zz * 128, 128)
            n = zz * 2 + h
            loads.append(pltpu.make_async_copy(gate_ref.at[0, rows, :], gate_v.at[h, put, :], w_sem.at[0]))
            loads.append(pltpu.make_async_copy(up_ref.at[0, rows, :], up_v.at[h, put, :], w_sem.at[1]))
            loads.append(pltpu.make_async_copy(down_ref.at[0, :, rows], down_v.at[h, :, put], w_sem.at[2]))

    def send_wo(i, pp):
        return p_copy(0, wo_ref.at[:, my_columns], wall.at[me], pp, 0)

    def send_hid(d, zz):
        return z_copy(2, hid_cols(zz), hcol.at[(d % 2) * 4 + pair], zz)

    def send_info(d, zz):
        return z_copy(3, info_ref.at[lax.rem(zz, 2)], infoall.at[z], zz)

    def greet():
        with jax.named_scope("a_barrier"):
            pl.semaphore_wait(barrier, (NZ - 1) + (PLANE - 1) + 1)
        over_plane(lambda i, pp: send_wo(i, pp).start())
        over_z(lambda d, zz: send_hid(d, zz).start())
        over_z(lambda d, zz: send_info(d, zz).start())
        for load in loads:
            load.start()

    for copy in get_small:
        copy.wait()
    three = lax.dot_general(
        normed[...], wkvf[...], (((1,), (1,)), ((), ())), preferred_element_type=jnp.float32
    )
    new_key = three[:, 0:64].astype(jnp.bfloat16)
    new_value = three[:, 64:128].astype(jnp.bfloat16)
    key_out[...] = new_key
    value_out[...] = new_value
    own_col[...] = new_key.astype(jnp.float32)
    new_val[...] = new_value.astype(jnp.float32)
    pre = three[:, 128:144] + bias_ref[...].reshape(1, 16)
    gate_col[...] = -(jnp.maximum(-pre, 0.0) + jnp.log1p(jnp.exp(-jnp.abs(pre))))

    head_of_row = lax.broadcasted_iota(jnp.int32, (ROWS, HALF), 0)
    head_of_lane = lax.broadcasted_iota(jnp.int32, (ROWS, HALF), 1) // HD
    own_lanes = head_of_row == head_of_lane
    for s in range(ROWS):
        spread[s * 16 : (s + 1) * 16, :] = jnp.where(
            own_lanes, jnp.broadcast_to(queries[s : s + 1, :], (16, HALF)), 0.0
        ).astype(jnp.bfloat16)
    fold = jnp.where(
        lax.rem(lax.broadcasted_iota(jnp.int32, (HALF, HD), 0), HD)
        == lax.broadcasted_iota(jnp.int32, (HALF, HD), 1),
        1.0,
        0.0,
    ).astype(jnp.bfloat16)
    heads_q[...] = jnp.dot(spread[...], fold, preferred_element_type=jnp.float32).astype(jnp.bfloat16)

    position = lax.broadcasted_iota(jnp.int32, (16, 1024), 1)
    diagonal = lax.broadcasted_iota(jnp.int32, (16, 16), 0) == lax.broadcasted_iota(jnp.int32, (16, 16), 1)
    score_scale = HD ** (-0.5)

    def send_att(piece, d, zz):
        rows = pl.ds(piece * 8, 8)
        return z_copy(piece, att_ref.at[rows], aall.at[(d % 2) * 4 + pair, rows], zz)

    for s in range(ROWS):
        if s == 4:
            greet()
        if s % 4 == 0:
            for copy in get_cache[s // 4]:
                copy.wait()
        rows = slice(s * 16, (s + 1) * 16)
        q_s = heads_q[rows, :]
        scores = jnp.dot(q_s, keys[s], preferred_element_type=jnp.float32) * score_scale
        length = len_ref[s]
        sums = logsum[s]
        last = jnp.sum(jnp.where(position == length - 1, sums, 0.0), axis=-1, keepdims=True)
        forget = jnp.sum(
            jnp.where(diagonal, jnp.broadcast_to(gate_col[s : s + 1, :], (16, 16)), 0.0), axis=-1, keepdims=True
        )
        new_sum = last + forget
        logsum_out[s : s + 1, :] = jnp.sum(
            jnp.where(diagonal, jnp.broadcast_to(new_sum, (16, 16)), 0.0), axis=0, keepdims=True
        )
        scores = jnp.where(position < length, scores + new_sum - sums, -jnp.inf)
        own_score = (
            jnp.sum(q_s.astype(jnp.float32) * own_col[s : s + 1, :], axis=-1, keepdims=True) * score_scale
        )
        top = jnp.maximum(jnp.max(scores, axis=-1, keepdims=True), own_score)
        past = jnp.exp(scores - top)
        own_exp = jnp.exp(own_score - top)
        share = 1.0 / (jnp.sum(past, axis=-1, keepdims=True) + own_exp)
        past_weight = (past * share).astype(jnp.bfloat16)
        own_weight = (own_exp * share).astype(jnp.bfloat16).astype(jnp.float32)
        attended = lax.dot_general(
            past_weight, values[s], (((1,), (1,)), ((), ())), preferred_element_type=jnp.float32
        )
        att_rows[rows, :] = (attended + own_weight * new_val[s : s + 1, :]).astype(jnp.bfloat16)
        if s % 8 == 7:
            piece = s // 8
            wide = lax.dot_general(
                att_rows[piece * 128 : (piece + 1) * 128, :],
                fold,
                (((1,), (1,)), ((), ())),
                preferred_element_type=jnp.float32,
            )
            for i in range(8):
                att_flat[i : i + 1, :] = jnp.sum(
                    jnp.where(own_lanes, wide[i * 16 : (i + 1) * 16, :], 0.0), axis=0, keepdims=True
                )
            att_ref[piece * 8 : (piece + 1) * 8, :] = att_flat[...].astype(jnp.bfloat16)
            over_z(lambda d, zz, piece=piece: send_att(piece, d, zz).start())
    aall[pair] = att_ref[...]

    with jax.named_scope("d_info"):
        z_wait(3, infoall.at[pl.ds(0, 7)])
    info = jnp.sum(infoall[...], axis=0)
    row = lax.broadcasted_iota(jnp.int32, (256, 128), 0)
    token = lax.broadcasted_iota(jnp.int32, (256, 128), 1)
    expert = (lax.rem(row, 128) // 8 + z * PLANE).astype(jnp.float32)
    named = jnp.zeros((256, 128), jnp.float32)
    scale = jnp.zeros((256, 128), jnp.float32)
    for j in range(TOP_K):
        hit = info[j : j + 1, :] == expert
        named = named + jnp.where(hit, 1.0, 0.0)
        scale = scale + jnp.where(hit, info[8 + j : 9 + j, :], 0.0)
    first = lax.broadcasted_iota(jnp.int32, (128, 128), 0)
    second = lax.broadcasted_iota(jnp.int32, (128, 128), 1)
    ahead = jnp.where((first // ROWS == second // ROWS) & (first < second), 1.0, 0.0).astype(jnp.bfloat16)
    rank = jnp.dot(named.astype(jnp.bfloat16), ahead, preferred_element_type=jnp.float32)
    slot = lax.rem(row, 2).astype(jnp.float32)
    here = (row // 128) * 4 + lax.rem(row, 8) // 2 == token // ROWS
    pick = jnp.where(here & (rank == slot), named, 0.0)
    combine = jnp.transpose(pick * scale)
    picks = [pick[0:128, 0:64].astype(jnp.bfloat16), pick[128:256, 64:128].astype(jnp.bfloat16)]
    combine_high, combine_low = [], []
    for j in range(2):
        part_of = combine[j * 64 : (j + 1) * 64, j * 128 : (j + 1) * 128]
        combine_high.append(part_of.astype(jnp.bfloat16))
        combine_low.append((part_of - combine_high[j].astype(jnp.float32)).astype(jnp.bfloat16))

    get_wo.wait()
    with jax.named_scope("b_w"):
        p_wait(0, wall.at[pl.ds(0, 15)])
    with jax.named_scope("c_att"):
        for piece in range(2):
            z_wait(piece, aall.at[pl.ds(0, 7), pl.ds(piece * 8, 8)])

    att = aall[...].reshape(NZ * ROWS, HALF)
    for h in range(2):
        weights = wall[h * 8 : (h + 1) * 8].reshape(128, HALF)
        part[h] = lax.dot_general(att, weights, (((1,), (1,)), ((), ())), preferred_element_type=jnp.float32)
    give = t_copy(0, part, part_in)
    give.start()
    with jax.named_scope("e_hid"):
        z_wait(2, hcol.at[pl.ds(0, 7)])
    with jax.named_scope("e_give"):
        give.wait_recv()
    squares = jnp.zeros((NZ * ROWS, 128), jnp.float32)
    for h in range(2):
        mixed_now = (part[h] + part_in[h]).astype(jnp.bfloat16)
        hid_now = hcol[:, :, h * 128 : (h + 1) * 128].reshape(NZ * ROWS, 128).astype(jnp.float32)
        residual = hid_now + mixed_now.astype(jnp.float32)
        squares = squares + residual * residual
        mixed[h] = mixed_now.reshape(8, ROWS, 128)
        rounded[h] = residual.astype(jnp.bfloat16).reshape(2, 4, ROWS, 128)

    def send_rounded(j, d, zz):
        return z_copy(4 + j, rounded.at[t, (d + j) % 2], rall.at[j, z], zz)

    def send_mixed(d, zz):
        return z_copy(6, mixed.at[t, (d % 2) * 4 + zz // 2], mown.at[z], zz)

    def send_ss(d, zz):
        return z_copy(8, ss.at[d % 2], ssall.at[z], zz)

    over_z(lambda d, zz: send_rounded(0, d, zz).start())
    sums = lax.dot_general(
        jnp.ones((8, 128), jnp.float32),
        squares,
        (((1,), (1,)), ((), ())),
        precision=lax.Precision.HIGHEST,
        preferred_element_type=jnp.float32,
    )
    ss[0] = sums
    ss[1] = pltpu.roll(sums, 64, 1)
    over_z(lambda d, zz: send_ss(d, zz).start())
    over_z(lambda d, zz: send_rounded(1, d, zz).start())
    over_z(lambda d, zz: send_mixed(d, zz).start())
    ssall[z] = ss[0]
    for j in range(2):
        rall[j, z] = rounded[t, j]
    mown[z] = mixed[t, pair]

    def send_rows(j, i, pp):
        return p_copy(1 + j, disp.at[j, pp], xrow.at[t, j, me], pp, 5 + j * 3 + i // 5)

    def forward(j, pp):
        return pltpu.make_async_remote_copy(
            src_ref=xrow.at[t, j, pp],
            dst_ref=xrow.at[t, j, pp],
            send_sem=f_send.at[j],
            recv_sem=f_recv.at[j],
            device_id={"tp": o},
            device_id_type=MESH,
        )

    def forwarded(j, ref):
        return pltpu.make_async_remote_copy(
            src_ref=ref,
            dst_ref=ref,
            send_sem=f_send.at[j],
            recv_sem=f_recv.at[j],
            device_id={"tp": o},
            device_id_type=MESH,
        )

    for j in range(2):
        with jax.named_scope(f"g_mixed#j={j}"):
            if j == 0:
                z_wait(8, ssall.at[pl.ds(0, 7)])
            z_wait(4 + j, rall.at[j, pl.ds(0, 7)])
        if j == 0:
            inverse = lax.rsqrt(jnp.sum(ssall[...], axis=0)[0:1, :] * (1.0 / WIDE) + epsilon)
            factor = jnp.sum(pick * inverse, axis=-1, keepdims=True)
        for zz in range(NZ):
            gain = gains[1, pl.ds(2 * zz + t, 1), :]
            rows = jnp.dot(picks[j], rall[j, zz].reshape(64, 128), preferred_element_type=jnp.float32)
            rows = rows * factor[j * 128 : (j + 1) * 128] * gain
            disp[j, :, :, zz * 128 : (zz + 1) * 128] = rows.astype(jnp.bfloat16).reshape(PLANE, 8, 128)
        over_plane(lambda i, pp, j=j: send_rows(j, i, pp).start())
        xrow[t, j, me] = disp[j, me]
        forward(j, me).start()

    def send_ret(j, i, pp):
        return p_copy(3 + j, ret.at[j, pp], back.at[j, me], pp, 3 + j)

    def take(j):
        with jax.named_scope(f"i_disp#j={j}"):
            for g in range(3):
                p_wait(5 + j * 3 + g, xrow.at[t, j, pl.ds(0, 5)])
                for i in range(g * 5, g * 5 + 5):
                    forward(j, source(i)).start()

    def first_half(j):
        mine = xrow[t, j].reshape(128, HALF)
        gate_act = jnp.dot(mine, gate_v[t], preferred_element_type=jnp.float32)
        return gate_act, jnp.dot(mine, up_v[t], preferred_element_type=jnp.float32)

    give_o = [t_copy(1 + j, o_out.at[j], o_in.at[j]) for j in range(2)]

    def second_half(j, gate_act, up_act):
        with jax.named_scope(f"k_fwd#j={j}"):
            forwarded(j, xrow.at[o, j]).wait_recv()
        other = xrow[o, j].reshape(128, HALF)
        gate_act = gate_act + jnp.dot(other, gate_v[o], preferred_element_type=jnp.float32)
        up_act = up_act + jnp.dot(other, up_v[o], preferred_element_type=jnp.float32)
        act = (gate_act * (1.0 / (1.0 + jnp.exp(-gate_act))) * up_act).astype(jnp.bfloat16)
        o_out[j] = jnp.dot(act, down_v[o], preferred_element_type=jnp.float32).astype(jnp.bfloat16)
        give_o[j].start()
        return jnp.dot(act, down_v[t], preferred_element_type=jnp.float32).astype(jnp.bfloat16)

    def give_back(j, own):
        with jax.named_scope(f"l_o#j={j}"):
            give_o[j].wait_recv()
        both = own.astype(jnp.float32) + o_in[j].astype(jnp.float32)
        ret[j] = both.astype(jnp.bfloat16).reshape(PLANE, 8, HALF)
        over_plane(lambda i, pp: send_ret(j, i, pp).start())
        back[j, me] = ret[j, me]

    for n, whole in enumerate((gate_v, up_v, down_v)):
        pltpu.make_async_copy(whole, whole, w_sem.at[n]).wait()
    take(0)
    own_0 = second_half(0, *first_half(0))
    take(1)
    acts = first_half(1)
    give_back(0, own_0)
    own_1 = second_half(1, *acts)
    give_back(1, own_1)

    def send_sum(j, d, zz):
        return z_copy(7, psum.at[j, zz // 2], tsum.at[z], zz)

    for j in range(2):
        with jax.named_scope(f"m_ret#j={j}"):
            p_wait(3 + j, back.at[j, pl.ds(0, 15)])
        outs = back[j].reshape(128, HALF)
        total = jnp.dot(combine_high[j], outs, preferred_element_type=jnp.float32)
        total = total + jnp.dot(combine_low[j], outs, preferred_element_type=jnp.float32)
        psum[j] = total.astype(jnp.bfloat16).reshape(4, ROWS, HALF)
        for d in z_steps:
            if d % 2 == j:
                send_sum(j, d, lax.rem(z + d, NZ)).start()
        if j == 0:
            tsum[z] = psum[0, pair]
    z_wait(6, mown.at[pl.ds(0, 7)])
    with jax.named_scope("n_z"):
        z_wait(7, tsum.at[pl.ds(0, 7)])
    mix = jnp.sum(tsum[...].astype(jnp.float32), axis=0)
    for zz in range(NZ):
        block = hid_block(zz)[...].astype(jnp.float32) + mown[zz].astype(jnp.float32)
        upd[:, zz * 128 : (zz + 1) * 128] = (block + mix[:, zz * 128 : (zz + 1) * 128]).astype(jnp.bfloat16)
    give_u = t_copy(3, upd, upd_in)
    give_u.start()
    for zz in range(NZ):
        out_ref[:, pl.ds(pl.multiple_of(zz * 256 + t * 128, 128), 128)] = upd[:, zz * 128 : (zz + 1) * 128]
    with jax.named_scope("o_u"):
        give_u.wait_recv()
    for zz in range(NZ):
        out_ref[:, pl.ds(pl.multiple_of(zz * 256 + o * 128, 128), 128)] = upd_in[:, zz * 128 : (zz + 1) * 128]

    with jax.named_scope("p_sends"):
        next_z, next_p = lax.rem(z + 1, NZ), lax.rem(me + 1, PLANE)
        sent = (
            aall.at[pl.ds(0, 7), pl.ds(0, 8)],
            aall.at[pl.ds(0, 7), pl.ds(8, 8)],
            hcol.at[pl.ds(0, 7)],
            infoall.at[pl.ds(0, 7)],
            rall.at[0, pl.ds(0, 7)],
            rall.at[1, pl.ds(0, 7)],
            mown.at[pl.ds(0, 7)],
            tsum.at[pl.ds(0, 7)],
            ssall.at[pl.ds(0, 7)],
        )
        for phase, ref in enumerate(sent):
            z_copy(phase, ref, ref, next_z).wait_send()
        sent = (
            wall.at[pl.ds(0, 15)],
            disp.at[0, pl.ds(0, 15)],
            disp.at[1, pl.ds(0, 15)],
            ret.at[0, pl.ds(0, 15)],
            ret.at[1, pl.ds(0, 15)],
        )
        for phase, ref in enumerate(sent):
            p_copy(phase, ref, ref, next_p, 0).wait_send()
        for j in range(2):
            forwarded(j, xrow.at[t, j]).wait_send()
        for give_one in [give, give_u] + give_o:
            give_one.wait_send()


def layer(lengths, *arrays):
    bf16, f32 = jnp.bfloat16, jnp.float32
    vmem = pl.BlockSpec(memory_space=pltpu.VMEM)
    hbm = pl.BlockSpec(memory_space=pltpu.HBM)
    dma = pltpu.SemaphoreType.DMA
    return pl.pallas_call(
        layer_kernel,
        out_shape=(
            pltpu.VMEM((ROWS, WIDE), bf16),
            pltpu.VMEM((ROWS, HD), bf16),
            pltpu.VMEM((ROWS, HD), bf16),
            pltpu.VMEM((ROWS, 16), f32),
        ),
        in_specs=[pl.BlockSpec(memory_space=pltpu.SMEM)] + [vmem] * 5 + [hbm] * 12,
        out_specs=(vmem,) * 4,
        scratch_shapes=[
            pltpu.VMEM((ROWS, WIDE), bf16),
            pltpu.VMEM((WIDE, HALF), bf16),
            pltpu.VMEM((144, WIDE), bf16),
            pltpu.VMEM((ROWS, HD, 1024), bf16),
            pltpu.VMEM((ROWS, HD, 1024), bf16),
            pltpu.VMEM((ROWS, 16, 1024), f32),
            pltpu.VMEM((ROWS, WIDE), bf16),
            pltpu.VMEM((ROWS, HALF), f32),
            pltpu.VMEM((256, HALF), bf16),
            pltpu.VMEM((256, HD), bf16),
            pltpu.VMEM((ROWS, 16), f32),
            pltpu.VMEM((ROWS, HD), f32),
            pltpu.VMEM((ROWS, HD), f32),
            pltpu.VMEM((256, HD), bf16),
            pltpu.VMEM((8, HALF), f32),
            pltpu.VMEM((ROWS, HALF), bf16),
            pltpu.VMEM((2, 16, 128), f32),
            pltpu.VMEM((2, 16, 128), f32),
            pltpu.VMEM((NZ, 16, 128), f32),
            pltpu.VMEM((PLANE, ROWS, HALF), bf16),
            pltpu.VMEM((8, ROWS, HALF), bf16),
            pltpu.VMEM((8, ROWS, 256), bf16),
            pltpu.VMEM((2, NZ * ROWS, 128), f32),
            pltpu.VMEM((2, NZ * ROWS, 128), f32),
            pltpu.VMEM((2, 8, ROWS, 128), bf16),
            pltpu.VMEM((2, 2, 4, ROWS, 128), bf16),
            pltpu.VMEM((NZ, ROWS, 128), bf16),
            pltpu.VMEM((2, NZ, 4, ROWS, 128), bf16),
            pltpu.VMEM((2, 8, 128), f32),
            pltpu.VMEM((NZ, 8, 128), f32),
            pltpu.VMEM((2, PLANE, 8, HALF), bf16),
            pltpu.VMEM((2, 2, PLANE, 8, HALF), bf16),
            pltpu.VMEM((2, HALF, 256), bf16),
            pltpu.VMEM((2, HALF, 256), bf16),
            pltpu.VMEM((2, 256, HALF), bf16),
            pltpu.VMEM((2, 128, HALF), bf16),
            pltpu.VMEM((2, 128, HALF), bf16),
            pltpu.VMEM((2, PLANE, 8, HALF), bf16),
            pltpu.VMEM((2, PLANE, 8, HALF), bf16),
            pltpu.VMEM((2, 4, ROWS, HALF), bf16),
            pltpu.VMEM((NZ, ROWS, HALF), bf16),
            pltpu.VMEM((ROWS, HALF), bf16),
            pltpu.VMEM((ROWS, HALF), bf16),
            dma((9,)),
            dma((9,)),
            dma((5,)),
            dma((11,)),
            dma((2,)),
            dma((2,)),
            dma((4,)),
            dma((4,)),
            dma((3,)),
            dma((21,)),
        ],
        compiler_params=pltpu.CompilerParams(
            collective_id=0, has_side_effects=True, vmem_limit_bytes=56 * 1024 * 1024
        ),
    )(lengths, *arrays)


def hand_over(*refs):
    for source, target in zip(refs[:4], refs[4:]):
        target[...] = source[...]


def write_out(*results):
    vmem = pl.BlockSpec(memory_space=pltpu.VMEM)
    return pl.pallas_call(
        hand_over,
        out_shape=tuple(jax.ShapeDtypeStruct(r.shape, r.dtype) for r in results),
        in_specs=[vmem] * 4,
        out_specs=(vmem,) * 4,
        compiler_params=pltpu.CompilerParams(vmem_limit_bytes=1024 * 1024),
    )(*results)


def per_device(
    hidden,
    attn_gain,
    query_weight,
    key_weight,
    value_weight,
    forget_weight,
    forget_bias,
    cache_keys,
    cache_values,
    cache_logsum,
    lengths,
    out_weight,
    ffn_gain,
    expert_ids,
    expert_scores,
    gate_weights,
    up_weights,
    down_weights,
):
    results = layer(
        lengths,
        attn_gain,
        ffn_gain,
        forget_bias,
        expert_ids.T,
        expert_scores.T,
        hidden,
        query_weight,
        key_weight.T,
        value_weight.T,
        forget_weight.T,
        cache_keys,
        cache_values,
        cache_logsum,
        out_weight,
        gate_weights,
        up_weights,
        down_weights,
    )
    updated, key_new, value_new, new_logsum = write_out(*results)
    return (updated, key_new[:, None, :], value_new[:, None, :], new_logsum)


def solution(mesh):
    split = Mesh(mesh.devices.reshape(8, 4, 4, mesh.shape["tp"]), ("ep_0", "ep_1", "ep_2", "tp"))
    in_specs = (
        P(EP, None),
        P(),
        P(None, "tp"),
        P(None, "tp"),
        P(None, "tp"),
        P(None, "tp"),
        P("tp"),
        P(EP, "tp", None, None),
        P(EP, "tp", None, None),
        P(EP, "tp", None),
        P(EP),
        P(EP, None),
        P(),
        P(EP, None),
        P(EP, None),
        P(EP, None, "tp"),
        P(EP, None, "tp"),
        P(EP, "tp", None),
    )
    out_specs = (P(EP, None), P(EP, "tp", None), P(EP, "tp", None), P(EP, "tp"))
    return jax.shard_map(
        per_device, mesh=split, in_specs=in_specs, out_specs=out_specs, check_vma=False
    )
```

```python
import jax
import jax.numpy as jnp
from jax import lax
from jax.experimental import pallas as pl
from jax.experimental.pallas import tpu as pltpu
from jax.sharding import Mesh
from jax.sharding import PartitionSpec as P

HD = 64
TOP_K = 6
EP = ("ep_0", "ep_1", "ep_2")
NZ = 8
NX = 4
PLANE = 16
ROWS = 16
HALF = 1024
WIDE = 2048
MESH = pl.DeviceIdType.MESH

epsilon = 1e-06


def layer_kernel(
    len_ref,
    attn_gain_ref,
    ffn_gain_ref,
    bias_ref,
    ids_ref,
    scores_ref,
    hid_hbm,
    wq_hbm,
    wk_hbm,
    wv_hbm,
    wf_hbm,
    keys_hbm,
    values_hbm,
    logsum_hbm,
    wo_ref,
    gate_ref,
    up_ref,
    down_ref,
    out_ref,
    key_out,
    value_out,
    logsum_out,
    hid_ref,
    wq,
    wkvf,
    keys,
    values,
    logsum,
    normed,
    queries,
    spread,
    heads_q,
    gate_col,
    own_col,
    new_val,
    att_rows,
    att_flat,
    att_ref,
    gains,
    info_ref,
    infoall,
    wall,
    aall,
    hcol,
    part,
    part_in,
    mixed,
    rounded,
    mown,
    rall,
    ss,
    ssall,
    disp,
    xrow,
    gate_v,
    up_v,
    down_v,
    gate_p,
    up_p,
    down_p,
    ret,
    back,
    psum,
    tsum,
    upd,
    upd_in,
    z_send,
    z_recv,
    p_send,
    p_recv,
    t_send,
    t_recv,
    w_sem,
    a_sem,
):
    z = lax.axis_index("ep_0")
    y = lax.axis_index("ep_1")
    x = lax.axis_index("ep_2")
    t = lax.axis_index("tp")
    me = y * NX + x
    o = 1 - t
    parity = lax.rem(z, 2)
    pair = z // 2

    def z_copy(phase, src, dst, zz):
        return pltpu.make_async_remote_copy(
            src_ref=src,
            dst_ref=dst,
            send_sem=z_send.at[phase],
            recv_sem=z_recv.at[phase],
            device_id={"ep_0": zz},
            device_id_type=MESH,
        )

    def p_copy(phase, src, dst, pp, arrive, core):
        return pltpu.make_async_remote_copy(
            src_ref=src,
            dst_ref=dst,
            send_sem=p_send.at[phase],
            recv_sem=p_recv.at[arrive],
            device_id={"ep_1": pp // NX, "ep_2": lax.rem(pp, NX), "tp": core},
            device_id_type=MESH,
        )

    def t_copy(phase, src, dst):
        return pltpu.make_async_remote_copy(
            src_ref=src,
            dst_ref=dst,
            send_sem=t_send.at[phase],
            recv_sem=t_recv.at[phase],
            device_id={"tp": o},
            device_id_type=MESH,
        )

    z_steps = (4, 3, 5, 2, 6, 1, 7)
    p_steps = sorted(
        ((dy, dx) for dy in range(4) for dx in range(4) if dy or dx),
        key=lambda d: -(min(d[0], 4 - d[0]) + min(d[1], 4 - d[1])),
    )

    def over_z(fn):
        for d in z_steps:
            fn(d, lax.rem(z + d, NZ))

    def over_plane(fn):
        for i, (dy, dx) in enumerate(p_steps):
            fn(i, lax.rem(y + dy, 4) * NX + lax.rem(x + dx, 4))

    def z_wait(phase, ref):
        z_copy(phase, ref, ref, lax.rem(z + 1, NZ)).wait_recv()

    def p_wait(arrive, ref):
        p_copy(0, ref, ref, lax.rem(me + 1, PLANE), arrive, t).wait_recv()

    get_hid = pltpu.make_async_copy(hid_hbm, hid_ref, a_sem.at[0])
    get_hid.start()
    get_q = []
    for i in range(4):
        rows = pl.ds(i * 512, 512)
        get_q.append(pltpu.make_async_copy(wq_hbm.at[rows, :], wq.at[rows, :], a_sem.at[1 + i]))
    get_small = [
        pltpu.make_async_copy(wk_hbm, wkvf.at[pl.ds(0, 64)], a_sem.at[5]),
        pltpu.make_async_copy(wv_hbm, wkvf.at[pl.ds(64, 64)], a_sem.at[6]),
        pltpu.make_async_copy(wf_hbm, wkvf.at[pl.ds(128, 16)], a_sem.at[7]),
    ]
    get_cache = []
    for i in range(4):
        rows = pl.ds(i * 4, 4)
        get_cache.append(
            (
                pltpu.make_async_copy(keys_hbm.at[rows, 0], keys.at[rows], a_sem.at[8 + i]),
                pltpu.make_async_copy(logsum_hbm.at[rows], logsum.at[rows], a_sem.at[12 + i]),
                pltpu.make_async_copy(values_hbm.at[rows, 0], values.at[rows], a_sem.at[16 + i]),
            )
        )
    for copy in get_q + get_small:
        copy.start()
    for group in get_cache:
        for copy in group:
            copy.start()

    barrier = pltpu.get_barrier_semaphore()
    over_z(lambda d, zz: pl.semaphore_signal(barrier, inc=1, device_id={"ep_0": zz}, device_id_type=MESH))
    for core in range(2):
        over_plane(
            lambda d, pp, core=core: pl.semaphore_signal(
                barrier,
                inc=1,
                device_id={"ep_1": pp // NX, "ep_2": lax.rem(pp, NX), "tp": core},
                device_id_type=MESH,
            )
        )
    pl.semaphore_signal(barrier, inc=1, device_id={"tp": o}, device_id_type=MESH)

    info_ref[...] = jnp.zeros((8, 128), jnp.float32)
    info_ref[0:TOP_K, 0:ROWS] = ids_ref[...].astype(jnp.float32)
    shares = scores_ref[...] / jnp.sum(scores_ref[...], axis=0, keepdims=True)
    info_ref[0:TOP_K, ROWS : 2 * ROWS] = shares
    infoall[z] = info_ref[...]
    gains[0] = attn_gain_ref[...].astype(jnp.float32).reshape(16, 128)
    gains[1] = ffn_gain_ref[...].astype(jnp.float32).reshape(16, 128)

    get_hid.wait()
    total_sq = jnp.zeros((ROWS, 128), jnp.float32)
    for i in range(16):
        block = hid_ref[:, i * 128 : (i + 1) * 128].astype(jnp.float32)
        total_sq = total_sq + block * block
    inverse = lax.rsqrt(jnp.sum(total_sq, axis=-1, keepdims=True) * (1.0 / WIDE) + epsilon)
    for i in range(16):
        block = hid_ref[:, i * 128 : (i + 1) * 128].astype(jnp.float32)
        normed[:, i * 128 : (i + 1) * 128] = (block * inverse * gains[0, i : i + 1, :]).astype(jnp.bfloat16)
    my_columns = pl.ds(pl.multiple_of(t * HALF, HALF), HALF)

    def hid_block(zz):
        return hid_ref.at[:, pl.ds(pl.multiple_of(zz * 256 + t * 128, 128), 128)]

    def hid_cols(zz):
        return hid_ref.at[:, pl.ds(pl.multiple_of(zz * 256, 256), 256)]

    hcol[pair] = hid_cols(z)[...]

    query = jnp.zeros((ROWS, HALF), jnp.float32)
    for i in range(4):
        get_q[i].wait()
        query = query + jnp.dot(
            normed[:, i * 512 : (i + 1) * 512],
            wq[i * 512 : (i + 1) * 512, :],
            preferred_element_type=jnp.float32,
        )
    queries[...] = query.astype(jnp.bfloat16).astype(jnp.float32)

    get_wo = pltpu.make_async_copy(wo_ref.at[:, my_columns], wall.at[me], a_sem.at[20])
    get_wo.start()
    loads = []
    for zz in range(NZ):
        for h in range(2):
            rows = pl.ds(zz * 256 + h * 128, 128)
            put = pl.ds(zz * 128, 128)
            n = zz * 2 + h
            loads.append(pltpu.make_async_copy(gate_ref.at[0, rows, :], gate_v.at[h, put, :], w_sem.at[0]))
            loads.append(pltpu.make_async_copy(up_ref.at[0, rows, :], up_v.at[h, put, :], w_sem.at[1]))
            loads.append(pltpu.make_async_copy(down_ref.at[0, :, rows], down_v.at[h, :, put], w_sem.at[2]))

    def send_wo(i, pp):
        return p_copy(0, wo_ref.at[:, my_columns], wall.at[me], pp, 0, t)

    def send_hid(d, zz):
        return z_copy(2, hid_cols(zz), hcol.at[(d % 2) * 4 + pair], zz)

    def send_info(d, zz):
        return z_copy(3, info_ref, infoall.at[z], zz)

    def greet():
        with jax.named_scope("a_barrier"):
            pl.semaphore_wait(barrier, (NZ - 1) + 2 * (PLANE - 1) + 1)
        over_plane(lambda i, pp: send_wo(i, pp).start())
        over_z(lambda d, zz: send_hid(d, zz).start())
        for load in loads:
            load.start()

    for copy in get_small:
        copy.wait()
    three = lax.dot_general(
        normed[...], wkvf[...], (((1,), (1,)), ((), ())), preferred_element_type=jnp.float32
    )
    new_key = three[:, 0:64].astype(jnp.bfloat16)
    new_value = three[:, 64:128].astype(jnp.bfloat16)
    key_out[...] = new_key
    value_out[...] = new_value
    own_col[...] = new_key.astype(jnp.float32)
    new_val[...] = new_value.astype(jnp.float32)
    pre = three[:, 128:144] + bias_ref[...].reshape(1, 16)
    gate_col[...] = -(jnp.maximum(-pre, 0.0) + jnp.log1p(jnp.exp(-jnp.abs(pre))))

    head_of_row = lax.broadcasted_iota(jnp.int32, (ROWS, HALF), 0)
    head_of_lane = lax.broadcasted_iota(jnp.int32, (ROWS, HALF), 1) // HD
    own_lanes = head_of_row == head_of_lane
    for s in range(ROWS):
        spread[s * 16 : (s + 1) * 16, :] = jnp.where(
            own_lanes, jnp.broadcast_to(queries[s : s + 1, :], (16, HALF)), 0.0
        ).astype(jnp.bfloat16)
    fold = jnp.where(
        lax.rem(lax.broadcasted_iota(jnp.int32, (HALF, HD), 0), HD)
        == lax.broadcasted_iota(jnp.int32, (HALF, HD), 1),
        1.0,
        0.0,
    ).astype(jnp.bfloat16)
    heads_q[...] = jnp.dot(spread[...], fold, preferred_element_type=jnp.float32).astype(jnp.bfloat16)

    position = lax.broadcasted_iota(jnp.int32, (16, 1024), 1)
    diagonal = lax.broadcasted_iota(jnp.int32, (16, 16), 0) == lax.broadcasted_iota(jnp.int32, (16, 16), 1)
    score_scale = HD ** (-0.5)

    def send_att(piece, d, zz):
        rows = pl.ds(piece * 8, 8)
        return z_copy(piece, att_ref.at[rows], aall.at[(d % 2) * 4 + pair, rows], zz)

    for s in range(ROWS):
        if s == 4:
            greet()
        if s % 4 == 0:
            for copy in get_cache[s // 4]:
                copy.wait()
        rows = slice(s * 16, (s + 1) * 16)
        q_s = heads_q[rows, :]
        scores = jnp.dot(q_s, keys[s], preferred_element_type=jnp.float32) * score_scale
        length = len_ref[s]
        sums = logsum[s]
        last = jnp.sum(jnp.where(position == length - 1, sums, 0.0), axis=-1, keepdims=True)
        forget = jnp.sum(
            jnp.where(diagonal, jnp.broadcast_to(gate_col[s : s + 1, :], (16, 16)), 0.0), axis=-1, keepdims=True
        )
        new_sum = last + forget
        logsum_out[s : s + 1, :] = jnp.sum(
            jnp.where(diagonal, jnp.broadcast_to(new_sum, (16, 16)), 0.0), axis=0, keepdims=True
        )
        scores = jnp.where(position < length, scores + new_sum - sums, -jnp.inf)
        own_score = (
            jnp.sum(q_s.astype(jnp.float32) * own_col[s : s + 1, :], axis=-1, keepdims=True) * score_scale
        )
        top = jnp.maximum(jnp.max(scores, axis=-1, keepdims=True), own_score)
        past = jnp.exp(scores - top)
        own_exp = jnp.exp(own_score - top)
        share = 1.0 / (jnp.sum(past, axis=-1, keepdims=True) + own_exp)
        past_weight = (past * share).astype(jnp.bfloat16)
        own_weight = (own_exp * share).astype(jnp.bfloat16).astype(jnp.float32)
        attended = lax.dot_general(
            past_weight, values[s], (((1,), (1,)), ((), ())), preferred_element_type=jnp.float32
        )
        att_rows[rows, :] = (attended + own_weight * new_val[s : s + 1, :]).astype(jnp.bfloat16)
        if s % 8 == 7:
            piece = s // 8
            wide = lax.dot_general(
                att_rows[piece * 128 : (piece + 1) * 128, :],
                fold,
                (((1,), (1,)), ((), ())),
                preferred_element_type=jnp.float32,
            )
            for i in range(8):
                att_flat[i : i + 1, :] = jnp.sum(
                    jnp.where(own_lanes, wide[i * 16 : (i + 1) * 16, :], 0.0), axis=0, keepdims=True
                )
            att_ref[piece * 8 : (piece + 1) * 8, :] = att_flat[...].astype(jnp.bfloat16)
            over_z(lambda d, zz, piece=piece: send_att(piece, d, zz).start())
    over_z(lambda d, zz: send_info(d, zz).start())
    aall[pair] = att_ref[...]
    wholes = ((gate_v, gate_p), (up_v, up_p), (down_v, down_p))
    swaps = []
    for n, (mine, theirs) in enumerate(wholes):
        pltpu.make_async_copy(mine, mine, w_sem.at[n]).wait()
        swaps.append(t_copy(2 + n, mine, theirs))
        swaps[n].start()

    get_wo.wait()
    with jax.named_scope("b_w"):
        p_wait(0, wall.at[pl.ds(0, 15)])
    with jax.named_scope("c_att"):
        for piece in range(2):
            z_wait(piece, aall.at[pl.ds(0, 7), pl.ds(piece * 8, 8)])

    att = aall[...].reshape(NZ * ROWS, HALF)
    for h in range(2):
        weights = wall[h * 8 : (h + 1) * 8].reshape(128, HALF)
        part[h] = lax.dot_general(att, weights, (((1,), (1,)), ((), ())), preferred_element_type=jnp.float32)
    give = t_copy(0, part, part_in)
    give.start()
    with jax.named_scope("e_hid"):
        z_wait(2, hcol.at[pl.ds(0, 7)])
    with jax.named_scope("e_give"):
        give.wait_recv()
    squares = jnp.zeros((NZ * ROWS, 128), jnp.float32)
    for h in range(2):
        mixed_now = (part[h] + part_in[h]).astype(jnp.bfloat16)
        hid_now = hcol[:, :, h * 128 : (h + 1) * 128].reshape(NZ * ROWS, 128).astype(jnp.float32)
        residual = hid_now + mixed_now.astype(jnp.float32)
        squares = squares + residual * residual
        mixed[h] = mixed_now.reshape(8, ROWS, 128)
        rounded[h] = residual.astype(jnp.bfloat16).reshape(2, 4, ROWS, 128)

    def send_rounded(j, d, zz):
        return z_copy(4 + j, rounded.at[t, (d + j) % 2], rall.at[j, z], zz)

    def send_mixed(d, zz):
        return z_copy(6, mixed.at[t, (d % 2) * 4 + zz // 2], mown.at[z], zz)

    def send_ss(d, zz):
        return z_copy(8, ss.at[d % 2], ssall.at[z], zz)

    over_z(lambda d, zz: send_rounded(0, d, zz).start())
    sums = lax.dot_general(
        jnp.ones((8, 128), jnp.float32),
        squares,
        (((1,), (1,)), ((), ())),
        precision=lax.Precision.HIGHEST,
        preferred_element_type=jnp.float32,
    )
    ss[0] = sums
    ss[1] = pltpu.roll(sums, 64, 1)
    over_z(lambda d, zz: send_ss(d, zz).start())
    over_z(lambda d, zz: send_rounded(1, d, zz).start())
    over_z(lambda d, zz: send_mixed(d, zz).start())
    ssall[z] = ss[0]
    for j in range(2):
        rall[j, z] = rounded[t, j]
    mown[z] = mixed[t, pair]

    with jax.named_scope("d_info"):
        z_wait(3, infoall.at[pl.ds(0, 7)])
    lane = lax.broadcasted_iota(jnp.int32, (8, 128), 1)
    routes = jnp.zeros((8, 128), jnp.float32)
    weights_of = jnp.zeros((8, 128), jnp.float32)
    for zz in range(NZ):
        tile = infoall[zz]
        place = (lax.rem(z + zz, 2) * 4 + zz // 2) * ROWS
        routes = routes + pltpu.roll(jnp.where(lane < ROWS, tile, 0.0), place, 1)
        tile = jnp.where((lane >= ROWS) & (lane < 2 * ROWS), tile, 0.0)
        weights_of = weights_of + pltpu.roll(tile, lax.rem(place + 128 - ROWS, 128), 1)
    row = lax.broadcasted_iota(jnp.int32, (256, 128), 0)
    token = lax.broadcasted_iota(jnp.int32, (256, 128), 1)
    expert = (lax.rem(row, 128) // 8 + z * PLANE).astype(jnp.float32)
    named = jnp.zeros((256, 128), jnp.float32)
    scale = jnp.zeros((256, 128), jnp.float32)
    for j in range(TOP_K):
        hit = routes[j : j + 1, :] == expert
        named = named + jnp.where(hit, 1.0, 0.0)
        scale = scale + jnp.where(hit, weights_of[j : j + 1, :], 0.0)
    first = lax.broadcasted_iota(jnp.int32, (128, 128), 0)
    second = lax.broadcasted_iota(jnp.int32, (128, 128), 1)
    ahead = jnp.where((first // ROWS == second // ROWS) & (first < second), 1.0, 0.0).astype(jnp.bfloat16)
    rank = jnp.dot(named.astype(jnp.bfloat16), ahead, preferred_element_type=jnp.float32)
    slot = lax.rem(row, 2).astype(jnp.float32)
    here = (row // 128) * 4 + lax.rem(row, 8) // 2 == token // ROWS
    pick = jnp.where(here & (rank == slot), named, 0.0)
    combine = jnp.transpose(pick * scale)
    picks = [pick[0:128, 0:64].astype(jnp.bfloat16), pick[128:256, 64:128].astype(jnp.bfloat16)]
    combine_high, combine_low = [], []
    for j in range(2):
        part_of = combine[j * 64 : (j + 1) * 64, j * 128 : (j + 1) * 128]
        combine_high.append(part_of.astype(jnp.bfloat16))
        combine_low.append((part_of - combine_high[j].astype(jnp.float32)).astype(jnp.bfloat16))

    def send_rows(j, i, pp):
        return p_copy(1 + j, disp.at[j, pp], xrow.at[t, me], pp, 1 + t, j)

    for j in range(2):
        with jax.named_scope(f"g_mixed#j={j}"):
            if j == 0:
                z_wait(8, ssall.at[pl.ds(0, 7)])
            z_wait(4 + j, rall.at[j, pl.ds(0, 7)])
        if j == 0:
            inverse = lax.rsqrt(jnp.sum(ssall[...], axis=0)[0:1, :] * (1.0 / WIDE) + epsilon)
            factor = jnp.sum(pick * inverse, axis=-1, keepdims=True)
        for zz in range(NZ):
            gain = gains[1, pl.ds(2 * zz + t, 1), :]
            rows = jnp.dot(picks[j], rall[j, zz].reshape(64, 128), preferred_element_type=jnp.float32)
            rows = rows * factor[j * 128 : (j + 1) * 128] * gain
            disp[j, :, :, zz * 128 : (zz + 1) * 128] = rows.astype(jnp.bfloat16).reshape(PLANE, 8, 128)
        over_plane(lambda i, pp, j=j: send_rows(j, i, pp).start())

    xrow[t, me] = disp[t, me]

    def to_other(phase, src, dst, arrive):
        return pltpu.make_async_remote_copy(
            src_ref=src,
            dst_ref=dst,
            send_sem=t_send.at[phase],
            recv_sem=p_recv.at[arrive],
            device_id={"tp": o},
            device_id_type=MESH,
        )

    give_rows = to_other(5, disp.at[o, me], xrow.at[t, me], 1 + t)
    give_rows.start()
    for swap in swaps:
        swap.wait_recv()
    with jax.named_scope("i_disp"):
        p_wait(1 + t, xrow.at[t, pl.ds(0, 15)])
        p_wait(1 + o, xrow.at[o])

    rows_in = [xrow[h].reshape(128, HALF) for h in range(2)]

    def hidden_act(gate_w, up_w):
        gate_act = jnp.dot(rows_in[0], gate_w[0], preferred_element_type=jnp.float32)
        gate_act = gate_act + jnp.dot(rows_in[1], gate_w[1], preferred_element_type=jnp.float32)
        up_act = jnp.dot(rows_in[0], up_w[0], preferred_element_type=jnp.float32)
        up_act = up_act + jnp.dot(rows_in[1], up_w[1], preferred_element_type=jnp.float32)
        return (gate_act * (1.0 / (1.0 + jnp.exp(-gate_act))) * up_act).astype(jnp.bfloat16)

    act_mine = hidden_act(gate_v, up_v)
    act_theirs = hidden_act(gate_p, up_p)

    def send_ret(h, q, i, pp):
        return p_copy(3 + h * 2 + q, ret.at[h, q, pp], back.at[t, q, me], pp, 3 + t * 2 + q, h)

    def give_ret(q):
        return t_copy(6 + q, ret.at[o, q, me], back.at[t, q, me])

    for q in range(2):
        for h in range(2):
            columns = slice(q * 512, (q + 1) * 512)
            one = jnp.dot(act_mine, down_v[h, :, columns], preferred_element_type=jnp.float32)
            two = jnp.dot(act_theirs, down_p[h, :, columns], preferred_element_type=jnp.float32)
            both = one.astype(jnp.bfloat16).astype(jnp.float32) + two.astype(jnp.bfloat16).astype(jnp.float32)
            ret[h, q] = both.astype(jnp.bfloat16).reshape(PLANE, 8, 512)
            over_plane(lambda i, pp, h=h, q=q: send_ret(h, q, i, pp).start())
        give_ret(q).start()
        back[t, q, me] = ret[t, q, me]

    def send_sum(j, q, d, zz):
        return z_copy(7 + 2 * q, psum.at[j, q, zz // 2], tsum.at[q, z], zz)

    for q in range(2):
        give_ret(q).wait_recv()
    for j in range(2):
        for q in range(2):
            with jax.named_scope(f"m_ret#j={j}#q={q}"):
                p_wait(3 + j * 2 + q, back.at[j, q, pl.ds(0, 15)])
            outs = back[j, q].reshape(128, 512)
            total = jnp.dot(combine_high[j], outs, preferred_element_type=jnp.float32)
            total = total + jnp.dot(combine_low[j], outs, preferred_element_type=jnp.float32)
            psum[j, q] = total.astype(jnp.bfloat16).reshape(4, ROWS, 512)
            for d in z_steps:
                if d % 2 == j:
                    send_sum(j, q, d, lax.rem(z + d, NZ)).start()
            if j == 0:
                tsum[q, z] = psum[0, q, pair]
    z_wait(6, mown.at[pl.ds(0, 7)])
    for q in range(2):
        with jax.named_scope(f"n_z#q={q}"):
            z_wait(7 + 2 * q, tsum.at[q, pl.ds(0, 7)])
        mix = jnp.sum(tsum[q].astype(jnp.float32), axis=0)
        for i in range(4):
            zz = q * 4 + i
            block = hid_block(zz)[...].astype(jnp.float32) + mown[zz].astype(jnp.float32)
            upd[:, zz * 128 : (zz + 1) * 128] = (block + mix[:, i * 128 : (i + 1) * 128]).astype(jnp.bfloat16)
    give_u = t_copy(1, upd, upd_in)
    give_u.start()
    for zz in range(NZ):
        out_ref[:, pl.ds(pl.multiple_of(zz * 256 + t * 128, 128), 128)] = upd[:, zz * 128 : (zz + 1) * 128]
    with jax.named_scope("o_u"):
        give_u.wait_recv()
    for zz in range(NZ):
        out_ref[:, pl.ds(pl.multiple_of(zz * 256 + o * 128, 128), 128)] = upd_in[:, zz * 128 : (zz + 1) * 128]

    with jax.named_scope("p_sends"):
        next_z, next_p = lax.rem(z + 1, NZ), lax.rem(me + 1, PLANE)
        sent = (
            aall.at[pl.ds(0, 7), pl.ds(0, 8)],
            aall.at[pl.ds(0, 7), pl.ds(8, 8)],
            hcol.at[pl.ds(0, 7)],
            infoall.at[pl.ds(0, 7)],
            rall.at[0, pl.ds(0, 7)],
            rall.at[1, pl.ds(0, 7)],
            mown.at[pl.ds(0, 7)],
            tsum.at[0, pl.ds(0, 7)],
            ssall.at[pl.ds(0, 7)],
            tsum.at[1, pl.ds(0, 7)],
        )
        for phase, ref in enumerate(sent):
            z_copy(phase, ref, ref, next_z).wait_send()
        sent = [wall.at[pl.ds(0, 15)], disp.at[0, pl.ds(0, 15)], disp.at[1, pl.ds(0, 15)]]
        sent += [ret.at[h, q, pl.ds(0, 15)] for h in range(2) for q in range(2)]
        for phase, ref in enumerate(sent):
            p_copy(phase, ref, ref, next_p, 0, t).wait_send()
        for give_one in [give, give_u, give_rows, give_ret(0), give_ret(1)] + swaps:
            give_one.wait_send()


def layer(lengths, *arrays):
    bf16, f32 = jnp.bfloat16, jnp.float32
    vmem = pl.BlockSpec(memory_space=pltpu.VMEM)
    hbm = pl.BlockSpec(memory_space=pltpu.HBM)
    dma = pltpu.SemaphoreType.DMA
    return pl.pallas_call(
        layer_kernel,
        out_shape=(
            pltpu.VMEM((ROWS, WIDE), bf16),
            pltpu.VMEM((ROWS, HD), bf16),
            pltpu.VMEM((ROWS, HD), bf16),
            pltpu.VMEM((ROWS, 16), f32),
        ),
        in_specs=[pl.BlockSpec(memory_space=pltpu.SMEM)] + [vmem] * 5 + [hbm] * 12,
        out_specs=(vmem,) * 4,
        scratch_shapes=[
            pltpu.VMEM((ROWS, WIDE), bf16),
            pltpu.VMEM((WIDE, HALF), bf16),
            pltpu.VMEM((144, WIDE), bf16),
            pltpu.VMEM((ROWS, HD, 1024), bf16),
            pltpu.VMEM((ROWS, HD, 1024), bf16),
            pltpu.VMEM((ROWS, 16, 1024), f32),
            pltpu.VMEM((ROWS, WIDE), bf16),
            pltpu.VMEM((ROWS, HALF), f32),
            pltpu.VMEM((256, HALF), bf16),
            pltpu.VMEM((256, HD), bf16),
            pltpu.VMEM((ROWS, 16), f32),
            pltpu.VMEM((ROWS, HD), f32),
            pltpu.VMEM((ROWS, HD), f32),
            pltpu.VMEM((256, HD), bf16),
            pltpu.VMEM((8, HALF), f32),
            pltpu.VMEM((ROWS, HALF), bf16),
            pltpu.VMEM((2, 16, 128), f32),
            pltpu.VMEM((8, 128), f32),
            pltpu.VMEM((NZ, 8, 128), f32),
            pltpu.VMEM((PLANE, ROWS, HALF), bf16),
            pltpu.VMEM((8, ROWS, HALF), bf16),
            pltpu.VMEM((8, ROWS, 256), bf16),
            pltpu.VMEM((2, NZ * ROWS, 128), f32),
            pltpu.VMEM((2, NZ * ROWS, 128), f32),
            pltpu.VMEM((2, 8, ROWS, 128), bf16),
            pltpu.VMEM((2, 2, 4, ROWS, 128), bf16),
            pltpu.VMEM((NZ, ROWS, 128), bf16),
            pltpu.VMEM((2, NZ, 4, ROWS, 128), bf16),
            pltpu.VMEM((2, 8, 128), f32),
            pltpu.VMEM((NZ, 8, 128), f32),
            pltpu.VMEM((2, PLANE, 8, HALF), bf16),
            pltpu.VMEM((2, PLANE, 8, HALF), bf16),
            pltpu.VMEM((2, HALF, 256), bf16),
            pltpu.VMEM((2, HALF, 256), bf16),
            pltpu.VMEM((2, 256, HALF), bf16),
            pltpu.VMEM((2, HALF, 256), bf16),
            pltpu.VMEM((2, HALF, 256), bf16),
            pltpu.VMEM((2, 256, HALF), bf16),
            pltpu.VMEM((2, 2, PLANE, 8, 512), bf16),
            pltpu.VMEM((2, 2, PLANE, 8, 512), bf16),
            pltpu.VMEM((2, 2, 4, ROWS, 512), bf16),
            pltpu.VMEM((2, NZ, ROWS, 512), bf16),
            pltpu.VMEM((ROWS, HALF), bf16),
            pltpu.VMEM((ROWS, HALF), bf16),
            dma((10,)),
            dma((10,)),
            dma((7,)),
            dma((7,)),
            dma((8,)),
            dma((8,)),
            dma((3,)),
            dma((21,)),
        ],
        compiler_params=pltpu.CompilerParams(
            collective_id=0, has_side_effects=True, vmem_limit_bytes=56 * 1024 * 1024
        ),
    )(lengths, *arrays)


def hand_over(*refs):
    for source, target in zip(refs[:4], refs[4:]):
        target[...] = source[...]


def write_out(*results):
    vmem = pl.BlockSpec(memory_space=pltpu.VMEM)
    return pl.pallas_call(
        hand_over,
        out_shape=tuple(jax.ShapeDtypeStruct(r.shape, r.dtype) for r in results),
        in_specs=[vmem] * 4,
        out_specs=(vmem,) * 4,
        compiler_params=pltpu.CompilerParams(vmem_limit_bytes=1024 * 1024),
    )(*results)


def per_device(
    hidden,
    attn_gain,
    query_weight,
    key_weight,
    value_weight,
    forget_weight,
    forget_bias,
    cache_keys,
    cache_values,
    cache_logsum,
    lengths,
    out_weight,
    ffn_gain,
    expert_ids,
    expert_scores,
    gate_weights,
    up_weights,
    down_weights,
):
    results = layer(
        lengths,
        attn_gain,
        ffn_gain,
        forget_bias,
        expert_ids.T,
        expert_scores.T,
        hidden,
        query_weight,
        key_weight.T,
        value_weight.T,
        forget_weight.T,
        cache_keys,
        cache_values,
        cache_logsum,
        out_weight,
        gate_weights,
        up_weights,
        down_weights,
    )
    updated, key_new, value_new, new_logsum = write_out(*results)
    return (updated, key_new[:, None, :], value_new[:, None, :], new_logsum)


def solution(mesh):
    split = Mesh(mesh.devices.reshape(8, 4, 4, mesh.shape["tp"]), ("ep_0", "ep_1", "ep_2", "tp"))
    in_specs = (
        P(EP, None),
        P(),
        P(None, "tp"),
        P(None, "tp"),
        P(None, "tp"),
        P(None, "tp"),
        P("tp"),
        P(EP, "tp", None, None),
        P(EP, "tp", None, None),
        P(EP, "tp", None),
        P(EP),
        P(EP, None),
        P(),
        P(EP, None),
        P(EP, None),
        P(EP, None, "tp"),
        P(EP, None, "tp"),
        P(EP, "tp", None),
    )
    out_specs = (P(EP, None), P(EP, "tp", None), P(EP, "tp", None), P(EP, "tp"))
    return jax.shard_map(
        per_device, mesh=split, in_specs=in_specs, out_specs=out_specs, check_vma=False
    )
```

```python
import jax
import jax.numpy as jnp
from jax import lax
from jax.experimental import pallas as pl
from jax.experimental.pallas import tpu as pltpu
from jax.sharding import Mesh
from jax.sharding import PartitionSpec as P

HD = 64
TOP_K = 6
EP = ("ep_0", "ep_1", "ep_2")
NZ = 8
NX = 4
PLANE = 16
ROWS = 16
HALF = 1024
WIDE = 2048
MESH = pl.DeviceIdType.MESH

epsilon = 1e-06


def layer_kernel(
    len_hbm,
    attn_gain_hbm,
    ffn_gain_hbm,
    bias_hbm,
    ids_hbm,
    scores_hbm,
    hid_hbm,
    wq_hbm,
    wk_hbm,
    wv_hbm,
    wf_hbm,
    keys_hbm,
    values_hbm,
    logsum_hbm,
    wo_ref,
    gate_ref,
    up_ref,
    down_ref,
    out_ref,
    key_out,
    value_out,
    logsum_out,
    len_ref,
    attn_gain_ref,
    ffn_gain_ref,
    bias_ref,
    ids_ref,
    scores_ref,
    hid_ref,
    wq,
    wkvf,
    keys,
    values,
    logsum,
    normed,
    queries,
    spread,
    heads_q,
    gate_col,
    own_col,
    new_val,
    scores,
    past_weight,
    att_rows,
    att_flat,
    att_ref,
    gains,
    info_ref,
    infoall,
    wall,
    aall,
    hcol,
    part,
    part_in,
    mixed,
    rounded,
    mown,
    rall,
    all_squares,
    ss,
    ssall,
    disp,
    xrow,
    gate_v,
    up_v,
    down_v,
    gate_p,
    up_p,
    down_p,
    ret,
    back,
    psum,
    tsum,
    upd,
    upd_in,
    z_send,
    z_recv,
    p_send,
    p_recv,
    t_send,
    t_recv,
    w_sem,
    a_sem,
):
    z = lax.axis_index("ep_0")
    y = lax.axis_index("ep_1")
    x = lax.axis_index("ep_2")
    t = lax.axis_index("tp")
    me = y * NX + x
    o = 1 - t
    parity = lax.rem(z, 2)
    pair = z // 2

    def z_copy(phase, src, dst, zz):
        return pltpu.make_async_remote_copy(
            src_ref=src,
            dst_ref=dst,
            send_sem=z_send.at[phase],
            recv_sem=z_recv.at[phase],
            device_id={"ep_0": zz},
            device_id_type=MESH,
        )

    def p_copy(phase, src, dst, pp, arrive, core):
        return pltpu.make_async_remote_copy(
            src_ref=src,
            dst_ref=dst,
            send_sem=p_send.at[phase],
            recv_sem=p_recv.at[arrive],
            device_id={"ep_1": pp // NX, "ep_2": lax.rem(pp, NX), "tp": core},
            device_id_type=MESH,
        )

    def t_copy(phase, src, dst):
        return pltpu.make_async_remote_copy(
            src_ref=src,
            dst_ref=dst,
            send_sem=t_send.at[phase],
            recv_sem=t_recv.at[phase],
            device_id={"tp": o},
            device_id_type=MESH,
        )

    z_steps = (4, 3, 5, 2, 6, 1, 7)
    p_steps = sorted(
        ((dy, dx) for dy in range(4) for dx in range(4) if dy or dx),
        key=lambda d: -(min(d[0], 4 - d[0]) + min(d[1], 4 - d[1])),
    )

    def over_z(fn):
        for d in z_steps:
            fn(d, lax.rem(z + d, NZ))

    def over_plane(fn):
        for i, (dy, dx) in enumerate(p_steps):
            fn(i, lax.rem(y + dy, 4) * NX + lax.rem(x + dx, 4))

    def z_wait(phase, ref):
        z_copy(phase, ref, ref, lax.rem(z + 1, NZ)).wait_recv()

    def p_wait(arrive, ref):
        p_copy(0, ref, ref, lax.rem(me + 1, PLANE), arrive, t).wait_recv()

    get_hid = pltpu.make_async_copy(hid_hbm, hid_ref, a_sem.at[0])
    get_hid.start()
    small = (
        (attn_gain_hbm, attn_gain_ref),
        (ids_hbm, ids_ref),
        (scores_hbm, scores_ref),
        (ffn_gain_hbm, ffn_gain_ref),
        (bias_hbm, bias_ref),
        (len_hbm, len_ref),
    )
    get_facts = [pltpu.make_async_copy(a, b, a_sem.at[21 + n]) for n, (a, b) in enumerate(small)]
    for copy in get_facts:
        copy.start()
    get_q = []
    for i in range(4):
        rows = pl.ds(i * 512, 512)
        get_q.append(pltpu.make_async_copy(wq_hbm.at[rows, :], wq.at[rows, :], a_sem.at[1 + i]))
    get_small = [
        pltpu.make_async_copy(wk_hbm, wkvf.at[pl.ds(0, 64)], a_sem.at[5]),
        pltpu.make_async_copy(wv_hbm, wkvf.at[pl.ds(64, 64)], a_sem.at[6]),
        pltpu.make_async_copy(wf_hbm, wkvf.at[pl.ds(128, 16)], a_sem.at[7]),
    ]
    get_cache = []
    for i in range(4):
        rows = pl.ds(i * 4, 4)
        get_cache.append(
            (
                pltpu.make_async_copy(keys_hbm.at[rows, 0], keys.at[rows], a_sem.at[8 + i]),
                pltpu.make_async_copy(logsum_hbm.at[rows], logsum.at[rows], a_sem.at[12 + i]),
                pltpu.make_async_copy(values_hbm.at[rows, 0], values.at[rows], a_sem.at[16 + i]),
            )
        )
    for copy in get_q + get_small:
        copy.start()
    for group in get_cache:
        for copy in group:
            copy.start()

    barrier = pltpu.get_barrier_semaphore()
    over_z(lambda d, zz: pl.semaphore_signal(barrier, inc=1, device_id={"ep_0": zz}, device_id_type=MESH))
    for core in range(2):
        over_plane(
            lambda d, pp, core=core: pl.semaphore_signal(
                barrier,
                inc=1,
                device_id={"ep_1": pp // NX, "ep_2": lax.rem(pp, NX), "tp": core},
                device_id_type=MESH,
            )
        )
    pl.semaphore_signal(barrier, inc=1, device_id={"tp": o}, device_id_type=MESH)

    get_facts[0].wait()
    gains[0] = attn_gain_ref[...].astype(jnp.float32).reshape(16, 128)
    get_hid.wait()
    total_sq = jnp.zeros((ROWS, 128), jnp.float32)
    for i in range(16):
        block = hid_ref[:, i * 128 : (i + 1) * 128].astype(jnp.float32)
        total_sq = total_sq + block * block
    inverse = lax.rsqrt(jnp.sum(total_sq, axis=-1, keepdims=True) * (1.0 / WIDE) + epsilon)
    for i in range(16):
        block = hid_ref[:, i * 128 : (i + 1) * 128].astype(jnp.float32)
        normed[:, i * 128 : (i + 1) * 128] = (block * inverse * gains[0, i : i + 1, :]).astype(jnp.bfloat16)
    my_columns = pl.ds(pl.multiple_of(t * HALF, HALF), HALF)

    def hid_block(zz):
        return hid_ref.at[:, pl.ds(pl.multiple_of(zz * 256 + t * 128, 128), 128)]

    def hid_cols(zz):
        return hid_ref.at[:, pl.ds(pl.multiple_of(zz * 256, 256), 256)]

    hcol[pair] = hid_cols(z)[...]

    query = jnp.zeros((ROWS, HALF), jnp.float32)
    for i in range(4):
        get_q[i].wait()
        query = query + jnp.dot(
            normed[:, i * 512 : (i + 1) * 512],
            wq[i * 512 : (i + 1) * 512, :],
            preferred_element_type=jnp.float32,
        )
    queries[...] = query.astype(jnp.bfloat16).astype(jnp.float32)

    get_wo = pltpu.make_async_copy(wo_ref.at[:, my_columns], wall.at[me], a_sem.at[20])
    get_wo.start()
    loads = []
    for zz in range(NZ):
        for h in range(2):
            rows = pl.ds(zz * 256 + h * 128, 128)
            put = pl.ds(zz * 128, 128)
            n = zz * 2 + h
            loads.append(pltpu.make_async_copy(gate_ref.at[0, rows, :], gate_v.at[h, put, :], w_sem.at[0]))
            loads.append(pltpu.make_async_copy(up_ref.at[0, rows, :], up_v.at[h, put, :], w_sem.at[1]))
            loads.append(pltpu.make_async_copy(down_ref.at[0, :, rows], down_v.at[h, :, put], w_sem.at[2]))

    def send_wo(i, pp):
        return p_copy(0, wo_ref.at[:, my_columns], wall.at[me], pp, 0, t)

    def send_hid(d, zz):
        return z_copy(2, hid_cols(zz), hcol.at[(d % 2) * 4 + pair], zz)

    def send_info(d, zz):
        return z_copy(3, info_ref, infoall.at[z], zz)

    def greet():
        with jax.named_scope("a_barrier"):
            pl.semaphore_wait(barrier, (NZ - 1) + 2 * (PLANE - 1) + 1)
        over_plane(lambda i, pp: send_wo(i, pp).start())
        over_z(lambda d, zz: send_hid(d, zz).start())
        for load in loads:
            load.start()

    greet()
    for copy in get_facts[1:]:
        copy.wait()
    info_ref[...] = jnp.zeros((8, 128), jnp.float32)
    info_ref[0:TOP_K, 0:ROWS] = ids_ref[...].astype(jnp.float32)
    shares = scores_ref[...] / jnp.sum(scores_ref[...], axis=0, keepdims=True)
    info_ref[0:TOP_K, ROWS : 2 * ROWS] = shares
    infoall[z] = info_ref[...]
    gains[1] = ffn_gain_ref[...].astype(jnp.float32).reshape(16, 128)

    for copy in get_small:
        copy.wait()
    three = lax.dot_general(
        normed[...], wkvf[...], (((1,), (1,)), ((), ())), preferred_element_type=jnp.float32
    )
    new_key = three[:, 0:64].astype(jnp.bfloat16)
    new_value = three[:, 64:128].astype(jnp.bfloat16)
    key_out[...] = new_key
    value_out[...] = new_value
    own_col[...] = new_key.astype(jnp.float32)
    new_val[...] = new_value.astype(jnp.float32)
    pre = three[:, 128:144] + bias_ref[...].reshape(1, 16)
    gate_col[...] = -(jnp.maximum(-pre, 0.0) + jnp.log1p(jnp.exp(-jnp.abs(pre))))

    head_of_row = lax.broadcasted_iota(jnp.int32, (ROWS, HALF), 0)
    head_of_lane = lax.broadcasted_iota(jnp.int32, (ROWS, HALF), 1) // HD
    own_lanes = head_of_row == head_of_lane
    for s in range(ROWS):
        spread[s * 16 : (s + 1) * 16, :] = jnp.where(
            own_lanes, jnp.broadcast_to(queries[s : s + 1, :], (16, HALF)), 0.0
        ).astype(jnp.bfloat16)
    fold = jnp.where(
        lax.rem(lax.broadcasted_iota(jnp.int32, (HALF, HD), 0), HD)
        == lax.broadcasted_iota(jnp.int32, (HALF, HD), 1),
        1.0,
        0.0,
    ).astype(jnp.bfloat16)
    heads_q[...] = jnp.dot(spread[...], fold, preferred_element_type=jnp.float32).astype(jnp.bfloat16)

    position = lax.broadcasted_iota(jnp.int32, (16, 1024), 1)
    diagonal = lax.broadcasted_iota(jnp.int32, (16, 16), 0) == lax.broadcasted_iota(jnp.int32, (16, 16), 1)
    score_scale = HD ** (-0.5)

    def send_att(piece, d, zz):
        rows = pl.ds(piece * 8, 8)
        return z_copy(piece, att_ref.at[rows], aall.at[(d % 2) * 4 + pair, rows], zz)

    for piece in range(2):
        for group in get_cache[2 * piece : 2 * piece + 2]:
            for copy in group:
                copy.wait()
        tops, own_scores, own_weights = [], [], []
        for i in range(8):
            s = piece * 8 + i
            q_s = heads_q[s * 16 : (s + 1) * 16, :]
            raw = jnp.dot(q_s, keys[s], preferred_element_type=jnp.float32) * score_scale
            length = len_ref[s]
            sums = logsum[s]
            last = jnp.sum(jnp.where(position == length - 1, sums, 0.0), axis=-1, keepdims=True)
            forget = jnp.sum(
                jnp.where(diagonal, jnp.broadcast_to(gate_col[s : s + 1, :], (16, 16)), 0.0),
                axis=-1,
                keepdims=True,
            )
            new_sum = last + forget
            logsum_out[s : s + 1, :] = jnp.sum(
                jnp.where(diagonal, jnp.broadcast_to(new_sum, (16, 16)), 0.0), axis=0, keepdims=True
            )
            masked = jnp.where(position < length, raw + new_sum - sums, -jnp.inf)
            own_score = (
                jnp.sum(q_s.astype(jnp.float32) * own_col[s : s + 1, :], axis=-1, keepdims=True) * score_scale
            )
            scores[i] = masked
            own_scores.append(own_score)
            tops.append(jnp.maximum(jnp.max(masked, axis=-1, keepdims=True), own_score))
        for i in range(8):
            past = jnp.exp(scores[i] - tops[i])
            own_exp = jnp.exp(own_scores[i] - tops[i])
            share = 1.0 / (jnp.sum(past, axis=-1, keepdims=True) + own_exp)
            past_weight[i] = (past * share).astype(jnp.bfloat16)
            own_weights.append((own_exp * share).astype(jnp.bfloat16).astype(jnp.float32))
        for i in range(8):
            s = piece * 8 + i
            attended = lax.dot_general(
                past_weight[i], values[s], (((1,), (1,)), ((), ())), preferred_element_type=jnp.float32
            )
            attended = attended + own_weights[i] * new_val[s : s + 1, :]
            att_rows[s * 16 : (s + 1) * 16, :] = attended.astype(jnp.bfloat16)
        wide = lax.dot_general(
            att_rows[piece * 128 : (piece + 1) * 128, :],
            fold,
            (((1,), (1,)), ((), ())),
            preferred_element_type=jnp.float32,
        )
        for i in range(8):
            att_flat[i : i + 1, :] = jnp.sum(
                jnp.where(own_lanes, wide[i * 16 : (i + 1) * 16, :], 0.0), axis=0, keepdims=True
            )
        att_ref[piece * 8 : (piece + 1) * 8, :] = att_flat[...].astype(jnp.bfloat16)
        over_z(lambda d, zz, piece=piece: send_att(piece, d, zz).start())
    over_z(lambda d, zz: send_info(d, zz).start())
    aall[pair] = att_ref[...]
    wholes = ((gate_v, gate_p), (up_v, up_p), (down_v, down_p))
    swaps = []
    for n, (mine, theirs) in enumerate(wholes):
        pltpu.make_async_copy(mine, mine, w_sem.at[n]).wait()
        swaps.append(t_copy(2 + n, mine, theirs))
        swaps[n].start()

    get_wo.wait()
    with jax.named_scope("b_w"):
        p_wait(0, wall.at[pl.ds(0, 15)])
    def send_rounded(j, piece, d, zz):
        return z_copy(4 + 6 * piece + j, rounded.at[t, piece, (d + j) % 2], rall.at[j, z, piece], zz)

    def send_mixed(d, zz):
        return z_copy(6, mixed.at[t, (d % 2) * 4 + zz // 2], mown.at[z], zz)

    def send_ss(d, zz):
        return z_copy(8, ss.at[d % 2], ssall.at[z], zz)

    gives = [t_copy(8 * piece, part.at[piece], part_in.at[piece]) for piece in range(2)]
    for piece in range(2):
        eight = slice(piece * 8, (piece + 1) * 8)
        with jax.named_scope(f"c_att#p={piece}"):
            z_wait(piece, aall.at[pl.ds(0, 7), pl.ds(piece * 8, 8)])
        att = aall[:, eight, :].reshape(64, HALF)
        for h in range(2):
            weights = wall[h * 8 : (h + 1) * 8].reshape(128, HALF)
            part[piece, h] = lax.dot_general(
                att, weights, (((1,), (1,)), ((), ())), preferred_element_type=jnp.float32
            )
        gives[piece].start()
    with jax.named_scope("e_hid"):
        z_wait(2, hcol.at[pl.ds(0, 7)])
    for piece in range(2):
        eight = slice(piece * 8, (piece + 1) * 8)
        with jax.named_scope(f"e_give#p={piece}"):
            gives[piece].wait_recv()
        squares = jnp.zeros((64, 128), jnp.float32)
        for h in range(2):
            mixed_now = (part[piece, h] + part_in[piece, h]).astype(jnp.bfloat16)
            hid_now = hcol[:, eight, h * 128 : (h + 1) * 128].reshape(64, 128).astype(jnp.float32)
            residual = hid_now + mixed_now.astype(jnp.float32)
            squares = squares + residual * residual
            mixed[h, :, eight, :] = mixed_now.reshape(8, 8, 128)
            rounded[h, piece] = residual.astype(jnp.bfloat16).reshape(2, 4, 8, 128)
        for j in range(2):
            all_squares[j, piece] = squares[j * 32 : (j + 1) * 32]
        over_z(lambda d, zz, piece=piece: send_rounded(0, piece, d, zz).start())
        if piece == 1:
            sums = lax.dot_general(
                jnp.ones((8, 128), jnp.float32),
                all_squares[...].reshape(128, 128),
                (((1,), (1,)), ((), ())),
                precision=lax.Precision.HIGHEST,
                preferred_element_type=jnp.float32,
            )
            ss[0] = sums
            ss[1] = pltpu.roll(sums, 64, 1)
            over_z(lambda d, zz: send_ss(d, zz).start())
        over_z(lambda d, zz, piece=piece: send_rounded(1, piece, d, zz).start())
    over_z(lambda d, zz: send_mixed(d, zz).start())
    ssall[z] = ss[0]
    for j in range(2):
        for piece in range(2):
            rall[j, z, piece] = rounded[t, piece, j]
    mown[z] = mixed[t, pair]

    with jax.named_scope("d_info"):
        z_wait(3, infoall.at[pl.ds(0, 7)])
    lane = lax.broadcasted_iota(jnp.int32, (8, 128), 1)
    routes = jnp.zeros((8, 128), jnp.float32)
    weights_of = jnp.zeros((8, 128), jnp.float32)
    for zz in range(NZ):
        tile = infoall[zz]
        place = lax.rem(z + zz, 2) * 64 + (zz // 2) * 8
        for piece in range(2):
            low = piece * 8
            one = jnp.where((lane >= low) & (lane < low + 8), tile, 0.0)
            routes = routes + pltpu.roll(one, lax.rem(place + 32 * piece + 128 - low, 128), 1)
            low = ROWS + piece * 8
            one = jnp.where((lane >= low) & (lane < low + 8), tile, 0.0)
            weights_of = weights_of + pltpu.roll(one, lax.rem(place + 32 * piece + 128 - low, 128), 1)
    row = lax.broadcasted_iota(jnp.int32, (256, 128), 0)
    token = lax.broadcasted_iota(jnp.int32, (256, 128), 1)
    expert = (lax.rem(row, 128) // 8 + z * PLANE).astype(jnp.float32)
    named = jnp.zeros((256, 128), jnp.float32)
    scale = jnp.zeros((256, 128), jnp.float32)
    for j in range(TOP_K):
        hit = routes[j : j + 1, :] == expert
        named = named + jnp.where(hit, 1.0, 0.0)
        scale = scale + jnp.where(hit, weights_of[j : j + 1, :], 0.0)
    first = lax.broadcasted_iota(jnp.int32, (128, 128), 0)
    second = lax.broadcasted_iota(jnp.int32, (128, 128), 1)
    same = (first // 64 == second // 64) & (lax.rem(first, 32) // 8 == lax.rem(second, 32) // 8)
    place_first = lax.rem(first, 64) // 32 * 8 + lax.rem(first, 8)
    place_second = lax.rem(second, 64) // 32 * 8 + lax.rem(second, 8)
    ahead = jnp.where(same & (place_first < place_second), 1.0, 0.0).astype(jnp.bfloat16)
    rank = jnp.dot(named.astype(jnp.bfloat16), ahead, preferred_element_type=jnp.float32)
    slot = lax.rem(row, 2).astype(jnp.float32)
    here = (row // 128 == token // 64) & (lax.rem(row, 8) // 2 == lax.rem(token, 32) // 8)
    pick = jnp.where(here & (rank == slot), named, 0.0)
    combine = jnp.transpose(pick * scale)
    picks = [pick[0:128, 0:64].astype(jnp.bfloat16), pick[128:256, 64:128].astype(jnp.bfloat16)]
    combine_high, combine_low = [], []
    for j in range(2):
        part_of = combine[j * 64 : (j + 1) * 64, j * 128 : (j + 1) * 128]
        combine_high.append(part_of.astype(jnp.bfloat16))
        combine_low.append((part_of - combine_high[j].astype(jnp.float32)).astype(jnp.bfloat16))

    def send_rows(j, i, pp):
        return p_copy(1 + j, disp.at[j, pp], xrow.at[t, me], pp, 1 + t, j)

    for j in range(2):
        with jax.named_scope(f"g_mixed#j={j}"):
            if j == 0:
                z_wait(8, ssall.at[pl.ds(0, 7)])
            for piece in range(2):
                z_wait(4 + 6 * piece + j, rall.at[j, pl.ds(0, 7), piece])
        if j == 0:
            inverse = lax.rsqrt(jnp.sum(ssall[...], axis=0)[0:1, :] * (1.0 / WIDE) + epsilon)
            factor = jnp.sum(pick * inverse, axis=-1, keepdims=True)
        for zz in range(NZ):
            gain = gains[1, pl.ds(2 * zz + t, 1), :]
            rows = jnp.dot(picks[j], rall[j, zz].reshape(64, 128), preferred_element_type=jnp.float32)
            rows = rows * factor[j * 128 : (j + 1) * 128] * gain
            disp[j, :, :, zz * 128 : (zz + 1) * 128] = rows.astype(jnp.bfloat16).reshape(PLANE, 8, 128)
        over_plane(lambda i, pp, j=j: send_rows(j, i, pp).start())

    xrow[t, me] = disp[t, me]

    def to_other(phase, src, dst, arrive):
        return pltpu.make_async_remote_copy(
            src_ref=src,
            dst_ref=dst,
            send_sem=t_send.at[phase],
            recv_sem=p_recv.at[arrive],
            device_id={"tp": o},
            device_id_type=MESH,
        )

    give_rows = to_other(5, disp.at[o, me], xrow.at[t, me], 1 + t)
    give_rows.start()
    for swap in swaps:
        swap.wait_recv()
    with jax.named_scope("i_disp"):
        p_wait(1 + t, xrow.at[t, pl.ds(0, 15)])
        p_wait(1 + o, xrow.at[o])

    rows_in = [xrow[h].reshape(128, HALF) for h in range(2)]

    def hidden_act(gate_w, up_w):
        gate_act = jnp.dot(rows_in[0], gate_w[0], preferred_element_type=jnp.float32)
        gate_act = gate_act + jnp.dot(rows_in[1], gate_w[1], preferred_element_type=jnp.float32)
        up_act = jnp.dot(rows_in[0], up_w[0], preferred_element_type=jnp.float32)
        up_act = up_act + jnp.dot(rows_in[1], up_w[1], preferred_element_type=jnp.float32)
        return (gate_act * (1.0 / (1.0 + jnp.exp(-gate_act))) * up_act).astype(jnp.bfloat16)

    act_mine = hidden_act(gate_v, up_v)
    act_theirs = hidden_act(gate_p, up_p)

    def send_ret(h, q, i, pp):
        return p_copy(3 + h * 2 + q, ret.at[h, q, pp], back.at[t, q, me], pp, 3 + t * 2 + q, h)

    def give_ret(q):
        return t_copy(6 + q, ret.at[o, q, me], back.at[t, q, me])

    for q in range(2):
        for h in range(2):
            columns = slice(q * 512, (q + 1) * 512)
            one = jnp.dot(act_mine, down_v[h, :, columns], preferred_element_type=jnp.float32)
            two = jnp.dot(act_theirs, down_p[h, :, columns], preferred_element_type=jnp.float32)
            both = one.astype(jnp.bfloat16).astype(jnp.float32) + two.astype(jnp.bfloat16).astype(jnp.float32)
            ret[h, q] = both.astype(jnp.bfloat16).reshape(PLANE, 8, 512)
            over_plane(lambda i, pp, h=h, q=q: send_ret(h, q, i, pp).start())
        give_ret(q).start()
        back[t, q, me] = ret[t, q, me]

    def send_sum(j, q, d, zz):
        return z_copy(7 + 2 * q, psum.at[j, q, zz // 2], tsum.at[q, z], zz)

    for q in range(2):
        give_ret(q).wait_recv()
    for j in range(2):
        for q in range(2):
            with jax.named_scope(f"m_ret#j={j}#q={q}"):
                p_wait(3 + j * 2 + q, back.at[j, q, pl.ds(0, 15)])
            outs = back[j, q].reshape(128, 512)
            total = jnp.dot(combine_high[j], outs, preferred_element_type=jnp.float32)
            total = total + jnp.dot(combine_low[j], outs, preferred_element_type=jnp.float32)
            for piece in range(2):
                half = total[piece * 32 : (piece + 1) * 32]
                psum[j, q, :, piece * 8 : (piece + 1) * 8, :] = half.astype(jnp.bfloat16).reshape(4, 8, 512)
            for d in z_steps:
                if d % 2 == j:
                    send_sum(j, q, d, lax.rem(z + d, NZ)).start()
            if j == 0:
                tsum[q, z] = psum[0, q, pair]
    z_wait(6, mown.at[pl.ds(0, 7)])
    for q in range(2):
        with jax.named_scope(f"n_z#q={q}"):
            z_wait(7 + 2 * q, tsum.at[q, pl.ds(0, 7)])
        mix = jnp.sum(tsum[q].astype(jnp.float32), axis=0)
        for i in range(4):
            zz = q * 4 + i
            block = hid_block(zz)[...].astype(jnp.float32) + mown[zz].astype(jnp.float32)
            upd[:, zz * 128 : (zz + 1) * 128] = (block + mix[:, i * 128 : (i + 1) * 128]).astype(jnp.bfloat16)
    give_u = t_copy(1, upd, upd_in)
    give_u.start()
    for zz in range(NZ):
        out_ref[:, pl.ds(pl.multiple_of(zz * 256 + t * 128, 128), 128)] = upd[:, zz * 128 : (zz + 1) * 128]
    with jax.named_scope("o_u"):
        give_u.wait_recv()
    for zz in range(NZ):
        out_ref[:, pl.ds(pl.multiple_of(zz * 256 + o * 128, 128), 128)] = upd_in[:, zz * 128 : (zz + 1) * 128]

    with jax.named_scope("p_sends"):
        next_z, next_p = lax.rem(z + 1, NZ), lax.rem(me + 1, PLANE)
        sent = (
            aall.at[pl.ds(0, 7), pl.ds(0, 8)],
            aall.at[pl.ds(0, 7), pl.ds(8, 8)],
            hcol.at[pl.ds(0, 7)],
            infoall.at[pl.ds(0, 7)],
            rall.at[0, pl.ds(0, 7), 0],
            rall.at[1, pl.ds(0, 7), 0],
            mown.at[pl.ds(0, 7)],
            tsum.at[0, pl.ds(0, 7)],
            ssall.at[pl.ds(0, 7)],
            tsum.at[1, pl.ds(0, 7)],
            rall.at[0, pl.ds(0, 7), 1],
            rall.at[1, pl.ds(0, 7), 1],
        )
        for phase, ref in enumerate(sent):
            z_copy(phase, ref, ref, next_z).wait_send()
        sent = [wall.at[pl.ds(0, 15)], disp.at[0, pl.ds(0, 15)], disp.at[1, pl.ds(0, 15)]]
        sent += [ret.at[h, q, pl.ds(0, 15)] for h in range(2) for q in range(2)]
        for phase, ref in enumerate(sent):
            p_copy(phase, ref, ref, next_p, 0, t).wait_send()
        for give_one in [give_u, give_rows, give_ret(0), give_ret(1)] + gives + swaps:
            give_one.wait_send()


def layer(lengths, *arrays):
    bf16, f32 = jnp.bfloat16, jnp.float32
    vmem = pl.BlockSpec(memory_space=pltpu.VMEM)
    hbm = pl.BlockSpec(memory_space=pltpu.HBM)
    dma = pltpu.SemaphoreType.DMA
    return pl.pallas_call(
        layer_kernel,
        out_shape=(
            pltpu.VMEM((ROWS, WIDE), bf16),
            pltpu.VMEM((ROWS, HD), bf16),
            pltpu.VMEM((ROWS, HD), bf16),
            pltpu.VMEM((ROWS, 16), f32),
        ),
        in_specs=[hbm] * 18,
        out_specs=(vmem,) * 4,
        scratch_shapes=[
            pltpu.SMEM((ROWS,), jnp.int32),
            pltpu.VMEM((WIDE,), bf16),
            pltpu.VMEM((WIDE,), bf16),
            pltpu.VMEM((16,), f32),
            pltpu.VMEM((TOP_K, ROWS), jnp.int32),
            pltpu.VMEM((TOP_K, ROWS), f32),
            pltpu.VMEM((ROWS, WIDE), bf16),
            pltpu.VMEM((WIDE, HALF), bf16),
            pltpu.VMEM((144, WIDE), bf16),
            pltpu.VMEM((ROWS, HD, 1024), bf16),
            pltpu.VMEM((ROWS, HD, 1024), bf16),
            pltpu.VMEM((ROWS, 16, 1024), f32),
            pltpu.VMEM((ROWS, WIDE), bf16),
            pltpu.VMEM((ROWS, HALF), f32),
            pltpu.VMEM((256, HALF), bf16),
            pltpu.VMEM((256, HD), bf16),
            pltpu.VMEM((ROWS, 16), f32),
            pltpu.VMEM((ROWS, HD), f32),
            pltpu.VMEM((ROWS, HD), f32),
            pltpu.VMEM((8, 16, 1024), f32),
            pltpu.VMEM((8, 16, 1024), bf16),
            pltpu.VMEM((256, HD), bf16),
            pltpu.VMEM((8, HALF), f32),
            pltpu.VMEM((ROWS, HALF), bf16),
            pltpu.VMEM((2, 16, 128), f32),
            pltpu.VMEM((8, 128), f32),
            pltpu.VMEM((NZ, 8, 128), f32),
            pltpu.VMEM((PLANE, ROWS, HALF), bf16),
            pltpu.VMEM((8, ROWS, HALF), bf16),
            pltpu.VMEM((8, ROWS, 256), bf16),
            pltpu.VMEM((2, 2, 64, 128), f32),
            pltpu.VMEM((2, 2, 64, 128), f32),
            pltpu.VMEM((2, 8, ROWS, 128), bf16),
            pltpu.VMEM((2, 2, 2, 4, 8, 128), bf16),
            pltpu.VMEM((NZ, ROWS, 128), bf16),
            pltpu.VMEM((2, NZ, 2, 4, 8, 128), bf16),
            pltpu.VMEM((2, 2, 32, 128), f32),
            pltpu.VMEM((2, 8, 128), f32),
            pltpu.VMEM((NZ, 8, 128), f32),
            pltpu.VMEM((2, PLANE, 8, HALF), bf16),
            pltpu.VMEM((2, PLANE, 8, HALF), bf16),
            pltpu.VMEM((2, HALF, 256), bf16),
            pltpu.VMEM((2, HALF, 256), bf16),
            pltpu.VMEM((2, 256, HALF), bf16),
            pltpu.VMEM((2, HALF, 256), bf16),
            pltpu.VMEM((2, HALF, 256), bf16),
            pltpu.VMEM((2, 256, HALF), bf16),
            pltpu.VMEM((2, 2, PLANE, 8, 512), bf16),
            pltpu.VMEM((2, 2, PLANE, 8, 512), bf16),
            pltpu.VMEM((2, 2, 4, ROWS, 512), bf16),
            pltpu.VMEM((2, NZ, ROWS, 512), bf16),
            pltpu.VMEM((ROWS, HALF), bf16),
            pltpu.VMEM((ROWS, HALF), bf16),
            dma((12,)),
            dma((12,)),
            dma((7,)),
            dma((7,)),
            dma((9,)),
            dma((9,)),
            dma((3,)),
            dma((27,)),
        ],
        compiler_params=pltpu.CompilerParams(
            collective_id=0, has_side_effects=True, vmem_limit_bytes=56 * 1024 * 1024
        ),
    )(lengths, *arrays)


def hand_over(*refs):
    for source, target in zip(refs[:4], refs[4:]):
        target[...] = source[...]


def write_out(*results):
    vmem = pl.BlockSpec(memory_space=pltpu.VMEM)
    return pl.pallas_call(
        hand_over,
        out_shape=tuple(jax.ShapeDtypeStruct(r.shape, r.dtype) for r in results),
        in_specs=[vmem] * 4,
        out_specs=(vmem,) * 4,
        compiler_params=pltpu.CompilerParams(vmem_limit_bytes=1024 * 1024),
    )(*results)


def per_device(
    hidden,
    attn_gain,
    query_weight,
    key_weight,
    value_weight,
    forget_weight,
    forget_bias,
    cache_keys,
    cache_values,
    cache_logsum,
    lengths,
    out_weight,
    ffn_gain,
    expert_ids,
    expert_scores,
    gate_weights,
    up_weights,
    down_weights,
):
    results = layer(
        lengths,
        attn_gain,
        ffn_gain,
        forget_bias,
        expert_ids.T,
        expert_scores.T,
        hidden,
        query_weight,
        key_weight.T,
        value_weight.T,
        forget_weight.T,
        cache_keys,
        cache_values,
        cache_logsum,
        out_weight,
        gate_weights,
        up_weights,
        down_weights,
    )
    updated, key_new, value_new, new_logsum = write_out(*results)
    return (updated, key_new[:, None, :], value_new[:, None, :], new_logsum)


def solution(mesh):
    split = Mesh(mesh.devices.reshape(8, 4, 4, mesh.shape["tp"]), ("ep_0", "ep_1", "ep_2", "tp"))
    in_specs = (
        P(EP, None),
        P(),
        P(None, "tp"),
        P(None, "tp"),
        P(None, "tp"),
        P(None, "tp"),
        P("tp"),
        P(EP, "tp", None, None),
        P(EP, "tp", None, None),
        P(EP, "tp", None),
        P(EP),
        P(EP, None),
        P(),
        P(EP, None),
        P(EP, None),
        P(EP, None, "tp"),
        P(EP, None, "tp"),
        P(EP, "tp", None),
    )
    out_specs = (P(EP, None), P(EP, "tp", None), P(EP, "tp", None), P(EP, "tp"))
    return jax.shard_map(
        per_device, mesh=split, in_specs=in_specs, out_specs=out_specs, check_vma=False
    )
```

```python
import jax
import jax.numpy as jnp
from jax import lax
from jax.experimental import pallas as pl
from jax.experimental.pallas import tpu as pltpu
from jax.sharding import Mesh
from jax.sharding import PartitionSpec as P

HD = 64
TOP_K = 6
EP = ("ep_0", "ep_1", "ep_2")
NZ = 8
NX = 4
PLANE = 16
ROWS = 16
HALF = 1024
WIDE = 2048
MESH = pl.DeviceIdType.MESH

epsilon = 1e-06


def layer_kernel(
    len_hbm,
    attn_gain_hbm,
    ffn_gain_hbm,
    bias_hbm,
    ids_hbm,
    scores_hbm,
    hid_hbm,
    wq_hbm,
    wk_hbm,
    wv_hbm,
    wf_hbm,
    keys_hbm,
    values_hbm,
    logsum_hbm,
    wo_ref,
    gate_ref,
    up_ref,
    down_ref,
    out_ref,
    key_out,
    value_out,
    logsum_out,
    len_ref,
    attn_gain_ref,
    ffn_gain_ref,
    bias_ref,
    ids_ref,
    scores_ref,
    hid_ref,
    wq,
    wkvf,
    keys,
    values,
    logsum,
    normed,
    queries,
    spread,
    heads_q,
    gate_col,
    own_col,
    new_val,
    scores,
    past_weight,
    att_rows,
    att_flat,
    att_ref,
    gains,
    info_ref,
    infoall,
    wall,
    aall,
    hcol,
    part,
    part_in,
    mixed,
    rounded,
    mown,
    rall,
    all_squares,
    ss,
    ssall,
    disp,
    xrow,
    gate_v,
    up_v,
    down_v,
    gate_p,
    up_p,
    down_p,
    ret,
    back,
    psum,
    tsum,
    upd,
    upd_in,
    z_send,
    z_recv,
    p_send,
    p_recv,
    t_send,
    t_recv,
    w_sem,
    a_sem,
):
    z = lax.axis_index("ep_0")
    y = lax.axis_index("ep_1")
    x = lax.axis_index("ep_2")
    t = lax.axis_index("tp")
    me = y * NX + x
    o = 1 - t
    parity = lax.rem(z, 2)
    pair = z // 2

    def z_copy(phase, src, dst, zz):
        return pltpu.make_async_remote_copy(
            src_ref=src,
            dst_ref=dst,
            send_sem=z_send.at[phase],
            recv_sem=z_recv.at[phase],
            device_id={"ep_0": zz},
            device_id_type=MESH,
        )

    def p_copy(phase, src, dst, pp, arrive, core):
        return pltpu.make_async_remote_copy(
            src_ref=src,
            dst_ref=dst,
            send_sem=p_send.at[phase],
            recv_sem=p_recv.at[arrive],
            device_id={"ep_1": pp // NX, "ep_2": lax.rem(pp, NX), "tp": core},
            device_id_type=MESH,
        )

    def t_copy(phase, src, dst):
        return pltpu.make_async_remote_copy(
            src_ref=src,
            dst_ref=dst,
            send_sem=t_send.at[phase],
            recv_sem=t_recv.at[phase],
            device_id={"tp": o},
            device_id_type=MESH,
        )

    z_steps = (4, 3, 5, 2, 6, 1, 7)
    p_steps = sorted(
        ((dy, dx) for dy in range(4) for dx in range(4) if dy or dx),
        key=lambda d: -(min(d[0], 4 - d[0]) + min(d[1], 4 - d[1])),
    )

    def over_z(fn):
        for d in z_steps:
            fn(d, lax.rem(z + d, NZ))

    def over_plane(fn):
        for i, (dy, dx) in enumerate(p_steps):
            fn(i, lax.rem(y + dy, 4) * NX + lax.rem(x + dx, 4))

    def z_wait(phase, ref):
        z_copy(phase, ref, ref, lax.rem(z + 1, NZ)).wait_recv()

    def p_wait(arrive, ref):
        p_copy(0, ref, ref, lax.rem(me + 1, PLANE), arrive, t).wait_recv()

    get_hid = pltpu.make_async_copy(hid_hbm, hid_ref, a_sem.at[0])
    get_hid.start()
    small = (
        (attn_gain_hbm, attn_gain_ref),
        (ids_hbm, ids_ref),
        (scores_hbm, scores_ref),
        (ffn_gain_hbm, ffn_gain_ref),
        (bias_hbm, bias_ref),
        (len_hbm, len_ref),
    )
    get_facts = [pltpu.make_async_copy(a, b, a_sem.at[21 + n]) for n, (a, b) in enumerate(small)]
    for copy in get_facts:
        copy.start()
    get_q = []
    for i in range(4):
        rows = pl.ds(i * 512, 512)
        get_q.append(pltpu.make_async_copy(wq_hbm.at[rows, :], wq.at[rows, :], a_sem.at[1 + i]))
    get_small = [
        pltpu.make_async_copy(wk_hbm, wkvf.at[pl.ds(0, 64)], a_sem.at[5]),
        pltpu.make_async_copy(wv_hbm, wkvf.at[pl.ds(64, 64)], a_sem.at[6]),
        pltpu.make_async_copy(wf_hbm, wkvf.at[pl.ds(128, 16)], a_sem.at[7]),
    ]
    get_cache = []
    for i in range(4):
        rows = pl.ds(i * 4, 4)
        get_cache.append(
            (
                pltpu.make_async_copy(keys_hbm.at[rows, 0], keys.at[rows], a_sem.at[8 + i]),
                pltpu.make_async_copy(logsum_hbm.at[rows], logsum.at[rows], a_sem.at[12 + i]),
                pltpu.make_async_copy(values_hbm.at[rows, 0], values.at[rows], a_sem.at[16 + i]),
            )
        )
    for copy in get_q + get_small:
        copy.start()
    for group in get_cache:
        for copy in group:
            copy.start()

    barrier = pltpu.get_barrier_semaphore()
    over_z(lambda d, zz: pl.semaphore_signal(barrier, inc=1, device_id={"ep_0": zz}, device_id_type=MESH))
    for core in range(2):
        over_plane(
            lambda d, pp, core=core: pl.semaphore_signal(
                barrier,
                inc=1,
                device_id={"ep_1": pp // NX, "ep_2": lax.rem(pp, NX), "tp": core},
                device_id_type=MESH,
            )
        )
    pl.semaphore_signal(barrier, inc=1, device_id={"tp": o}, device_id_type=MESH)

    get_facts[0].wait()
    gains[0] = attn_gain_ref[...].astype(jnp.float32).reshape(16, 128)
    get_hid.wait()
    total_sq = jnp.zeros((ROWS, 128), jnp.float32)
    for i in range(16):
        block = hid_ref[:, i * 128 : (i + 1) * 128].astype(jnp.float32)
        total_sq = total_sq + block * block
    inverse = lax.rsqrt(jnp.sum(total_sq, axis=-1, keepdims=True) * (1.0 / WIDE) + epsilon)
    for i in range(16):
        block = hid_ref[:, i * 128 : (i + 1) * 128].astype(jnp.float32)
        normed[:, i * 128 : (i + 1) * 128] = (block * inverse * gains[0, i : i + 1, :]).astype(jnp.bfloat16)
    my_columns = pl.ds(pl.multiple_of(t * HALF, HALF), HALF)

    def hid_block(zz):
        return hid_ref.at[:, pl.ds(pl.multiple_of(zz * 256 + t * 128, 128), 128)]

    def hid_cols(zz):
        return hid_ref.at[:, pl.ds(pl.multiple_of(zz * 256, 256), 256)]

    hcol[pair] = hid_cols(z)[...]

    query = jnp.zeros((ROWS, HALF), jnp.float32)
    for i in range(4):
        get_q[i].wait()
        query = query + jnp.dot(
            normed[:, i * 512 : (i + 1) * 512],
            wq[i * 512 : (i + 1) * 512, :],
            preferred_element_type=jnp.float32,
        )
    queries[...] = query.astype(jnp.bfloat16).astype(jnp.float32)

    get_wo = pltpu.make_async_copy(wo_ref.at[:, my_columns], wall.at[me], a_sem.at[20])
    get_wo.start()
    loads = []
    for zz in range(NZ):
        for h in range(2):
            rows = pl.ds(zz * 256 + h * 128, 128)
            put = pl.ds(zz * 128, 128)
            n = zz * 2 + h
            loads.append(pltpu.make_async_copy(gate_ref.at[0, rows, :], gate_v.at[h, put, :], w_sem.at[0]))
            loads.append(pltpu.make_async_copy(up_ref.at[0, rows, :], up_v.at[h, put, :], w_sem.at[1]))
            loads.append(pltpu.make_async_copy(down_ref.at[0, :, rows], down_v.at[h, :, put], w_sem.at[2]))

    def send_wo(i, pp):
        return p_copy(0, wo_ref.at[:, my_columns], wall.at[me], pp, 0, t)

    def send_hid(d, zz):
        return z_copy(2, hid_cols(zz), hcol.at[(d % 2) * 4 + pair], zz)

    def send_info(d, zz):
        return z_copy(3, info_ref, infoall.at[z], zz)

    def greet():
        with jax.named_scope("a_barrier"):
            pl.semaphore_wait(barrier, (NZ - 1) + 2 * (PLANE - 1) + 1)
        over_plane(lambda i, pp: send_wo(i, pp).start())
        over_z(lambda d, zz: send_hid(d, zz).start())
        for load in loads:
            load.start()

    greet()
    for copy in get_facts[1:]:
        copy.wait()
    info_ref[...] = jnp.zeros((8, 128), jnp.float32)
    info_ref[0:TOP_K, 0:ROWS] = ids_ref[...].astype(jnp.float32)
    shares = scores_ref[...] / jnp.sum(scores_ref[...], axis=0, keepdims=True)
    info_ref[0:TOP_K, ROWS : 2 * ROWS] = shares
    infoall[z] = info_ref[...]
    gains[1] = ffn_gain_ref[...].astype(jnp.float32).reshape(16, 128)

    for copy in get_small:
        copy.wait()
    three = lax.dot_general(
        normed[...], wkvf[...], (((1,), (1,)), ((), ())), preferred_element_type=jnp.float32
    )
    new_key = three[:, 0:64].astype(jnp.bfloat16)
    new_value = three[:, 64:128].astype(jnp.bfloat16)
    key_out[...] = new_key
    value_out[...] = new_value
    own_col[...] = new_key.astype(jnp.float32)
    new_val[...] = new_value.astype(jnp.float32)
    pre = three[:, 128:144] + bias_ref[...].reshape(1, 16)
    gate_col[...] = -(jnp.maximum(-pre, 0.0) + jnp.log1p(jnp.exp(-jnp.abs(pre))))

    head_of_row = lax.broadcasted_iota(jnp.int32, (ROWS, HALF), 0)
    head_of_lane = lax.broadcasted_iota(jnp.int32, (ROWS, HALF), 1) // HD
    own_lanes = head_of_row == head_of_lane
    for s in range(ROWS):
        spread[s * 16 : (s + 1) * 16, :] = jnp.where(
            own_lanes, jnp.broadcast_to(queries[s : s + 1, :], (16, HALF)), 0.0
        ).astype(jnp.bfloat16)
    fold = jnp.where(
        lax.rem(lax.broadcasted_iota(jnp.int32, (HALF, HD), 0), HD)
        == lax.broadcasted_iota(jnp.int32, (HALF, HD), 1),
        1.0,
        0.0,
    ).astype(jnp.bfloat16)
    heads_q[...] = jnp.dot(spread[...], fold, preferred_element_type=jnp.float32).astype(jnp.bfloat16)

    position = lax.broadcasted_iota(jnp.int32, (16, 1024), 1)
    diagonal = lax.broadcasted_iota(jnp.int32, (16, 16), 0) == lax.broadcasted_iota(jnp.int32, (16, 16), 1)
    score_scale = HD ** (-0.5)

    def send_att(piece, d, zz):
        rows = pl.ds(piece * 8, 8)
        return z_copy(piece, att_ref.at[rows], aall.at[(d % 2) * 4 + pair, rows], zz)

    for piece in range(2):
        for group in get_cache[2 * piece : 2 * piece + 2]:
            for copy in group:
                copy.wait()
        tops, own_scores, own_weights = [], [], []
        for i in range(8):
            s = piece * 8 + i
            q_s = heads_q[s * 16 : (s + 1) * 16, :]
            raw = jnp.dot(q_s, keys[s], preferred_element_type=jnp.float32) * score_scale
            length = len_ref[s]
            sums = logsum[s]
            last = jnp.sum(jnp.where(position == length - 1, sums, 0.0), axis=-1, keepdims=True)
            forget = jnp.sum(
                jnp.where(diagonal, jnp.broadcast_to(gate_col[s : s + 1, :], (16, 16)), 0.0),
                axis=-1,
                keepdims=True,
            )
            new_sum = last + forget
            logsum_out[s : s + 1, :] = jnp.sum(
                jnp.where(diagonal, jnp.broadcast_to(new_sum, (16, 16)), 0.0), axis=0, keepdims=True
            )
            masked = jnp.where(position < length, raw + new_sum - sums, -jnp.inf)
            own_score = (
                jnp.sum(q_s.astype(jnp.float32) * own_col[s : s + 1, :], axis=-1, keepdims=True) * score_scale
            )
            scores[i] = masked
            own_scores.append(own_score)
            tops.append(jnp.maximum(jnp.max(masked, axis=-1, keepdims=True), own_score))
        for i in range(8):
            past = jnp.exp(scores[i] - tops[i])
            own_exp = jnp.exp(own_scores[i] - tops[i])
            share = 1.0 / (jnp.sum(past, axis=-1, keepdims=True) + own_exp)
            past_weight[i] = (past * share).astype(jnp.bfloat16)
            own_weights.append((own_exp * share).astype(jnp.bfloat16).astype(jnp.float32))
        for i in range(8):
            s = piece * 8 + i
            attended = lax.dot_general(
                past_weight[i], values[s], (((1,), (1,)), ((), ())), preferred_element_type=jnp.float32
            )
            attended = attended + own_weights[i] * new_val[s : s + 1, :]
            att_rows[s * 16 : (s + 1) * 16, :] = attended.astype(jnp.bfloat16)
        wide = lax.dot_general(
            att_rows[piece * 128 : (piece + 1) * 128, :],
            fold,
            (((1,), (1,)), ((), ())),
            preferred_element_type=jnp.float32,
        )
        for i in range(8):
            att_flat[i : i + 1, :] = jnp.sum(
                jnp.where(own_lanes, wide[i * 16 : (i + 1) * 16, :], 0.0), axis=0, keepdims=True
            )
        att_ref[piece * 8 : (piece + 1) * 8, :] = att_flat[...].astype(jnp.bfloat16)
        over_z(lambda d, zz, piece=piece: send_att(piece, d, zz).start())
    over_z(lambda d, zz: send_info(d, zz).start())
    aall[pair] = att_ref[...]
    wholes = ((gate_v, gate_p), (up_v, up_p), (down_v, down_p))
    swaps = []
    for n, (mine, theirs) in enumerate(wholes):
        pltpu.make_async_copy(mine, mine, w_sem.at[n]).wait()
        swaps.append(t_copy(2 + n, mine, theirs))
        swaps[n].start()

    get_wo.wait()
    with jax.named_scope("b_w"):
        p_wait(0, wall.at[pl.ds(0, 15)])
    def send_rounded(j, piece, d, zz):
        return z_copy(4 + 6 * piece + j, rounded.at[t, piece, (d + j) % 2], rall.at[j, z, piece], zz)

    def send_mixed(d, zz):
        return z_copy(6, mixed.at[t, (d % 2) * 4 + zz // 2], mown.at[z], zz)

    def send_ss(d, zz):
        return z_copy(8, ss.at[d % 2], ssall.at[z], zz)

    gives = [t_copy(8 * piece, part.at[piece], part_in.at[piece]) for piece in range(2)]
    for piece in range(2):
        eight = slice(piece * 8, (piece + 1) * 8)
        with jax.named_scope(f"c_att#p={piece}"):
            z_wait(piece, aall.at[pl.ds(0, 7), pl.ds(piece * 8, 8)])
        att = aall[:, eight, :].reshape(64, HALF)
        for h in range(2):
            weights = wall[h * 8 : (h + 1) * 8].reshape(128, HALF)
            part[piece, h] = lax.dot_general(
                att, weights, (((1,), (1,)), ((), ())), preferred_element_type=jnp.float32
            )
        gives[piece].start()
    with jax.named_scope("e_hid"):
        z_wait(2, hcol.at[pl.ds(0, 7)])
    for piece in range(2):
        eight = slice(piece * 8, (piece + 1) * 8)
        with jax.named_scope(f"e_give#p={piece}"):
            gives[piece].wait_recv()
        squares = jnp.zeros((64, 128), jnp.float32)
        for h in range(2):
            mixed_now = (part[piece, h] + part_in[piece, h]).astype(jnp.bfloat16)
            hid_now = hcol[:, eight, h * 128 : (h + 1) * 128].reshape(64, 128).astype(jnp.float32)
            residual = hid_now + mixed_now.astype(jnp.float32)
            squares = squares + residual * residual
            mixed[h, :, eight, :] = mixed_now.reshape(8, 8, 128)
            rounded[h, piece] = residual.astype(jnp.bfloat16).reshape(2, 4, 8, 128)
        for j in range(2):
            all_squares[j, piece] = squares[j * 32 : (j + 1) * 32]
        over_z(lambda d, zz, piece=piece: send_rounded(0, piece, d, zz).start())
        if piece == 1:
            sums = lax.dot_general(
                jnp.ones((8, 128), jnp.float32),
                all_squares[...].reshape(128, 128),
                (((1,), (1,)), ((), ())),
                precision=lax.Precision.HIGHEST,
                preferred_element_type=jnp.float32,
            )
            ss[0] = sums
            ss[1] = pltpu.roll(sums, 64, 1)
            over_z(lambda d, zz: send_ss(d, zz).start())
        over_z(lambda d, zz, piece=piece: send_rounded(1, piece, d, zz).start())
    over_z(lambda d, zz: send_mixed(d, zz).start())
    ssall[z] = ss[0]
    for j in range(2):
        for piece in range(2):
            rall[j, z, piece] = rounded[t, piece, j]
    mown[z] = mixed[t, pair]

    with jax.named_scope("d_info"):
        z_wait(3, infoall.at[pl.ds(0, 7)])
    lane = lax.broadcasted_iota(jnp.int32, (8, 128), 1)
    routes = jnp.zeros((8, 128), jnp.float32)
    weights_of = jnp.zeros((8, 128), jnp.float32)
    for zz in range(NZ):
        tile = infoall[zz]
        place = lax.rem(z + zz, 2) * 64 + (zz // 2) * 8
        for piece in range(2):
            low = piece * 8
            one = jnp.where((lane >= low) & (lane < low + 8), tile, 0.0)
            routes = routes + pltpu.roll(one, lax.rem(place + 32 * piece + 128 - low, 128), 1)
            low = ROWS + piece * 8
            one = jnp.where((lane >= low) & (lane < low + 8), tile, 0.0)
            weights_of = weights_of + pltpu.roll(one, lax.rem(place + 32 * piece + 128 - low, 128), 1)
    row = lax.broadcasted_iota(jnp.int32, (256, 128), 0)
    token = lax.broadcasted_iota(jnp.int32, (256, 128), 1)
    expert = (lax.rem(row, 128) // 8 + z * PLANE).astype(jnp.float32)
    named = jnp.zeros((256, 128), jnp.float32)
    scale = jnp.zeros((256, 128), jnp.float32)
    for j in range(TOP_K):
        hit = routes[j : j + 1, :] == expert
        named = named + jnp.where(hit, 1.0, 0.0)
        scale = scale + jnp.where(hit, weights_of[j : j + 1, :], 0.0)
    first = lax.broadcasted_iota(jnp.int32, (128, 128), 0)
    second = lax.broadcasted_iota(jnp.int32, (128, 128), 1)
    same = (first // 64 == second // 64) & (lax.rem(first, 32) // 8 == lax.rem(second, 32) // 8)
    place_first = lax.rem(first, 64) // 32 * 8 + lax.rem(first, 8)
    place_second = lax.rem(second, 64) // 32 * 8 + lax.rem(second, 8)
    ahead = jnp.where(same & (place_first < place_second), 1.0, 0.0).astype(jnp.bfloat16)
    rank = jnp.dot(named.astype(jnp.bfloat16), ahead, preferred_element_type=jnp.float32)
    slot = lax.rem(row, 2).astype(jnp.float32)
    here = (row // 128 == token // 64) & (lax.rem(row, 8) // 2 == lax.rem(token, 32) // 8)
    pick = jnp.where(here & (rank == slot), named, 0.0)
    combine = jnp.transpose(pick * scale)
    picks = [pick[0:128, 0:64].astype(jnp.bfloat16), pick[128:256, 64:128].astype(jnp.bfloat16)]
    combine_high, combine_low = [], []
    for j in range(2):
        part_of = combine[j * 64 : (j + 1) * 64, j * 128 : (j + 1) * 128]
        combine_high.append(part_of.astype(jnp.bfloat16))
        combine_low.append((part_of - combine_high[j].astype(jnp.float32)).astype(jnp.bfloat16))

    def send_rows(j, i, pp):
        return p_copy(1 + j, disp.at[j, pp], xrow.at[t, me], pp, 1 + t, j)

    for j in range(2):
        with jax.named_scope(f"g_mixed#j={j}"):
            if j == 0:
                z_wait(8, ssall.at[pl.ds(0, 7)])
            for piece in range(2):
                z_wait(4 + 6 * piece + j, rall.at[j, pl.ds(0, 7), piece])
        if j == 0:
            inverse = lax.rsqrt(jnp.sum(ssall[...], axis=0)[0:1, :] * (1.0 / WIDE) + epsilon)
            factor = jnp.sum(pick * inverse, axis=-1, keepdims=True)
        for zz in range(NZ):
            gain = gains[1, pl.ds(2 * zz + t, 1), :]
            rows = jnp.dot(picks[j], rall[j, zz].reshape(64, 128), preferred_element_type=jnp.float32)
            rows = rows * factor[j * 128 : (j + 1) * 128] * gain
            disp[j, :, :, zz * 128 : (zz + 1) * 128] = rows.astype(jnp.bfloat16).reshape(PLANE, 8, 128)
        over_plane(lambda i, pp, j=j: send_rows(j, i, pp).start())

    xrow[t, me] = disp[t, me]

    def to_other(phase, src, dst, arrive):
        return pltpu.make_async_remote_copy(
            src_ref=src,
            dst_ref=dst,
            send_sem=t_send.at[phase],
            recv_sem=p_recv.at[arrive],
            device_id={"tp": o},
            device_id_type=MESH,
        )

    give_rows = to_other(5, disp.at[o, me], xrow.at[t, me], 1 + t)
    give_rows.start()
    for swap in swaps:
        swap.wait_recv()
    with jax.named_scope("i_disp"):
        p_wait(1 + t, xrow.at[t, pl.ds(0, 15)])
        p_wait(1 + o, xrow.at[o])

    rows_in = [xrow[h].reshape(128, HALF) for h in range(2)]

    def hidden_act(gate_w, up_w):
        gate_act = jnp.dot(rows_in[0], gate_w[0], preferred_element_type=jnp.float32)
        gate_act = gate_act + jnp.dot(rows_in[1], gate_w[1], preferred_element_type=jnp.float32)
        up_act = jnp.dot(rows_in[0], up_w[0], preferred_element_type=jnp.float32)
        up_act = up_act + jnp.dot(rows_in[1], up_w[1], preferred_element_type=jnp.float32)
        return (gate_act * (1.0 / (1.0 + jnp.exp(-gate_act))) * up_act).astype(jnp.bfloat16)

    act_mine = hidden_act(gate_v, up_v)
    act_theirs = hidden_act(gate_p, up_p)

    def send_ret(h, q, i, pp):
        return p_copy(3 + h * 2 + q, ret.at[h, q, pp], back.at[t, q, me], pp, 3 + t * 2 + q, h)

    def give_ret(q):
        return t_copy(6 + q, ret.at[o, q, me], back.at[t, q, me])

    for q in range(2):
        for h in range(2):
            columns = slice(q * 512, (q + 1) * 512)
            one = jnp.dot(act_mine, down_v[h, :, columns], preferred_element_type=jnp.float32)
            two = jnp.dot(act_theirs, down_p[h, :, columns], preferred_element_type=jnp.float32)
            both = one.astype(jnp.bfloat16).astype(jnp.float32) + two.astype(jnp.bfloat16).astype(jnp.float32)
            ret[h, q] = both.astype(jnp.bfloat16).reshape(PLANE, 8, 512)
            over_plane(lambda i, pp, h=h, q=q: send_ret(h, q, i, pp).start())
        give_ret(q).start()
        back[t, q, me] = ret[t, q, me]

    def send_sum(j, q, d, zz):
        return z_copy(7 + 2 * q, psum.at[j, q, zz // 2], tsum.at[q, z], zz)

    for q in range(2):
        give_ret(q).wait_recv()
    for q in range(2):
        for j in range(2):
            with jax.named_scope(f"m_ret#j={j}#q={q}"):
                p_wait(3 + j * 2 + q, back.at[j, q, pl.ds(0, 15)])
            outs = back[j, q].reshape(128, 512)
            total = jnp.dot(combine_high[j], outs, preferred_element_type=jnp.float32)
            total = total + jnp.dot(combine_low[j], outs, preferred_element_type=jnp.float32)
            for piece in range(2):
                half = total[piece * 32 : (piece + 1) * 32]
                psum[j, q, :, piece * 8 : (piece + 1) * 8, :] = half.astype(jnp.bfloat16).reshape(4, 8, 512)
            for d in z_steps:
                if d % 2 == j:
                    send_sum(j, q, d, lax.rem(z + d, NZ)).start()
            if j == 0:
                tsum[q, z] = psum[0, q, pair]
    z_wait(6, mown.at[pl.ds(0, 7)])
    for q in range(2):
        with jax.named_scope(f"n_z#q={q}"):
            z_wait(7 + 2 * q, tsum.at[q, pl.ds(0, 7)])
        mix = jnp.sum(tsum[q].astype(jnp.float32), axis=0)
        for i in range(4):
            zz = q * 4 + i
            block = hid_block(zz)[...].astype(jnp.float32) + mown[zz].astype(jnp.float32)
            upd[:, zz * 128 : (zz + 1) * 128] = (block + mix[:, i * 128 : (i + 1) * 128]).astype(jnp.bfloat16)
    give_u = t_copy(1, upd, upd_in)
    give_u.start()
    for zz in range(NZ):
        out_ref[:, pl.ds(pl.multiple_of(zz * 256 + t * 128, 128), 128)] = upd[:, zz * 128 : (zz + 1) * 128]
    with jax.named_scope("o_u"):
        give_u.wait_recv()
    for zz in range(NZ):
        out_ref[:, pl.ds(pl.multiple_of(zz * 256 + o * 128, 128), 128)] = upd_in[:, zz * 128 : (zz + 1) * 128]

    with jax.named_scope("p_sends"):
        next_z, next_p = lax.rem(z + 1, NZ), lax.rem(me + 1, PLANE)
        sent = (
            aall.at[pl.ds(0, 7), pl.ds(0, 8)],
            aall.at[pl.ds(0, 7), pl.ds(8, 8)],
            hcol.at[pl.ds(0, 7)],
            infoall.at[pl.ds(0, 7)],
            rall.at[0, pl.ds(0, 7), 0],
            rall.at[1, pl.ds(0, 7), 0],
            mown.at[pl.ds(0, 7)],
            tsum.at[0, pl.ds(0, 7)],
            ssall.at[pl.ds(0, 7)],
            tsum.at[1, pl.ds(0, 7)],
            rall.at[0, pl.ds(0, 7), 1],
            rall.at[1, pl.ds(0, 7), 1],
        )
        for phase, ref in enumerate(sent):
            z_copy(phase, ref, ref, next_z).wait_send()
        sent = [wall.at[pl.ds(0, 15)], disp.at[0, pl.ds(0, 15)], disp.at[1, pl.ds(0, 15)]]
        sent += [ret.at[h, q, pl.ds(0, 15)] for h in range(2) for q in range(2)]
        for phase, ref in enumerate(sent):
            p_copy(phase, ref, ref, next_p, 0, t).wait_send()
        for give_one in [give_u, give_rows, give_ret(0), give_ret(1)] + gives + swaps:
            give_one.wait_send()


def layer(lengths, *arrays):
    bf16, f32 = jnp.bfloat16, jnp.float32
    vmem = pl.BlockSpec(memory_space=pltpu.VMEM)
    hbm = pl.BlockSpec(memory_space=pltpu.HBM)
    dma = pltpu.SemaphoreType.DMA
    return pl.pallas_call(
        layer_kernel,
        out_shape=(
            pltpu.VMEM((ROWS, WIDE), bf16),
            pltpu.VMEM((ROWS, HD), bf16),
            pltpu.VMEM((ROWS, HD), bf16),
            pltpu.VMEM((ROWS, 16), f32),
        ),
        in_specs=[hbm] * 18,
        out_specs=(vmem,) * 4,
        scratch_shapes=[
            pltpu.SMEM((ROWS,), jnp.int32),
            pltpu.VMEM((WIDE,), bf16),
            pltpu.VMEM((WIDE,), bf16),
            pltpu.VMEM((16,), f32),
            pltpu.VMEM((TOP_K, ROWS), jnp.int32),
            pltpu.VMEM((TOP_K, ROWS), f32),
            pltpu.VMEM((ROWS, WIDE), bf16),
            pltpu.VMEM((WIDE, HALF), bf16),
            pltpu.VMEM((144, WIDE), bf16),
            pltpu.VMEM((ROWS, HD, 1024), bf16),
            pltpu.VMEM((ROWS, HD, 1024), bf16),
            pltpu.VMEM((ROWS, 16, 1024), f32),
            pltpu.VMEM((ROWS, WIDE), bf16),
            pltpu.VMEM((ROWS, HALF), f32),
            pltpu.VMEM((256, HALF), bf16),
            pltpu.VMEM((256, HD), bf16),
            pltpu.VMEM((ROWS, 16), f32),
            pltpu.VMEM((ROWS, HD), f32),
            pltpu.VMEM((ROWS, HD), f32),
            pltpu.VMEM((8, 16, 1024), f32),
            pltpu.VMEM((8, 16, 1024), bf16),
            pltpu.VMEM((256, HD), bf16),
            pltpu.VMEM((8, HALF), f32),
            pltpu.VMEM((ROWS, HALF), bf16),
            pltpu.VMEM((2, 16, 128), f32),
            pltpu.VMEM((8, 128), f32),
            pltpu.VMEM((NZ, 8, 128), f32),
            pltpu.VMEM((PLANE, ROWS, HALF), bf16),
            pltpu.VMEM((8, ROWS, HALF), bf16),
            pltpu.VMEM((8, ROWS, 256), bf16),
            pltpu.VMEM((2, 2, 64, 128), f32),
            pltpu.VMEM((2, 2, 64, 128), f32),
            pltpu.VMEM((2, 8, ROWS, 128), bf16),
            pltpu.VMEM((2, 2, 2, 4, 8, 128), bf16),
            pltpu.VMEM((NZ, ROWS, 128), bf16),
            pltpu.VMEM((2, NZ, 2, 4, 8, 128), bf16),
            pltpu.VMEM((2, 2, 32, 128), f32),
            pltpu.VMEM((2, 8, 128), f32),
            pltpu.VMEM((NZ, 8, 128), f32),
            pltpu.VMEM((2, PLANE, 8, HALF), bf16),
            pltpu.VMEM((2, PLANE, 8, HALF), bf16),
            pltpu.VMEM((2, HALF, 256), bf16),
            pltpu.VMEM((2, HALF, 256), bf16),
            pltpu.VMEM((2, 256, HALF), bf16),
            pltpu.VMEM((2, HALF, 256), bf16),
            pltpu.VMEM((2, HALF, 256), bf16),
            pltpu.VMEM((2, 256, HALF), bf16),
            pltpu.VMEM((2, 2, PLANE, 8, 512), bf16),
            pltpu.VMEM((2, 2, PLANE, 8, 512), bf16),
            pltpu.VMEM((2, 2, 4, ROWS, 512), bf16),
            pltpu.VMEM((2, NZ, ROWS, 512), bf16),
            pltpu.VMEM((ROWS, HALF), bf16),
            pltpu.VMEM((ROWS, HALF), bf16),
            dma((12,)),
            dma((12,)),
            dma((7,)),
            dma((7,)),
            dma((9,)),
            dma((9,)),
            dma((3,)),
            dma((27,)),
        ],
        compiler_params=pltpu.CompilerParams(
            collective_id=0, has_side_effects=True, vmem_limit_bytes=56 * 1024 * 1024
        ),
    )(lengths, *arrays)


def hand_over(*refs):
    for source, target in zip(refs[:4], refs[4:]):
        target[...] = source[...]


def write_out(*results):
    vmem = pl.BlockSpec(memory_space=pltpu.VMEM)
    return pl.pallas_call(
        hand_over,
        out_shape=tuple(jax.ShapeDtypeStruct(r.shape, r.dtype) for r in results),
        in_specs=[vmem] * 4,
        out_specs=(vmem,) * 4,
        compiler_params=pltpu.CompilerParams(vmem_limit_bytes=1024 * 1024),
    )(*results)


def per_device(
    hidden,
    attn_gain,
    query_weight,
    key_weight,
    value_weight,
    forget_weight,
    forget_bias,
    cache_keys,
    cache_values,
    cache_logsum,
    lengths,
    out_weight,
    ffn_gain,
    expert_ids,
    expert_scores,
    gate_weights,
    up_weights,
    down_weights,
):
    results = layer(
        lengths,
        attn_gain,
        ffn_gain,
        forget_bias,
        expert_ids.T,
        expert_scores.T,
        hidden,
        query_weight,
        key_weight.T,
        value_weight.T,
        forget_weight.T,
        cache_keys,
        cache_values,
        cache_logsum,
        out_weight,
        gate_weights,
        up_weights,
        down_weights,
    )
    updated, key_new, value_new, new_logsum = write_out(*results)
    return (updated, key_new[:, None, :], value_new[:, None, :], new_logsum)


def solution(mesh):
    split = Mesh(mesh.devices.reshape(8, 4, 4, mesh.shape["tp"]), ("ep_0", "ep_1", "ep_2", "tp"))
    in_specs = (
        P(EP, None),
        P(),
        P(None, "tp"),
        P(None, "tp"),
        P(None, "tp"),
        P(None, "tp"),
        P("tp"),
        P(EP, "tp", None, None),
        P(EP, "tp", None, None),
        P(EP, "tp", None),
        P(EP),
        P(EP, None),
        P(),
        P(EP, None),
        P(EP, None),
        P(EP, None, "tp"),
        P(EP, None, "tp"),
        P(EP, "tp", None),
    )
    out_specs = (P(EP, None), P(EP, "tp", None), P(EP, "tp", None), P(EP, "tp"))
    return jax.shard_map(
        per_device, mesh=split, in_specs=in_specs, out_specs=out_specs, check_vma=False
    )
```
